512 devices in a mesh: dp: 4 (over x), kv: 64 (over z, y), tp: 2 (over core).
Axes of the slice: x: 4, y: 8, z: 8, core: 2. Of those that a mesh axis runs over, the one named last changes fastest.
Arguments:
- tokens: bfloat16 [512, 2048], P('dp', 'kv'), may hold values from -16 to 16
- pre_gain: float32 [2048], P('kv'), may hold values from 0.1 to 1.9
- query_weight: bfloat16 [2048, 1024], P('kv', 'tp'), may hold values from -0.125 to 0.125
- key_weight: bfloat16 [2048, 1024], P('kv', 'tp'), may hold values from -0.125 to 0.125
- value_weight: bfloat16 [2048, 1024], P('kv', 'tp'), may hold values from -0.125 to 0.125
- outgate_weight: bfloat16 [2048, 1024], P('kv', 'tp'), may hold values from -0.125 to 0.125
- input_gate_weight: bfloat16 [2048, 4], replicated, may hold values from -0.125 to 0.125
- forget_gate_weight: bfloat16 [2048, 4], replicated, may hold values from -0.125 to 0.125
- cache_keys: bfloat16 [512, 64, 1024], P(('dp', 'kv'), None, 'tp'), may hold values from -6 to 6
- cache_values: bfloat16 [512, 64, 1024], P(('dp', 'kv'), None, 'tp'), may hold values from -6 to 6
- cache_input: float32 [512, 64, 4], P(('dp', 'kv'), None, 'tp'), may hold values from -6 to 250
- cache_forget: float32 [512, 64, 4], P(('dp', 'kv'), None, 'tp'), may hold values from -0.7 to 0
- lengths: int32 [512], P(('dp', 'kv')), may hold values from 1 to 64, 13107 in all
- state_matrix: float32 [512, 4, 256, 256], P(('dp', 'kv'), 'tp'), may hold values from -6 to 6
- state_norm: float32 [512, 4, 256], P(('dp', 'kv'), 'tp'), may hold values from -6 to 6
- state_max: float32 [512, 4], P(('dp', 'kv'), 'tp'), may hold values from -4 to 253
- head_gain: float32 [1024], P('tp'), may hold values from 0.1 to 1.9
- out_weight: bfloat16 [1024, 2048], P('tp', 'kv'), may hold values from -0.375 to 0.375
- mixer_gain: float32 [2048], replicated, may hold values from 0.1 to 1.9
- gate_weight: bfloat16 [2048, 5632], P(None, ('kv', 'tp')), may hold values from -0.125 to 0.125
- up_weight: bfloat16 [2048, 5632], P(None, ('kv', 'tp')), may hold values from -0.125 to 0.125
- down_weight: bfloat16 [5632, 2048], P(('kv', 'tp')), may hold values from -0.625 to 0.625
Outputs:
- layer_out: bfloat16 [512, 2048], P('dp', ('kv', 'tp'))
The draws below stay inside these ranges and needn't reach their ends.
Inputs may be any that keep to these rules, and one draw needn't show every extreme that they name: `lengths`: positions from a sequence's length on take no part.
All inputs are finite; a program needn't handle non-finite values. No bound on the sum of `lengths` on one device may be relied on, other than what follows from the above.
Results may differ from the reference program's by a relative error of at most 0.018.
Values may be sent and summed in bfloat16 or wider, within the bound.
A program may use at most 64 MiB of HBM per device.

```python
import math
import jax
import jax.numpy as jnp
import numpy as np
from jax import lax

D = 2048
MEMORY_HEADS = 4
HEAD_DIM = 256
FF = 5632
FOLD_SPAN = 64
HW = 1024
SEQUENCE_TOTAL = 512
N_TP = 2


def draw_cache_input(key, part):
    noise = jnp.clip(jax.random.normal(jax.random.fold_in(key, 11), (SEQUENCE_TOTAL, FOLD_SPAN, MEMORY_HEADS), jnp.float32), -6.0, 6.0)
    return noise


def draw_state_max(key, part):
    noise = jnp.clip(jax.random.normal(jax.random.fold_in(key, 13), (SEQUENCE_TOTAL, MEMORY_HEADS), jnp.float32), -4.0, 4.0)
    return noise


def draw_cache_forget(key, part):
    divided_random_keys = jax.random.split(jax.random.fold_in(key, 17), 6)
    fast_share = 0.5
    fast = jax.random.bernoulli(divided_random_keys[0], fast_share, (SEQUENCE_TOTAL, MEMORY_HEADS))
    fast_rate = jax.random.uniform(divided_random_keys[1], (SEQUENCE_TOTAL, MEMORY_HEADS), jnp.float32, math.log(10.0) / 50.0, math.log(10.0) / 30.0)
    slow_rate = jax.random.uniform(divided_random_keys[2], (SEQUENCE_TOTAL, MEMORY_HEADS), jnp.float32, 0.1, 0.8) * (math.log(10.0) / FOLD_SPAN)
    rate = jnp.where(fast, fast_rate, slow_rate)
    jitter = jax.random.uniform(divided_random_keys[3], (SEQUENCE_TOTAL, FOLD_SPAN, MEMORY_HEADS), jnp.float32, 0.5, 1.5)
    retain_logarithm = -rate[:, None, :] * jitter
    sudden_spike = jax.random.bernoulli(divided_random_keys[4], 3.0 / FOLD_SPAN, (SEQUENCE_TOTAL, FOLD_SPAN, MEMORY_HEADS))
    discarded_entries = jnp.log(jax.random.uniform(divided_random_keys[5], (SEQUENCE_TOTAL, FOLD_SPAN, MEMORY_HEADS), jnp.float32, 0.5, 0.8))
    return jnp.where(sudden_spike, discarded_entries, retain_logarithm)


def spiked(values, key, source, target, blocks, factor):
    owner, partner = [(jnp.arange(values.shape[position]) // (values.shape[position] // blocks)).reshape([-1 if axis == position else 1 for axis in range(values.ndim)]) for position in (source, target)]
    chosen = jax.random.permutation(key, blocks)[partner]
    strong = (owner == chosen) | (owner == (partner + blocks // 2) % blocks)
    return jnp.where(strong, factor * values, values)


def block_levels(stream_key, shape, cuts, low, largest):
    level = 1.0
    for axis_at, blocks in cuts:
        draws = jax.random.uniform(jax.random.fold_in(jax.random.fold_in(stream_key, 6), axis_at), (blocks,), jnp.float32, low / len(cuts), largest / len(cuts))
        level = level * jnp.repeat(jnp.exp(draws), shape[axis_at] // blocks).reshape((-1,) + (1,) * (len(shape) - 1 - axis_at))
    return level


def split_up(number_of, total, limit, slope):
    weights = [(1 << 20) // math.isqrt(grade ** slope) + 1 for grade in range(2, number_of + 1)]
    surplus, counts = total - limit - (number_of - 1), [1] * (number_of - 1)
    while surplus > 0:
        candidates = [i for i in range(number_of - 1) if counts[i] < limit]
        whole, remaining = sum([weights[i] for i in candidates]), surplus
        for i in candidates:
            addition = min(limit - counts[i], max(1, remaining * weights[i] // whole), surplus)
            counts[i] = counts[i] + addition
            surplus = surplus - addition
    return np.array([limit] + counts)


def ragged_sizes(own_key, amount, total, most, slope):
    if amount == 2:
        one = jax.random.randint(own_key, (), max(1, total - most), min(most, total - 1) + 1)
        return jnp.stack([one, total - one])
    sizes = jnp.asarray(split_up(amount, total, most, slope), jnp.int32)
    twos = (amount - 1) // 2
    donor, sink = sizes[1:1 + 2 * twos:2], sizes[2:2 + 2 * twos:2]
    room = jnp.minimum(donor - 1, most - sink)
    moved = jax.random.randint(jax.random.fold_in(own_key, 1), (twos,), 0, 1 << 20) % (room + 1)
    sizes = sizes.at[1:1 + 2 * twos:2].set(donor - moved).at[2:2 + 2 * twos:2].set(sink + moved)
    return sizes[jax.random.permutation(jax.random.fold_in(own_key, 2), amount)]


def gaussian(rng, extent, scale, reach, cuts=(), kind=jnp.bfloat16):
    level = block_levels(rng, extent, cuts, -0.22, 0.18) if cuts else 1.0
    result = jax.random.normal(rng, extent, jnp.float32) * scale * level
    return jnp.minimum(jnp.maximum(result, -reach), reach).astype(kind)


def gaussian_with(key, extent, spread, reach, cuts, heavy, held_as=jnp.bfloat16):
    array = spread * jax.random.normal(key, extent, jnp.float32)
    if cuts:
        array = array * block_levels(key, extent, cuts, -0.22, 0.18)
    return jnp.clip(spiked(array, jax.random.fold_in(key, 3), *heavy), -reach, reach).astype(held_as)


def setup_inputs(seed: int = 0) -> dict:
    key_of = jax.random.split(jax.random.key(seed), 23)
    return {
        "tokens": gaussian_with(key_of[0], (SEQUENCE_TOTAL, D), 1.0, 16.0, ((0, 4), (1, 64)), (1, 0, 64, 4.0)),
        "pre_gain": jnp.clip(1.0 + 0.18 * jax.random.normal(key_of[1], (D,), jnp.float32), 0.1, 1.9),
        "query_weight": gaussian(key_of[2], (D, HW), D ** -0.5, 0.125, ((0, 64), (1, 2))),
        "key_weight": gaussian(key_of[3], (D, HW), D ** -0.5, 0.125, ((0, 64), (1, 2))),
        "value_weight": gaussian(key_of[4], (D, HW), D ** -0.5, 0.125, ((0, 64), (1, 2))),
        "outgate_weight": gaussian(key_of[5], (D, HW), D ** -0.5, 0.125, ((0, 64), (1, 2))),
        "input_gate_weight": gaussian(key_of[6], (D, MEMORY_HEADS), D ** -0.5, 0.125),
        "forget_gate_weight": gaussian(key_of[7], (D, MEMORY_HEADS), D ** -0.5, 0.125),
        "cache_keys": gaussian(key_of[8], (SEQUENCE_TOTAL, FOLD_SPAN, HW), 1.0, 6.0, ((0, 256), (2, 2))),
        "cache_values": gaussian(key_of[9], (SEQUENCE_TOTAL, FOLD_SPAN, HW), 1.0, 6.0, ((0, 256), (2, 2))),
        "cache_input": draw_cache_input(jax.random.fold_in(key_of[22], 71), 0),
        "cache_forget": draw_cache_forget(jax.random.fold_in(key_of[22], 71), 0),
        "lengths": ragged_sizes(key_of[12], SEQUENCE_TOTAL, SEQUENCE_TOTAL * FOLD_SPAN * 2 // 5, FOLD_SPAN, 2).astype(jnp.int32),
        "state_matrix": gaussian(key_of[13], (SEQUENCE_TOTAL, MEMORY_HEADS, HEAD_DIM, HEAD_DIM), 1.0, 6.0, ((0, 256), (1, 2)), jnp.float32),
        "state_norm": gaussian(key_of[14], (SEQUENCE_TOTAL, MEMORY_HEADS, HEAD_DIM), 1.0, 6.0, ((0, 256), (1, 2)), jnp.float32),
        "state_max": draw_state_max(jax.random.fold_in(key_of[22], 71), 0),
        "head_gain": jnp.clip(1.0 + 0.18 * jax.random.normal(key_of[16], (HW,), jnp.float32), 0.1, 1.9),
        "out_weight": gaussian(key_of[17], (HW, D), (HW // 4) ** -0.5, 0.375, ((0, 2), (1, 64))),
        "mixer_gain": jnp.clip(1.0 + 0.18 * jax.random.normal(key_of[18], (D,), jnp.float32), 0.1, 1.9),
        "gate_weight": gaussian(key_of[19], (D, FF), D ** -0.5, 0.125, ((1, 128),)),
        "up_weight": gaussian(key_of[20], (D, FF), D ** -0.5, 0.125, ((1, 128),)),
        "down_weight": gaussian_with(key_of[21], (FF, D), (FF // 4) ** -0.5, 0.625, ((0, 128),), (0, 1, 128, 5.5)),
    }


EPS = 1e-06

def reference(tokens, pre_gain, query_weight, key_weight, value_weight, outgate_weight, input_gate_weight, forget_gate_weight, cache_keys, cache_values, cache_input, cache_forget, lengths, state_matrix, state_norm, state_max, head_gain, out_weight, mixer_gain, gate_weight, up_weight, down_weight):
    token_values = tokens.astype(jnp.float32)
    scale_first = lax.rsqrt(lax.optimization_barrier(jnp.mean(token_values * token_values, axis=1)) + EPS)[:, None]
    normed_first = (token_values * pre_gain[None, :]).astype(jnp.bfloat16)

    def project(weight):
        return scale_first * jnp.dot(normed_first, weight, preferred_element_type=jnp.float32)
    query = project(query_weight).astype(jnp.bfloat16)
    keys_new = project(key_weight).astype(jnp.bfloat16)
    values_new = project(value_weight).astype(jnp.bfloat16)
    outgate = project(outgate_weight).astype(jnp.bfloat16)
    in_gate = project(input_gate_weight)
    forget_new = jax.nn.log_sigmoid(project(forget_gate_weight))
    seq_count = tokens.shape[0]
    query_heads = query.astype(jnp.float32).reshape(seq_count, MEMORY_HEADS, HEAD_DIM) * HEAD_DIM ** (-0.5)
    key_heads = keys_new.astype(jnp.float32).reshape(seq_count, MEMORY_HEADS, HEAD_DIM)
    value_heads = values_new.astype(jnp.float32).reshape(seq_count, MEMORY_HEADS, HEAD_DIM)
    cached_keys = cache_keys.astype(jnp.float32).reshape(seq_count, FOLD_SPAN, MEMORY_HEADS, HEAD_DIM)
    cached_values = cache_values.astype(jnp.float32).reshape(seq_count, FOLD_SPAN, MEMORY_HEADS, HEAD_DIM)
    live_mask = (jnp.arange(FOLD_SPAN, dtype=jnp.int32)[None, :] < lengths[:, None])[:, :, None]
    forget_live = jnp.where(live_mask, cache_forget, jnp.float32(0.0))
    running = jnp.cumsum(forget_live, axis=1)
    total_log = running[:, -1, :] + forget_new
    weight_log = jnp.where(live_mask, total_log[:, None, :] - running + cache_input, -jnp.inf)
    state_log = total_log + state_max
    peak_log = jnp.maximum(jnp.maximum(state_log, in_gate), lax.optimization_barrier(jnp.max(weight_log, axis=1)))
    key_dots = jnp.einsum('bhd,blhd->blh', query_heads, cached_keys)
    block_scores = jnp.exp(weight_log - peak_log[:, None, :]) * key_dots
    self_score = jnp.exp(in_gate - peak_log) * lax.optimization_barrier(jnp.sum(query_heads * key_heads, axis=2))
    carried = jnp.exp(state_log - peak_log)
    block_weights = lax.optimization_barrier(block_scores.astype(jnp.bfloat16)).astype(jnp.float32)
    memory_read = jnp.einsum('bhvd,bhd->bhv', state_matrix, query_heads, precision=lax.Precision.HIGHEST)
    norm_read = jnp.einsum('bhd,bhd->bh', state_norm, query_heads, precision=lax.Precision.HIGHEST)
    numerator = carried[:, :, None] * memory_read + jnp.einsum('blh,blhd->bhd', block_weights, cached_values) + self_score[:, :, None] * value_heads
    denominator = carried * norm_read + lax.optimization_barrier(jnp.sum(block_scores, axis=1)) + self_score
    hidden = numerator / jnp.maximum(jnp.abs(denominator), 1.0)[:, :, None]
    mixed_heads = (hidden.reshape(seq_count, HW) * head_gain[None, :] * jax.nn.sigmoid(outgate.astype(jnp.float32))).astype(jnp.bfloat16)
    half_width = HW // N_TP
    mix_sum = jnp.zeros((seq_count, D), jnp.float32)
    for half_part in range(N_TP):
        piece_sum = jnp.dot(mixed_heads[:, half_part * half_width:(half_part + 1) * half_width], out_weight[half_part * half_width:(half_part + 1) * half_width], preferred_element_type=jnp.float32)
        mix_sum = mix_sum + lax.optimization_barrier(piece_sum.astype(jnp.bfloat16)).astype(jnp.float32)
    residual = (token_values + mix_sum).astype(jnp.bfloat16)
    residual_values = residual.astype(jnp.float32)
    scale_mid = lax.rsqrt(lax.optimization_barrier(jnp.mean(residual_values * residual_values, axis=1)) + EPS)[:, None]
    normed_mid = (residual_values * mixer_gain[None, :]).astype(jnp.bfloat16)
    gate_values = scale_mid * jnp.dot(normed_mid, gate_weight, preferred_element_type=jnp.float32)
    up_values = scale_mid * jnp.dot(normed_mid, up_weight, preferred_element_type=jnp.float32)
    hidden_units = (jax.nn.silu(gate_values) * up_values).astype(jnp.bfloat16)
    return (residual_values + jnp.dot(hidden_units, down_weight, preferred_element_type=jnp.float32)).astype(jnp.bfloat16)
```

```python
import functools

import jax
import jax.numpy as jnp
from jax import lax
from jax.experimental import pallas as pl
from jax.experimental.pallas import tpu as pltpu
from jax.sharding import PartitionSpec as P

EPS = 1e-06
MESH = pl.DeviceIdType.MESH
F32 = jnp.float32
BF16 = jnp.bfloat16
KINDS = 4
ROWS = 40
HIDDEN_PAD = 48


def ring_order(n):
    return sorted(range(1, n), key=lambda d: (-min(d, n - d), d))


def dot(a, b, ca=1, cb=0, precision=None):
    return lax.dot_general(
        a, b, (((ca,), (cb,)), ((), ())), preferred_element_type=F32, precision=precision
    )


def iota(shape, dim):
    return lax.broadcasted_iota(jnp.int32, shape, dim)


def kernel(
    n,
    tok_h,
    pre_h,
    qw_h,
    kw_h,
    vw_h,
    ow_h,
    ig_h,
    fg_h,
    ck_h,
    cv_h,
    ci_h,
    cf_h,
    len_h,
    sm_h,
    sn_h,
    smax_h,
    hg_h,
    mixw_h,
    mg_h,
    gw_h,
    uw_h,
    dw_h,
    out_ref,
    tok,
    pre,
    w4,
    gates,
    ck,
    cv,
    ci,
    cf,
    lens,
    state,
    sn,
    smax,
    hg,
    mixw,
    mg,
    gw,
    uw,
    dw,
    load_sem,
    p1,
    r1,
    q2f,
    q2b,
    r2,
    split,
    pick,
    mh,
    xs,
    xr,
    rbuf,
    rt,
    gu,
    dt,
    xo,
    xi,
    p5,
    p5b,
    r3,
    q4b,
    r4,
    s1,
    v1,
    s2,
    v2,
    s3,
    v3,
    s4,
    v4,
    s5,
    v5,
    s6,
    v6,
    s7,
    v7,
    s8,
    v8,
    s9,
    v9,
):
    kvs = n * n
    width = tok.shape[0]
    seqs = tok.shape[1]
    cols = w4.shape[2]
    blocks = cols // 128
    model = width * kvs
    dp = lax.axis_index("dp")
    kv = lax.axis_index("kv")
    tp = lax.axis_index("tp")
    z, y = kv // n, kv % n
    far = n - (n - 1) * tp
    near = 1 + (n - 1) * tp
    first = z + (y - z) * tp
    second = y + (z - y) * tp
    other = 1 - tp
    order = ring_order(n)

    def first_peer(d):
        return (dp, lax.rem(first + d, n) * far + second * near, tp)

    def second_peer(d):
        return (dp, first * far + lax.rem(second + d, n) * near, tp)

    sibling = (dp, kv, other)

    barrier = pltpu.get_barrier_semaphore()
    for d in range(1, n):
        pl.semaphore_signal(barrier, inc=1, device_id=first_peer(d), device_id_type=MESH)
        pl.semaphore_signal(barrier, inc=1, device_id=second_peer(d), device_id_type=MESH)
    pl.semaphore_signal(barrier, inc=1, device_id=sibling, device_id_type=MESH)

    loads = [
        (tok_h, tok),
        (pre_h, pre),
        (qw_h, w4.at[0]),
        (kw_h, w4.at[1]),
        (vw_h, w4.at[2]),
        (ow_h, w4.at[3]),
        (ig_h, gates.at[0]),
        (fg_h, gates.at[1]),
        (cf_h, cf),
        (ci_h, ci),
        (len_h, lens),
        (smax_h, smax),
        (sm_h, state),
        (sn_h, sn),
        (ck_h, ck),
        (cv_h, cv),
        (hg_h, hg),
        (mixw_h, mixw),
        (mg_h, mg),
        (gw_h, gw),
        (uw_h, uw),
        (dw_h, dw),
    ]
    copies = [pltpu.make_async_copy(a, b, load_sem.at[k]) for k, (a, b) in enumerate(loads)]
    for c in copies:
        c.start()
    for c in copies[:8]:
        c.wait()

    r = iota((seqs, seqs), 0)
    owner = (r // (2 * n)) * far + (r % n) * near
    perm = jnp.where(iota((seqs, seqs), 1) == owner * 2 + (r // n) % 2, 1.0, 0.0).astype(BF16)
    tokens = dot(perm, tok[...], 1, 1)
    squares = jnp.sum(tokens * tokens, axis=1, keepdims=True)
    normed = (tokens * pre[...]).astype(BF16)
    for k in range(KINDS):
        prod = dot(normed, w4[k]).astype(BF16)
        p1[:, :, k * cols : (k + 1) * cols] = prod.reshape(n, 2 * n, cols)
    lane0 = pl.multiple_of((kv // (128 // width)) * 128, 128)
    both = jnp.concatenate(
        [gates[0, :, pl.ds(lane0, 128)].astype(F32), gates[1, :, pl.ds(lane0, 128)].astype(F32)],
        axis=0,
    ).astype(BF16)
    at = (kv % (128 // width)) * width
    sel = jnp.where(iota((width, 128), 1) == iota((width, 128), 0) + at, 1.0, 0.0).astype(BF16)
    own_gates = dot(both, sel, 1, 1)
    own_gates = jnp.concatenate([own_gates, jnp.zeros((120, width), F32)], axis=0).astype(BF16)
    g = dot(normed, own_gates, 1, 1)
    g = jnp.where(iota((seqs, 128), 1) == 8, squares, g)
    p1[:, :, KINDS * cols :] = g.astype(BF16).reshape(n, 2 * n, 128)

    pl.semaphore_wait(barrier, 2 * (n - 1) + 1)

    def exchange(src, dst, send, recv, peer):
        made = {}
        for d in order:
            made[d] = pltpu.make_async_remote_copy(
                src_ref=src(d),
                dst_ref=dst(d),
                send_sem=send.at[d - 1],
                recv_sem=recv.at[d - 1],
                device_id=peer(d),
                device_id_type=MESH,
            )
            made[d].start()
        return made

    one = exchange(
        lambda d: p1.at[lax.rem(first + d, n)], lambda d: r1.at[d - 1], s1, v1, first_peer
    )

    for c in copies[8:]:
        c.wait()
    row64 = iota((8, ck.shape[1]), 0)
    lane64 = iota((8, ck.shape[1]), 1)
    zero4 = jnp.zeros((4, ck.shape[1]), F32)
    forget = jnp.concatenate([cf[0], cf[1], zero4], axis=0)
    gain_in = jnp.concatenate([ci[0], ci[1], zero4], axis=0)
    length = jnp.where(row64 < 2, lens[0], lens[1])
    live = lane64 < length
    forget = jnp.where(live, forget, 0.0)
    span = ck.shape[1]
    tri = jnp.where(iota((span, span), 0) <= iota((span, span), 1), 1.0, 0.0)
    running = dot(forget, tri, precision=lax.Precision.HIGHEST)
    run_last = jnp.sum(forget, axis=1, keepdims=True)
    base = jnp.where(live, run_last - running + gain_in, -jnp.inf)
    base = jnp.where(row64 < 4, base, 0.0)
    base_max = jnp.max(base, axis=1, keepdims=True)
    row1 = iota((8, 1), 0)
    state_top = jnp.where(
        row1 == 0,
        smax[0, 0],
        jnp.where(row1 == 1, smax[0, 1], jnp.where(row1 == 2, smax[1, 0], smax[1, 1])),
    )
    state_base = run_last + state_top
    for i in range(2):
        for h in range(2):
            whole = state[i, h]
            high = whole.astype(BF16)
            split[0, 2 * i + h] = high
            split[1, 2 * i + h] = (whole - high.astype(F32)).astype(BF16)
    size = sn.shape[2]
    zero_rows = jnp.zeros((4, size), F32)
    norm8 = jnp.concatenate([sn[0], sn[1], zero_rows], axis=0)
    halves = [hg[:, :size], hg[:, size:]]
    gain8 = jnp.concatenate(halves + halves + [zero_rows], axis=0)
    pr = iota((4 * seqs, 8 * kvs), 0)
    pc = iota((4 * seqs, 8 * kvs), 1)
    seq, hu = pr % seqs, pr // seqs
    target = (seq // 2) * 8 + (hu % 2) * 4 + (seq % 2) * 2 + hu // 2
    pick[...] = jnp.where(pc == target, 1.0, 0.0).astype(BF16)
    hidden_cols = gw.shape[0]
    gu[...] = jnp.zeros_like(gu)
    gu[:hidden_cols, :] = (gw[...].astype(F32) * mg[...]).astype(BF16)
    gu[HIDDEN_PAD : HIDDEN_PAD + hidden_cols, :] = (uw[...].astype(F32) * mg[...]).astype(BF16)
    group = 128 // width

    def arrange(b, carry):
        block = dw[:, pl.ds(pl.multiple_of(b * 128, 128), 128)].astype(F32)
        block = jnp.concatenate([block, jnp.zeros((HIDDEN_PAD - hidden_cols, 128), F32)], axis=0)
        block = block.T.astype(BF16)
        for k in range(group):
            at_kv = b * group + k
            mirrored = (at_kv % n) * n + at_kv // n
            half = width // 2
            dt[0, at_kv] = block[k * width : k * width + half]
            dt[1, mirrored] = block[k * width + half : (k + 1) * width]
        return carry

    lax.fori_loop(0, kvs // group, arrange, 0)

    own = p1[first].astype(F32)
    for d in order:
        one[d].wait_recv()
    for d in order:
        own = own + r1[d - 1].astype(F32)
    q2f[...] = jnp.zeros_like(q2f)
    for i in range(2):
        part = own[i * n : (i + 1) * n]
        for c in range(KINDS * blocks):
            kind, h, u = c // blocks, (c % blocks) // 2, c % 2
            q2f[pl.ds(kind * 8 + u * 4 + i * 2 + h, n, stride=ROWS), :] = part[
                :, c * 128 : (c + 1) * 128
            ]
        for h in range(2):
            q2f[pl.ds(32 + i * 2 + h, n, stride=ROWS), :] = part[:, KINDS * cols :]
    q2b[...] = q2f[...].reshape(n, ROWS, 128).astype(BF16)
    two = exchange(
        lambda d: q2b.at[lax.rem(second + d, n)], lambda d: r2.at[d - 1], s2, v2, second_peer
    )
    mine = q2f[pl.ds(pl.multiple_of(second * ROWS, 8), ROWS), :]
    for d in order:
        two[d].wait_recv()
    for d in order:
        mine = mine + r2[d - 1].astype(F32)

    def heads(kind):
        a = mine[kind * 8 : kind * 8 + 4]
        b = mine[kind * 8 + 4 : kind * 8 + 8]
        return jnp.concatenate([jnp.concatenate([a, b], axis=1), zero_rows], axis=0)

    gate8 = mine[32:40]
    lane = iota((8, 128), 1)
    row = iota((8, 128), 0)
    square = jnp.sum(jnp.where(lane == 8, gate8, 0.0), axis=1, keepdims=True)
    in_sum = jnp.sum(jnp.where(lane == 2 * tp + row % 2, gate8, 0.0), axis=1, keepdims=True)
    fg_sum = jnp.sum(jnp.where(lane == 4 + 2 * tp + row % 2, gate8, 0.0), axis=1, keepdims=True)
    scale = lax.rsqrt(square / model + EPS)
    query = (scale * heads(0)).astype(BF16).astype(F32)
    key_new = (scale * heads(1)).astype(BF16).astype(F32)
    value_new = (scale * heads(2)).astype(BF16).astype(F32)
    outgate = (scale * heads(3)).astype(BF16).astype(F32)
    in_gate = scale * in_sum
    fg = scale * fg_sum
    forget_new = jnp.minimum(fg, 0.0) - jnp.log1p(jnp.exp(-jnp.abs(fg)))
    weight_log = base + forget_new
    state_log = state_base + forget_new
    peak = jnp.maximum(jnp.maximum(state_log, in_gate), base_max + forget_new)
    query = query * (size**-0.5)
    rows = iota((8, size), 0)
    alone = [jnp.where(rows == k, query, 0.0) for k in range(4)]
    dots = dot(jnp.concatenate(alone[0:2], axis=1).astype(BF16), ck[0], 1, 1)
    dots = dots + dot(jnp.concatenate(alone[2:4], axis=1).astype(BF16), ck[1], 1, 1)
    scores = jnp.exp(weight_log - peak) * dots
    self_score = jnp.exp(in_gate - peak) * jnp.sum(query * key_new, axis=1, keepdims=True)
    carried = jnp.exp(state_log - peak)
    read = dot(alone[0].astype(BF16), split[0, 0], 1, 1)
    read = read + dot(alone[0].astype(BF16), split[1, 0], 1, 1)
    for k in range(1, 4):
        read = read + dot(alone[k].astype(BF16), split[0, k], 1, 1)
        read = read + dot(alone[k].astype(BF16), split[1, k], 1, 1)
    norm_read = jnp.sum(norm8 * query, axis=1, keepdims=True)
    values = dot(jnp.where(row64 < 2, scores, 0.0).astype(BF16), cv[0])
    values = values + dot(jnp.where(row64 >= 2, scores, 0.0).astype(BF16), cv[1])
    values = jnp.where(rows % 2 == 0, values[:, :size], values[:, size:])
    numerator = carried * read + values + self_score * value_new
    denominator = carried * norm_read + jnp.sum(scores, axis=1, keepdims=True) + self_score
    hidden = numerator / jnp.maximum(jnp.abs(denominator), 1.0)
    mixed = hidden * gain8 * jax.nn.sigmoid(outgate)
    mh[kv] = jnp.concatenate([mixed[:4, :128], mixed[:4, 128:]], axis=0).astype(BF16)

    stride = kvs // 2 + 5 if kvs > 8 else 1

    def spread(j, carry):
        peer = lax.rem(kv + lax.rem(j * stride, kvs), kvs)
        pltpu.make_async_remote_copy(
            src_ref=mh.at[kv],
            dst_ref=mh.at[kv],
            send_sem=s3,
            recv_sem=v3,
            device_id=(dp, peer, tp),
            device_id_type=MESH,
        ).start()
        return carry

    lax.fori_loop(1, kvs, spread, 0)
    all_mh = pltpu.make_async_remote_copy(
        src_ref=mh.at[pl.ds(0, kvs - 1)],
        dst_ref=mh.at[pl.ds(0, kvs - 1)],
        send_sem=s3,
        recv_sem=v3,
        device_id=sibling,
        device_id_type=MESH,
    )
    all_mh.wait_recv()

    flat = mh[...].astype(F32).reshape(8 * kvs, 128).astype(BF16)
    picked = dot(pick[...], flat).astype(BF16)
    mix = dot(mixw[:, :128], picked[:seqs], 1, 1)
    for k in range(1, 4):
        mix = mix + dot(mixw[:, k * 128 : (k + 1) * 128], picked[k * seqs : (k + 1) * seqs], 1, 1)
    mix = mix.astype(BF16)
    xs[...] = mix
    swap = pltpu.make_async_remote_copy(
        src_ref=xs,
        dst_ref=xr,
        send_sem=s4,
        recv_sem=v4,
        device_id=sibling,
        device_id_type=MESH,
    )
    swap.start()
    swap.wait_recv()
    total = tok[...].astype(F32) + (mix.astype(F32) + xr[...].astype(F32))
    rbuf[...] = total.astype(BF16).reshape(2, width // 2, seqs)
    rt[kv, tp] = rbuf[tp]

    for dz in order + [0]:

        def send_row(dy, carry, dz=dz):
            peer = lax.rem(z + dz, n) * n + lax.rem(y + dy, n)
            pltpu.make_async_remote_copy(
                src_ref=rbuf.at[tp],
                dst_ref=rt.at[kv, tp],
                send_sem=s5,
                recv_sem=v5.at[dz],
                device_id=(dp, peer, tp),
                device_id_type=MESH,
            ).start()
            return carry

        lax.fori_loop(1 if dz == 0 else 0, n, send_row, 0)

    forward = {}
    for dz in order + [0]:
        count = n - 1 if dz == 0 else n
        pltpu.make_async_remote_copy(
            src_ref=rt.at[pl.ds(0, count), 0],
            dst_ref=rt.at[pl.ds(0, count), 0],
            send_sem=s5,
            recv_sem=v5.at[dz],
            device_id=sibling,
            device_id_type=MESH,
        ).wait_recv()
        source = lax.rem(z + n - dz, n) * n
        forward[dz] = pltpu.make_async_remote_copy(
            src_ref=rt.at[pl.ds(source, n), tp],
            dst_ref=rt.at[pl.ds(source, n), tp],
            send_sem=s6.at[dz],
            recv_sem=v6.at[dz],
            device_id=sibling,
            device_id_type=MESH,
        )
        forward[dz].start()
    for dz in order + [0]:
        forward[dz].wait_recv()

    residual = rt[...].reshape(model, seqs)
    wide = residual.astype(F32)
    power = jnp.sum(wide * wide, axis=0, keepdims=True)
    acc = dot(gu[...], residual)
    scale_mid = lax.rsqrt(power / model + EPS)
    gate = scale_mid * acc[:HIDDEN_PAD]
    up = scale_mid * acc[HIDDEN_PAD:]
    units = (gate * jax.nn.sigmoid(gate) * up).astype(BF16)

    half = width // 2
    other_first = y + (z - y) * tp
    swaps = []
    steps = order + [0]
    for k, d in enumerate(steps):
        at_f = lax.rem(other_first + d, n)
        rows_of = dt[other, pl.ds(at_f * n, n)].reshape(n * half, HIDDEN_PAD)
        xo[k] = dot(rows_of, units).astype(BF16)
        c = pltpu.make_async_remote_copy(
            src_ref=xo.at[k],
            dst_ref=xi.at[k],
            send_sem=s7.at[k],
            recv_sem=v7.at[k],
            device_id=sibling,
            device_id_type=MESH,
        )
        c.start()
        swaps.append(c)
    for k, d in enumerate(steps):
        at_f = lax.rem(first + d, n)
        rows_of = dt[tp, pl.ds(at_f * n, n)].reshape(n * half, HIDDEN_PAD)
        p5[k] = dot(rows_of, units)
    three = {}
    for k, d in enumerate(steps):
        swaps[k].wait_recv()
        both = p5[k] + xi[k].astype(F32)
        if d == 0:
            own = both
            continue
        p5b[k] = both.astype(BF16)
        three[d] = pltpu.make_async_remote_copy(
            src_ref=p5b.at[k],
            dst_ref=r3.at[d - 1],
            send_sem=s8.at[d - 1],
            recv_sem=v8.at[d - 1],
            device_id=first_peer(d),
            device_id_type=MESH,
        )
        three[d].start()
    for d in order:
        three[d].wait_recv()
    for d in order:
        own = own + r3[d - 1].astype(F32)
    own = own.reshape(n, half, seqs)
    p5[0] = own.reshape(n * half, seqs)
    q4b[...] = own.astype(BF16)
    four = exchange(
        lambda d: q4b.at[lax.rem(second + d, n)], lambda d: r4.at[d - 1], s9, v9, second_peer
    )
    last = p5[0, pl.ds(pl.multiple_of(second * half, half), half), :]
    last = last + rt[kv, tp].astype(F32)
    for d in order:
        four[d].wait_recv()
    for d in order:
        last = last + r4[d - 1].astype(F32)
    out_ref[...] = last.astype(BF16)

    for made in (one, two, three, four, forward):
        for c in made.values():
            c.wait_send()
    for c in swaps:
        c.wait_send()
    swap.wait_send()
    all_mh.wait_send()
    pltpu.make_async_remote_copy(
        src_ref=rt.at[pl.ds(0, kvs - 1), 0],
        dst_ref=rt.at[pl.ds(0, kvs - 1), 0],
        send_sem=s5,
        recv_sem=v5.at[0],
        device_id=sibling,
        device_id_type=MESH,
    ).wait_send()


def per_device(n, *args):
    (tokens, pre, qw, kw, vw, ow, ig, fg, ck, cv, ci, cf, lens, sm, sn, smax) = args[:16]
    hg, mixw, mg, gw, uw, dw = args[16:]
    operands = (
        tokens.T,
        pre.reshape(1, -1),
        qw,
        kw,
        vw,
        ow,
        ig.T,
        fg.T,
        ck,
        cv,
        ci.transpose(0, 2, 1),
        cf.transpose(0, 2, 1),
        lens,
        sm,
        sn,
        smax,
        hg.reshape(1, -1),
        mixw.T,
        mg.reshape(1, -1),
        gw.T,
        uw.T,
        dw,
    )
    seqs, width = tokens.shape
    cols = qw.shape[1]
    kvs = n * n
    model = width * kvs
    span, size = ck.shape[1], sn.shape[2]
    wide = KINDS * cols + 128
    half = width // 2
    dma = pltpu.SemaphoreType.DMA
    vmem = pltpu.VMEM
    scratch = [
        vmem((width, seqs), BF16),
        vmem((1, width), F32),
        vmem((KINDS, width, cols), BF16),
        vmem((2, 4, model), BF16),
        vmem((2, span, cols), BF16),
        vmem((2, span, cols), BF16),
        vmem((2, 2, span), F32),
        vmem((2, 2, span), F32),
        pltpu.SMEM((2,), jnp.int32),
        vmem((2, 2, size, size), F32),
        vmem((2, 2, size), F32),
        pltpu.SMEM((2, 2), F32),
        vmem((1, cols), F32),
        vmem((width, cols), BF16),
        vmem((1, model), F32),
        vmem((gw.shape[1], model), BF16),
        vmem((gw.shape[1], model), BF16),
        vmem((gw.shape[1], model), BF16),
        dma((22,)),
        vmem((n, 2 * n, wide), BF16),
        vmem((n - 1, 2 * n, wide), BF16),
        vmem((n * ROWS, 128), F32),
        vmem((n, ROWS, 128), BF16),
        vmem((n - 1, ROWS, 128), BF16),
        vmem((2, 4, size, size), BF16),
        vmem((4 * seqs, 8 * kvs), BF16),
        vmem((kvs, 8, 128), BF16),
        vmem((width, seqs), BF16),
        vmem((width, seqs), BF16),
        vmem((2, half, seqs), BF16),
        vmem((kvs, 2, half, seqs), BF16),
        vmem((2 * HIDDEN_PAD, model), BF16),
        vmem((2, kvs, half, HIDDEN_PAD), BF16),
        vmem((n, n * half, seqs), BF16),
        vmem((n, n * half, seqs), BF16),
        vmem((n, n * half, seqs), F32),
        vmem((n, n * half, seqs), BF16),
        vmem((n - 1, n * half, seqs), BF16),
        vmem((n, half, seqs), BF16),
        vmem((n - 1, half, seqs), BF16),
        dma((n - 1,)),
        dma((n - 1,)),
        dma((n - 1,)),
        dma((n - 1,)),
        dma,
        dma,
        dma,
        dma,
        dma,
        dma((n,)),
        dma((n,)),
        dma((n,)),
        dma((n,)),
        dma((n,)),
        dma((n - 1,)),
        dma((n - 1,)),
        dma((n - 1,)),
        dma((n - 1,)),
    ]
    out = pl.pallas_call(
        functools.partial(kernel, n),
        out_shape=jax.ShapeDtypeStruct((half, seqs), BF16),
        in_specs=[pl.BlockSpec(memory_space=pl.ANY)] * len(operands),
        out_specs=pl.BlockSpec(memory_space=pltpu.VMEM),
        scratch_shapes=scratch,
        compiler_params=pltpu.CompilerParams(
            collective_id=0, has_side_effects=True, vmem_limit_bytes=62 * 1024 * 1024
        ),
        name="layer",
    )(*operands)
    return out.T


def solution(mesh):
    n = round(mesh.shape["kv"] ** 0.5)
    seq = ("dp", "kv")
    return jax.shard_map(
        functools.partial(per_device, n),
        mesh=mesh,
        in_specs=(
            P("dp", "kv"),
            P("kv"),
            P("kv", "tp"),
            P("kv", "tp"),
            P("kv", "tp"),
            P("kv", "tp"),
            P(),
            P(),
            P(seq, None, "tp"),
            P(seq, None, "tp"),
            P(seq, None, "tp"),
            P(seq, None, "tp"),
            P(seq),
            P(seq, "tp", None, None),
            P(seq, "tp", None),
            P(seq, "tp"),
            P("tp"),
            P("tp", "kv"),
            P(),
            P(None, ("kv", "tp")),
            P(None, ("kv", "tp")),
            P(("kv", "tp"), None),
        ),
        out_specs=P("dp", ("kv", "tp")),
        check_vma=False,
    )
```

```python
import functools

import jax
import jax.numpy as jnp
from jax import lax
from jax.experimental import pallas as pl
from jax.experimental.pallas import tpu as pltpu
from jax.sharding import PartitionSpec as P

EPS = 1e-06
MESH = pl.DeviceIdType.MESH
F32 = jnp.float32
BF16 = jnp.bfloat16
KINDS = 4
ROWS = 40
HIDDEN_PAD = 48
LAG = 3


def ring_order(n):
    return sorted(range(1, n), key=lambda d: (-min(d, n - d), d))


def plane_order(n):
    def hops(d):
        return min(d, n - d)

    pairs = [(dz, dy) for dz in range(n) for dy in range(n) if dz or dy]
    return sorted(pairs, key=lambda p: (-hops(p[0]) - hops(p[1]), (3 * p[0] + 5 * p[1]) % n))


def dot(a, b, ca=1, cb=0, precision=None):
    return lax.dot_general(
        a, b, (((ca,), (cb,)), ((), ())), preferred_element_type=F32, precision=precision
    )


def iota(shape, dim):
    return lax.broadcasted_iota(jnp.int32, shape, dim)


def kernel(
    n,
    tok_h,
    pre_h,
    qw_h,
    kw_h,
    vw_h,
    ow_h,
    ig_h,
    fg_h,
    ck_h,
    cv_h,
    ci_h,
    cf_h,
    len_h,
    sm_h,
    sn_h,
    smax_h,
    hg_h,
    mixw_h,
    mg_h,
    gw_h,
    uw_h,
    dw_h,
    out_ref,
    tok,
    pre,
    w4,
    gates,
    ck,
    cv,
    ci,
    cf,
    lens,
    state,
    sn,
    smax,
    hg,
    mixw,
    mg,
    gw,
    uw,
    dw,
    load_sem,
    p1,
    r1,
    q2f,
    q2b,
    r2,
    split,
    pick,
    mh,
    xs,
    xr,
    wg,
    tg,
    rbuf,
    rt,
    gu,
    dt,
    xo,
    xi,
    p5,
    p5b,
    r3,
    q4b,
    r4,
    s1,
    v1,
    s2,
    v2,
    s3,
    v3,
    s4,
    v4,
    s5,
    v5,
    s6,
    v6,
    s7,
    v7,
    s8,
    v8,
    s9,
    v9,
    sw,
    vw,
    st,
    vt,
):
    kvs = n * n
    width = tok.shape[0]
    seqs = tok.shape[1]
    cols = w4.shape[2]
    blocks = cols // 128
    model = width * kvs
    dp = lax.axis_index("dp")
    kv = lax.axis_index("kv")
    tp = lax.axis_index("tp")
    z, y = kv // n, kv % n
    far = n - (n - 1) * tp
    near = 1 + (n - 1) * tp
    first = z + (y - z) * tp
    second = y + (z - y) * tp
    other = 1 - tp
    order = ring_order(n)

    def first_peer(d):
        return (dp, lax.rem(first + d, n) * far + second * near, tp)

    def second_peer(d):
        return (dp, first * far + lax.rem(second + d, n) * near, tp)

    sibling = (dp, kv, other)

    barrier = pltpu.get_barrier_semaphore()
    for d in range(1, n):
        pl.semaphore_signal(barrier, inc=1, device_id=first_peer(d), device_id_type=MESH)
        pl.semaphore_signal(barrier, inc=1, device_id=second_peer(d), device_id_type=MESH)
    pl.semaphore_signal(barrier, inc=1, device_id=sibling, device_id_type=MESH)

    loads = [
        (tok_h, tok),
        (pre_h, pre),
        (qw_h, w4.at[0]),
        (kw_h, w4.at[1]),
        (vw_h, w4.at[2]),
        (ow_h, w4.at[3]),
        (ig_h, gates.at[0]),
        (fg_h, gates.at[1]),
        (cf_h, cf),
        (ci_h, ci),
        (len_h, lens),
        (smax_h, smax),
        (sm_h, state),
        (sn_h, sn),
        (ck_h, ck),
        (cv_h, cv),
        (hg_h, hg),
        (mixw_h, mixw),
        (mg_h, mg),
        (gw_h, gw),
        (uw_h, uw),
        (dw_h, dw),
    ]
    copies = [pltpu.make_async_copy(a, b, load_sem.at[k]) for k, (a, b) in enumerate(loads)]
    for c in copies:
        c.start()
    for c in copies[:8]:
        c.wait()

    r = iota((seqs, seqs), 0)
    owner = (r // (2 * n)) * far + (r % n) * near
    perm = jnp.where(iota((seqs, seqs), 1) == owner * 2 + (r // n) % 2, 1.0, 0.0).astype(BF16)
    tokens = dot(perm, tok[...], 1, 1)
    squares = jnp.sum(tokens * tokens, axis=1, keepdims=True)
    normed = (tokens * pre[...]).astype(BF16)
    for k in range(KINDS):
        prod = dot(normed, w4[k]).astype(BF16)
        p1[:, :, k * cols : (k + 1) * cols] = prod.reshape(n, 2 * n, cols)
    lane0 = pl.multiple_of((kv // (128 // width)) * 128, 128)
    both = jnp.concatenate(
        [gates[0, :, pl.ds(lane0, 128)].astype(F32), gates[1, :, pl.ds(lane0, 128)].astype(F32)],
        axis=0,
    ).astype(BF16)
    at = (kv % (128 // width)) * width
    sel = jnp.where(iota((width, 128), 1) == iota((width, 128), 0) + at, 1.0, 0.0).astype(BF16)
    own_gates = dot(both, sel, 1, 1)
    own_gates = jnp.concatenate([own_gates, jnp.zeros((120, width), F32)], axis=0).astype(BF16)
    g = dot(normed, own_gates, 1, 1)
    g = jnp.where(iota((seqs, 128), 1) == 8, squares, g)
    p1[:, :, KINDS * cols :] = g.astype(BF16).reshape(n, 2 * n, 128)

    pl.semaphore_wait(barrier, 2 * (n - 1) + 1)

    def exchange(src, dst, send, recv, peer):
        made = {}
        for d in order:
            made[d] = pltpu.make_async_remote_copy(
                src_ref=src(d),
                dst_ref=dst(d),
                send_sem=send.at[d - 1],
                recv_sem=recv.at[d - 1],
                device_id=peer(d),
                device_id_type=MESH,
            )
            made[d].start()
        return made

    one = exchange(
        lambda d: p1.at[lax.rem(first + d, n)], lambda d: r1.at[d - 1], s1, v1, first_peer
    )

    for c in copies[8:]:
        c.wait()
    row64 = iota((8, ck.shape[1]), 0)
    lane64 = iota((8, ck.shape[1]), 1)
    zero4 = jnp.zeros((4, ck.shape[1]), F32)
    forget = jnp.concatenate([cf[0], cf[1], zero4], axis=0)
    gain_in = jnp.concatenate([ci[0], ci[1], zero4], axis=0)
    length = jnp.where(row64 < 2, lens[0], lens[1])
    live = lane64 < length
    forget = jnp.where(live, forget, 0.0)
    span = ck.shape[1]
    tri = jnp.where(iota((span, span), 0) <= iota((span, span), 1), 1.0, 0.0)
    running = dot(forget, tri, precision=lax.Precision.HIGHEST)
    run_last = jnp.sum(forget, axis=1, keepdims=True)
    base = jnp.where(live, run_last - running + gain_in, -jnp.inf)
    base = jnp.where(row64 < 4, base, 0.0)
    base_max = jnp.max(base, axis=1, keepdims=True)
    row1 = iota((8, 1), 0)
    state_top = jnp.where(
        row1 == 0,
        smax[0, 0],
        jnp.where(row1 == 1, smax[0, 1], jnp.where(row1 == 2, smax[1, 0], smax[1, 1])),
    )
    state_base = run_last + state_top
    for i in range(2):
        for h in range(2):
            whole = state[i, h]
            high = whole.astype(BF16)
            split[0, 2 * i + h] = high
            split[1, 2 * i + h] = (whole - high.astype(F32)).astype(BF16)
    size = sn.shape[2]
    zero_rows = jnp.zeros((4, size), F32)
    norm8 = jnp.concatenate([sn[0], sn[1], zero_rows], axis=0)
    halves = [hg[:, :size], hg[:, size:]]
    gain8 = jnp.concatenate(halves + halves + [zero_rows], axis=0)
    pr = iota((4 * seqs, 8 * kvs), 0)
    pc = iota((4 * seqs, 8 * kvs), 1)
    seq, hu = pr % seqs, pr // seqs
    target = (seq // 2) * 8 + (hu % 2) * 4 + (seq % 2) * 2 + hu // 2
    pick[...] = jnp.where(pc == target, 1.0, 0.0).astype(BF16)
    hidden_cols = gw.shape[0]
    gu[...] = jnp.zeros_like(gu)
    gu[:hidden_cols, :] = (gw[...].astype(F32) * mg[...]).astype(BF16)
    gu[HIDDEN_PAD : HIDDEN_PAD + hidden_cols, :] = (uw[...].astype(F32) * mg[...]).astype(BF16)
    group = 128 // width

    def arrange(b, carry):
        block = dw[:, pl.ds(pl.multiple_of(b * 128, 128), 128)].astype(F32)
        block = jnp.concatenate([block, jnp.zeros((HIDDEN_PAD - hidden_cols, 128), F32)], axis=0)
        block = block.T.astype(BF16)
        for k in range(group):
            at_kv = b * group + k
            mirrored = (at_kv % n) * n + at_kv // n
            half = width // 2
            dt[0, at_kv] = block[k * width : k * width + half]
            dt[1, mirrored] = block[k * width + half : (k + 1) * width]
        return carry

    lax.fori_loop(0, kvs // group, arrange, 0)

    own = p1[first].astype(F32)
    for d in order:
        one[d].wait_recv()
    for d in order:
        own = own + r1[d - 1].astype(F32)
    q2f[...] = jnp.zeros_like(q2f)
    for i in range(2):
        part = own[i * n : (i + 1) * n]
        for c in range(KINDS * blocks):
            kind, h, u = c // blocks, (c % blocks) // 2, c % 2
            q2f[pl.ds(kind * 8 + u * 4 + i * 2 + h, n, stride=ROWS), :] = part[
                :, c * 128 : (c + 1) * 128
            ]
        for h in range(2):
            q2f[pl.ds(32 + i * 2 + h, n, stride=ROWS), :] = part[:, KINDS * cols :]
    q2b[...] = q2f[...].reshape(n, ROWS, 128).astype(BF16)
    two = exchange(
        lambda d: q2b.at[lax.rem(second + d, n)], lambda d: r2.at[d - 1], s2, v2, second_peer
    )
    half = width // 2
    axes = ((0, y, lambda d: z * n + lax.rem(y + d, n)), (1, z, lambda d: lax.rem(z + d, n) * n + y))
    for u, place, peer in axes:
        for d in order:
            pltpu.make_async_remote_copy(
                src_ref=mixw.at[pl.ds(u * half, half)],
                dst_ref=wg.at[u, place],
                send_sem=sw,
                recv_sem=vw,
                device_id=(dp, peer(d), tp),
                device_id_type=MESH,
            ).start()
        wg[u, place] = mixw[u * half : (u + 1) * half, :]
    own_rows = pl.ds(pl.multiple_of(tp * half, half), half)
    for d in order:
        pltpu.make_async_remote_copy(
            src_ref=tok.at[own_rows],
            dst_ref=tg.at[second],
            send_sem=st,
            recv_sem=vt,
            device_id=second_peer(d),
            device_id_type=MESH,
        ).start()
    tg[second] = tok[own_rows, :]
    all_wg = pltpu.make_async_remote_copy(
        src_ref=wg.at[:, pl.ds(0, n - 1)],
        dst_ref=wg.at[:, pl.ds(0, n - 1)],
        send_sem=sw,
        recv_sem=vw,
        device_id=sibling,
        device_id_type=MESH,
    )
    all_tg = pltpu.make_async_remote_copy(
        src_ref=tg.at[pl.ds(0, n - 1)],
        dst_ref=tg.at[pl.ds(0, n - 1)],
        send_sem=st,
        recv_sem=vt,
        device_id=sibling,
        device_id_type=MESH,
    )
    mine = q2f[pl.ds(pl.multiple_of(second * ROWS, 8), ROWS), :]
    for d in order:
        two[d].wait_recv()
    for d in order:
        mine = mine + r2[d - 1].astype(F32)

    def heads(kind):
        a = mine[kind * 8 : kind * 8 + 4]
        b = mine[kind * 8 + 4 : kind * 8 + 8]
        return jnp.concatenate([jnp.concatenate([a, b], axis=1), zero_rows], axis=0)

    gate8 = mine[32:40]
    lane = iota((8, 128), 1)
    row = iota((8, 128), 0)
    square = jnp.sum(jnp.where(lane == 8, gate8, 0.0), axis=1, keepdims=True)
    in_sum = jnp.sum(jnp.where(lane == 2 * tp + row % 2, gate8, 0.0), axis=1, keepdims=True)
    fg_sum = jnp.sum(jnp.where(lane == 4 + 2 * tp + row % 2, gate8, 0.0), axis=1, keepdims=True)
    scale = lax.rsqrt(square / model + EPS)
    query = (scale * heads(0)).astype(BF16).astype(F32)
    key_new = (scale * heads(1)).astype(BF16).astype(F32)
    value_new = (scale * heads(2)).astype(BF16).astype(F32)
    outgate = (scale * heads(3)).astype(BF16).astype(F32)
    in_gate = scale * in_sum
    fg = scale * fg_sum
    forget_new = jnp.minimum(fg, 0.0) - jnp.log1p(jnp.exp(-jnp.abs(fg)))
    weight_log = base + forget_new
    state_log = state_base + forget_new
    peak = jnp.maximum(jnp.maximum(state_log, in_gate), base_max + forget_new)
    query = query * (size**-0.5)
    rows = iota((8, size), 0)
    alone = [jnp.where(rows == k, query, 0.0) for k in range(4)]
    dots = dot(jnp.concatenate(alone[0:2], axis=1).astype(BF16), ck[0], 1, 1)
    dots = dots + dot(jnp.concatenate(alone[2:4], axis=1).astype(BF16), ck[1], 1, 1)
    scores = jnp.exp(weight_log - peak) * dots
    self_score = jnp.exp(in_gate - peak) * jnp.sum(query * key_new, axis=1, keepdims=True)
    carried = jnp.exp(state_log - peak)
    read = dot(alone[0].astype(BF16), split[0, 0], 1, 1)
    read = read + dot(alone[0].astype(BF16), split[1, 0], 1, 1)
    for k in range(1, 4):
        read = read + dot(alone[k].astype(BF16), split[0, k], 1, 1)
        read = read + dot(alone[k].astype(BF16), split[1, k], 1, 1)
    norm_read = jnp.sum(norm8 * query, axis=1, keepdims=True)
    values = dot(jnp.where(row64 < 2, scores, 0.0).astype(BF16), cv[0])
    values = values + dot(jnp.where(row64 >= 2, scores, 0.0).astype(BF16), cv[1])
    values = jnp.where(rows % 2 == 0, values[:, :size], values[:, size:])
    numerator = carried * read + values + self_score * value_new
    denominator = carried * norm_read + jnp.sum(scores, axis=1, keepdims=True) + self_score
    hidden = numerator / jnp.maximum(jnp.abs(denominator), 1.0)
    mixed = hidden * gain8 * jax.nn.sigmoid(outgate)
    mh[kv] = jnp.concatenate([mixed[:4, :128], mixed[:4, 128:]], axis=0).astype(BF16)

    for dz, dy in plane_order(n):
        pltpu.make_async_remote_copy(
            src_ref=mh.at[kv],
            dst_ref=mh.at[kv],
            send_sem=s3,
            recv_sem=v3,
            device_id=(dp, lax.rem(z + dz, n) * n + lax.rem(y + dy, n), tp),
            device_id_type=MESH,
        ).start()
    all_mh = pltpu.make_async_remote_copy(
        src_ref=mh.at[pl.ds(0, kvs - 1)],
        dst_ref=mh.at[pl.ds(0, kvs - 1)],
        send_sem=s3,
        recv_sem=v3,
        device_id=sibling,
        device_id_type=MESH,
    )
    all_wg.wait_recv()
    all_tg.wait_recv()
    all_mh.wait_recv()

    flat = mh[...].astype(F32).reshape(8 * kvs, 128).astype(BF16)
    picked = dot(pick[...], flat).astype(BF16)

    def project(u):
        w = wg[u].reshape(n * half, cols)
        total = dot(w[:, :128], picked[:seqs], 1, 1)
        for k in range(1, 4):
            block = picked[k * seqs : (k + 1) * seqs]
            total = total + dot(w[:, k * 128 : (k + 1) * 128], block, 1, 1)
        return total.astype(BF16)

    xs[...] = project(other)
    swap = pltpu.make_async_remote_copy(
        src_ref=xs,
        dst_ref=xr,
        send_sem=s4,
        recv_sem=v4,
        device_id=sibling,
        device_id_type=MESH,
    )
    swap.start()
    mix = project(tp)
    swap.wait_recv()
    total = tg[...].reshape(n * half, seqs).astype(F32) + (mix.astype(F32) + xr[...].astype(F32))
    rbuf[...] = total.astype(BF16).reshape(n, half, seqs)

    def gather(u):
        def rows(f):
            return rt.at[f, :, 0] if u == 0 else rt.at[:, f, 1]

        made = exchange(lambda d: rbuf, lambda d: rows(first), s5, v5, first_peer)
        if u == 0:
            rt[z, :, 0] = rbuf[...]
        else:
            rt[:, y, 1] = rbuf[...]
        for d in [0] + order[::-1]:
            if d:
                made[d].wait_recv()
            source = lax.rem(first + n - d, n)
            pltpu.make_async_remote_copy(
                src_ref=rows(source),
                dst_ref=rows(source),
                send_sem=s6.at[d],
                recv_sem=v6.at[d],
                device_id=sibling,
                device_id_type=MESH,
            ).start()

    @pl.when(tp == 0)
    def _():
        gather(0)

    @pl.when(tp == 1)
    def _():
        gather(1)

    def block_copy(send, recv):
        return pltpu.make_async_remote_copy(
            src_ref=rbuf,
            dst_ref=rt.at[0, :, 0],
            send_sem=send,
            recv_sem=recv,
            device_id=sibling,
            device_id_type=MESH,
        )

    for d in range(n):
        block_copy(s6.at[d], v6.at[d]).wait_recv()

    residual = rt[...].reshape(model, seqs)
    wide = residual.astype(F32)
    power = jnp.sum(wide * wide, axis=0, keepdims=True)
    acc = dot(gu[...], residual)
    scale_mid = lax.rsqrt(power / model + EPS)
    gate = scale_mid * acc[:HIDDEN_PAD]
    up = scale_mid * acc[HIDDEN_PAD:]
    units = (gate * jax.nn.sigmoid(gate) * up).astype(BF16)

    other_first = y + (z - y) * tp
    swaps = []
    steps = order + [0]
    three = {}

    def finish(k):
        swaps[k].wait_recv()
        both = p5[k] + xi[k].astype(F32)
        d = steps[k]
        if d == 0:
            return both
        p5b[k] = both.astype(BF16)
        three[d] = pltpu.make_async_remote_copy(
            src_ref=p5b.at[k],
            dst_ref=r3.at[d - 1],
            send_sem=s8.at[d - 1],
            recv_sem=v8.at[d - 1],
            device_id=first_peer(d),
            device_id_type=MESH,
        )
        three[d].start()
        return None

    for k, d in enumerate(steps):
        at_f = lax.rem(other_first + d, n)
        rows_of = dt[other, pl.ds(at_f * n, n)].reshape(n * half, HIDDEN_PAD)
        xo[k] = dot(rows_of, units).astype(BF16)
        c = pltpu.make_async_remote_copy(
            src_ref=xo.at[k],
            dst_ref=xi.at[k],
            send_sem=s7.at[k],
            recv_sem=v7.at[k],
            device_id=sibling,
            device_id_type=MESH,
        )
        c.start()
        swaps.append(c)
        at_f = lax.rem(first + d, n)
        rows_of = dt[tp, pl.ds(at_f * n, n)].reshape(n * half, HIDDEN_PAD)
        p5[k] = dot(rows_of, units)
        if k >= LAG:
            finish(k - LAG)
    for k in range(max(0, n - LAG), n):
        own = finish(k)
    for d in order:
        three[d].wait_recv()
    for d in order:
        own = own + r3[d - 1].astype(F32)
    own = own.reshape(n, half, seqs)
    p5[0] = own.reshape(n * half, seqs)
    q4b[...] = own.astype(BF16)
    four = exchange(
        lambda d: q4b.at[lax.rem(second + d, n)], lambda d: r4.at[d - 1], s9, v9, second_peer
    )
    last = p5[0, pl.ds(pl.multiple_of(second * half, half), half), :]
    last = last + rt[z, y, tp].astype(F32)
    for d in order:
        four[d].wait_recv()
    for d in order:
        last = last + r4[d - 1].astype(F32)
    out_ref[...] = last.astype(BF16)

    for made in (one, two, three, four):
        for c in made.values():
            c.wait_send()
    for c in swaps:
        c.wait_send()
    for c in (swap, all_mh, all_wg, all_tg):
        c.wait_send()
    for d in range(1, n):
        block_copy(s5.at[d - 1], v5.at[d - 1]).wait_send()
    for d in range(n):
        block_copy(s6.at[d], v6.at[d]).wait_send()


def per_device(n, *args):
    (tokens, pre, qw, kw, vw, ow, ig, fg, ck, cv, ci, cf, lens, sm, sn, smax) = args[:16]
    hg, mixw, mg, gw, uw, dw = args[16:]
    operands = (
        tokens.T,
        pre.reshape(1, -1),
        qw,
        kw,
        vw,
        ow,
        ig.T,
        fg.T,
        ck,
        cv,
        ci.transpose(0, 2, 1),
        cf.transpose(0, 2, 1),
        lens,
        sm,
        sn,
        smax,
        hg.reshape(1, -1),
        mixw.T,
        mg.reshape(1, -1),
        gw.T,
        uw.T,
        dw,
    )
    seqs, width = tokens.shape
    cols = qw.shape[1]
    kvs = n * n
    model = width * kvs
    span, size = ck.shape[1], sn.shape[2]
    wide = KINDS * cols + 128
    half = width // 2
    dma = pltpu.SemaphoreType.DMA
    vmem = pltpu.VMEM
    scratch = [
        vmem((width, seqs), BF16),
        vmem((1, width), F32),
        vmem((KINDS, width, cols), BF16),
        vmem((2, 4, model), BF16),
        vmem((2, span, cols), BF16),
        vmem((2, span, cols), BF16),
        vmem((2, 2, span), F32),
        vmem((2, 2, span), F32),
        pltpu.SMEM((2,), jnp.int32),
        vmem((2, 2, size, size), F32),
        vmem((2, 2, size), F32),
        pltpu.SMEM((2, 2), F32),
        vmem((1, cols), F32),
        vmem((width, cols), BF16),
        vmem((1, model), F32),
        vmem((gw.shape[1], model), BF16),
        vmem((gw.shape[1], model), BF16),
        vmem((gw.shape[1], model), BF16),
        dma((22,)),
        vmem((n, 2 * n, wide), BF16),
        vmem((n - 1, 2 * n, wide), BF16),
        vmem((n * ROWS, 128), F32),
        vmem((n, ROWS, 128), BF16),
        vmem((n - 1, ROWS, 128), BF16),
        vmem((2, 4, size, size), BF16),
        vmem((4 * seqs, 8 * kvs), BF16),
        vmem((kvs, 8, 128), BF16),
        vmem((n * half, seqs), BF16),
        vmem((n * half, seqs), BF16),
        vmem((2, n, half, cols), BF16),
        vmem((n, half, seqs), BF16),
        vmem((n, half, seqs), BF16),
        vmem((n, n, 2, half, seqs), BF16),
        vmem((2 * HIDDEN_PAD, model), BF16),
        vmem((2, kvs, half, HIDDEN_PAD), BF16),
        vmem((n, n * half, seqs), BF16),
        vmem((n, n * half, seqs), BF16),
        vmem((n, n * half, seqs), F32),
        vmem((n, n * half, seqs), BF16),
        vmem((n - 1, n * half, seqs), BF16),
        vmem((n, half, seqs), BF16),
        vmem((n - 1, half, seqs), BF16),
        dma((n - 1,)),
        dma((n - 1,)),
        dma((n - 1,)),
        dma((n - 1,)),
        dma,
        dma,
        dma,
        dma,
        dma((n - 1,)),
        dma((n - 1,)),
        dma((n,)),
        dma((n,)),
        dma((n,)),
        dma((n,)),
        dma((n - 1,)),
        dma((n - 1,)),
        dma((n - 1,)),
        dma((n - 1,)),
        dma,
        dma,
        dma,
        dma,
    ]
    out = pl.pallas_call(
        functools.partial(kernel, n),
        out_shape=jax.ShapeDtypeStruct((half, seqs), BF16),
        in_specs=[pl.BlockSpec(memory_space=pl.ANY)] * len(operands),
        out_specs=pl.BlockSpec(memory_space=pltpu.VMEM),
        scratch_shapes=scratch,
        compiler_params=pltpu.CompilerParams(
            collective_id=0, has_side_effects=True, vmem_limit_bytes=62 * 1024 * 1024
        ),
        name="layer",
    )(*operands)
    return out.T


def solution(mesh):
    n = round(mesh.shape["kv"] ** 0.5)
    seq = ("dp", "kv")
    return jax.shard_map(
        functools.partial(per_device, n),
        mesh=mesh,
        in_specs=(
            P("dp", "kv"),
            P("kv"),
            P("kv", "tp"),
            P("kv", "tp"),
            P("kv", "tp"),
            P("kv", "tp"),
            P(),
            P(),
            P(seq, None, "tp"),
            P(seq, None, "tp"),
            P(seq, None, "tp"),
            P(seq, None, "tp"),
            P(seq),
            P(seq, "tp", None, None),
            P(seq, "tp", None),
            P(seq, "tp"),
            P("tp"),
            P("tp", "kv"),
            P(),
            P(None, ("kv", "tp")),
            P(None, ("kv", "tp")),
            P(("kv", "tp"), None),
        ),
        out_specs=P("dp", ("kv", "tp")),
        check_vma=False,
    )
```

```python
import functools

import jax
import jax.numpy as jnp
from jax import lax
from jax.experimental import pallas as pl
from jax.experimental.pallas import tpu as pltpu
from jax.sharding import PartitionSpec as P

EPS = 1e-06
MESH = pl.DeviceIdType.MESH
F32 = jnp.float32
BF16 = jnp.bfloat16
KINDS = 4
ROWS = 40
HIDDEN_PAD = 48


def ring_order(n):
    return sorted(range(1, n), key=lambda d: (-min(d, n - d), d))


def plane_order(n):
    def hops(d):
        return min(d, n - d)

    pairs = [(dz, dy) for dz in range(n) for dy in range(n) if dz or dy]
    return sorted(pairs, key=lambda p: (-hops(p[0]) - hops(p[1]), (3 * p[0] + 5 * p[1]) % n))


def dot(a, b, ca=1, cb=0, precision=None):
    return lax.dot_general(
        a, b, (((ca,), (cb,)), ((), ())), preferred_element_type=F32, precision=precision
    )


def iota(shape, dim):
    return lax.broadcasted_iota(jnp.int32, shape, dim)


def kernel(
    n,
    tok_h,
    pre_h,
    qw_h,
    kw_h,
    vw_h,
    ow_h,
    ig_h,
    fg_h,
    ck_h,
    cv_h,
    ci_h,
    cf_h,
    len_h,
    sm_h,
    sn_h,
    smax_h,
    hg_h,
    mixw_h,
    mg_h,
    gw_h,
    uw_h,
    dw_h,
    out_ref,
    tok,
    pre,
    w4,
    gates,
    ck,
    cv,
    ci,
    cf,
    lens,
    state,
    sn,
    smax,
    hg,
    mixw,
    mg,
    gw,
    uw,
    dw,
    load_sem,
    p1,
    r1,
    relay,
    merged,
    q2f,
    q2b,
    r2,
    split,
    pick,
    mh,
    xs,
    xr,
    wg,
    tg,
    rbuf,
    rt,
    gu,
    dt,
    xo,
    xi,
    p5,
    p5b,
    r3,
    result,
    s1,
    v1,
    s2,
    v2,
    s3,
    v3,
    s4,
    v4,
    s5,
    v5,
    s6,
    v6,
    s7,
    v7,
    s8,
    v8,
    s9,
    sw,
    vw,
    st,
    vt,
    sr,
    vr,
    s10,
    v10,
):
    kvs = n * n
    width = tok.shape[0]
    seqs = tok.shape[1]
    cols = w4.shape[2]
    wide = p1.shape[2]
    blocks = cols // 128
    model = width * kvs
    dp = lax.axis_index("dp")
    kv = lax.axis_index("kv")
    tp = lax.axis_index("tp")
    z, y = kv // n, kv % n
    far = n - (n - 1) * tp
    near = 1 + (n - 1) * tp
    first = z + (y - z) * tp
    second = y + (z - y) * tp
    other = 1 - tp
    order = ring_order(n)

    def first_peer(d):
        return (dp, lax.rem(first + d, n) * far + second * near, tp)

    def second_peer(d):
        return (dp, first * far + lax.rem(second + d, n) * near, tp)

    sibling = (dp, kv, other)

    loads = [
        (tok_h, tok),
        (pre_h, pre),
        (qw_h, w4.at[0]),
        (kw_h, w4.at[1]),
        (vw_h, w4.at[2]),
        (ow_h, w4.at[3]),
        (ig_h, gates.at[0]),
        (fg_h, gates.at[1]),
        (cf_h, cf),
        (ci_h, ci),
        (len_h, lens),
        (smax_h, smax),
        (sm_h, state),
        (sn_h, sn),
        (ck_h, ck),
        (cv_h, cv),
        (hg_h, hg),
        (mixw_h, mixw),
        (mg_h, mg),
        (gw_h, gw),
        (uw_h, uw),
        (dw_h, dw),
    ]
    copies = [pltpu.make_async_copy(a, b, load_sem.at[k]) for k, (a, b) in enumerate(loads)]
    for c in copies[:8]:
        c.start()
    barrier = pltpu.get_barrier_semaphore()
    for d in range(1, n):
        pl.semaphore_signal(barrier, inc=1, device_id=first_peer(d), device_id_type=MESH)
        pl.semaphore_signal(barrier, inc=1, device_id=second_peer(d), device_id_type=MESH)
    pl.semaphore_signal(barrier, inc=1, device_id=sibling, device_id_type=MESH)
    for c in copies[8:]:
        c.start()
    for c in copies[:8]:
        c.wait()

    r = iota((seqs, seqs), 0)
    owner = (r // (2 * n)) * far + (r % n) * near
    perm = jnp.where(iota((seqs, seqs), 1) == owner * 2 + (r // n) % 2, 1.0, 0.0).astype(BF16)
    tokens = dot(perm, tok[...], 1, 1)
    squares = jnp.sum(tokens * tokens, axis=1, keepdims=True)
    normed = (tokens * pre[...]).astype(BF16)
    for k in range(KINDS):
        prod = dot(normed, w4[k]).astype(BF16)
        p1[:, :, k * cols : (k + 1) * cols] = prod.reshape(n, 2 * n, cols)
    lane0 = pl.multiple_of((kv // (128 // width)) * 128, 128)
    both = jnp.concatenate(
        [gates[0, :, pl.ds(lane0, 128)].astype(F32), gates[1, :, pl.ds(lane0, 128)].astype(F32)],
        axis=0,
    ).astype(BF16)
    at = (kv % (128 // width)) * width
    sel = jnp.where(iota((width, 128), 1) == iota((width, 128), 0) + at, 1.0, 0.0).astype(BF16)
    own_gates = dot(both, sel, 1, 1)
    own_gates = jnp.concatenate([own_gates, jnp.zeros((120, width), F32)], axis=0).astype(BF16)
    g = dot(normed, own_gates, 1, 1)
    g = jnp.where(iota((seqs, 128), 1) == 8, squares, g)
    p1[:, :, KINDS * cols :] = g.astype(BF16).reshape(n, 2 * n, 128)

    pl.semaphore_wait(barrier, 2 * (n - 1) + 1)

    def exchange(src, dst, send, recv, peer):
        made = {}
        for d in order:
            made[d] = pltpu.make_async_remote_copy(
                src_ref=src(d),
                dst_ref=dst(d),
                send_sem=send.at[d - 1],
                recv_sem=recv.at[d - 1],
                device_id=peer(d),
                device_id_type=MESH,
            )
            made[d].start()
        return made

    far_d = n // 2
    cut = (KINDS * blocks // 2 + 1) * 128
    parts = (pl.ds(0, cut), pl.ds(cut, wide - cut))

    def part_copy(src, dst, peer, send, recv, k):
        return pltpu.make_async_remote_copy(
            src_ref=src.at[:, parts[k]],
            dst_ref=dst.at[:, parts[k]],
            send_sem=send,
            recv_sem=recv,
            device_id=first_peer(peer),
            device_id_type=MESH,
        )

    def rows_for(d):
        return p1.at[lax.rem(first + d, n)]

    hops = (n - 1, 1)
    last_d = (far_d + 1, far_d - 1)
    handed = [
        part_copy(rows_for(far_d), relay, hops[k], sr.at[k], vr.at[k], k) for k in range(2)
    ]
    for c in handed:
        c.start()
    one = []
    for k in range(2):
        d = last_d[k]
        one.append(
            part_copy(rows_for(d), r1.at[d - 1], d, s1.at[d - 1], v1.at[d - 1], 1 - k)
        )
    for d in order:
        if d == far_d or d in last_d:
            continue
        one.append(
            pltpu.make_async_remote_copy(
                src_ref=rows_for(d),
                dst_ref=r1.at[d - 1],
                send_sem=s1.at[d - 1],
                recv_sem=v1.at[d - 1],
                device_id=first_peer(d),
                device_id_type=MESH,
            )
        )
    for c in one[:-2]:
        c.start()

    for c in copies[8:]:
        c.wait()
    row64 = iota((8, ck.shape[1]), 0)
    lane64 = iota((8, ck.shape[1]), 1)
    zero4 = jnp.zeros((4, ck.shape[1]), F32)
    forget = jnp.concatenate([cf[0], cf[1], zero4], axis=0)
    gain_in = jnp.concatenate([ci[0], ci[1], zero4], axis=0)
    length = jnp.where(row64 < 2, lens[0], lens[1])
    live = lane64 < length
    forget = jnp.where(live, forget, 0.0)
    span = ck.shape[1]
    tri = jnp.where(iota((span, span), 0) <= iota((span, span), 1), 1.0, 0.0)
    running = dot(forget, tri, precision=lax.Precision.HIGHEST)
    run_last = jnp.sum(forget, axis=1, keepdims=True)
    base = jnp.where(live, run_last - running + gain_in, -jnp.inf)
    base = jnp.where(row64 < 4, base, 0.0)
    base_max = jnp.max(base, axis=1, keepdims=True)
    row1 = iota((8, 1), 0)
    state_top = jnp.where(
        row1 == 0,
        smax[0, 0],
        jnp.where(row1 == 1, smax[0, 1], jnp.where(row1 == 2, smax[1, 0], smax[1, 1])),
    )
    state_base = run_last + state_top
    for i in range(2):
        for h in range(2):
            whole = state[i, h]
            high = whole.astype(BF16)
            split[0, 2 * i + h] = high
            split[1, 2 * i + h] = (whole - high.astype(F32)).astype(BF16)
    size = sn.shape[2]
    zero_rows = jnp.zeros((4, size), F32)
    norm8 = jnp.concatenate([sn[0], sn[1], zero_rows], axis=0)
    halves = [hg[:, :size], hg[:, size:]]
    gain8 = jnp.concatenate(halves + halves + [zero_rows], axis=0)
    pr = iota((4 * seqs, 8 * kvs), 0)
    pc = iota((4 * seqs, 8 * kvs), 1)
    seq, hu = pr % seqs, pr // seqs
    target = (seq // 2) * 8 + (hu % 2) * 4 + (seq % 2) * 2 + hu // 2
    pick[...] = jnp.where(pc == target, 1.0, 0.0).astype(BF16)
    hidden_cols = gw.shape[0]
    gu[...] = jnp.zeros_like(gu)
    gu[:hidden_cols, :] = (gw[...].astype(F32) * mg[...]).astype(BF16)
    gu[HIDDEN_PAD : HIDDEN_PAD + hidden_cols, :] = (uw[...].astype(F32) * mg[...]).astype(BF16)
    group = 128 // width

    def arrange(b, carry):
        block = dw[:, pl.ds(pl.multiple_of(b * 128, 128), 128)].astype(F32)
        block = jnp.concatenate([block, jnp.zeros((HIDDEN_PAD - hidden_cols, 128), F32)], axis=0)
        block = block.T.astype(BF16)
        for k in range(group):
            at_kv = b * group + k
            mirrored = (at_kv % n) * n + at_kv // n
            half = width // 2
            dt[0, at_kv] = block[k * width : k * width + half]
            dt[1, mirrored] = block[k * width + half : (k + 1) * width]
        return carry

    lax.fori_loop(0, kvs // group, arrange, 0)

    late = []
    late_sems = ((s1.at[far_d - 1], v1.at[far_d - 1]), (s10, v10))
    for k in range(2):
        d = last_d[k]
        handed[k].wait_recv()
        mine = p1[lax.rem(first + d, n), :, parts[k]].astype(F32)
        merged[:, parts[k]] = (mine + relay[:, parts[k]].astype(F32)).astype(BF16)
        c = part_copy(merged, r1.at[d - 1], d, late_sems[k][0], late_sems[k][1], k)
        c.start()
        late.append(c)
    for c in one[-2:]:
        c.start()
    one = one + late
    own = p1[first].astype(F32)
    for c in one:
        c.wait_recv()
    for d in order:
        if d != far_d:
            own = own + r1[d - 1].astype(F32)
    q2f[...] = jnp.zeros_like(q2f)
    for i in range(2):
        part = own[i * n : (i + 1) * n]
        for c in range(KINDS * blocks):
            kind, h, u = c // blocks, (c % blocks) // 2, c % 2
            q2f[pl.ds(kind * 8 + u * 4 + i * 2 + h, n, stride=ROWS), :] = part[
                :, c * 128 : (c + 1) * 128
            ]
        for h in range(2):
            q2f[pl.ds(32 + i * 2 + h, n, stride=ROWS), :] = part[:, KINDS * cols :]
    q2b[...] = q2f[...].reshape(n, ROWS, 128).astype(BF16)
    two = exchange(
        lambda d: q2b.at[lax.rem(second + d, n)], lambda d: r2.at[d - 1], s2, v2, second_peer
    )
    half = width // 2
    axes = ((0, y, lambda d: z * n + lax.rem(y + d, n)), (1, z, lambda d: lax.rem(z + d, n) * n + y))
    for u, place, peer in axes:
        for d in order:
            pltpu.make_async_remote_copy(
                src_ref=mixw.at[pl.ds(u * half, half)],
                dst_ref=wg.at[u, place],
                send_sem=sw,
                recv_sem=vw,
                device_id=(dp, peer(d), tp),
                device_id_type=MESH,
            ).start()
        wg[u, place] = mixw[u * half : (u + 1) * half, :]
    own_rows = pl.ds(pl.multiple_of(tp * half, half), half)
    for d in order:
        pltpu.make_async_remote_copy(
            src_ref=tok.at[own_rows],
            dst_ref=tg.at[second],
            send_sem=st,
            recv_sem=vt,
            device_id=second_peer(d),
            device_id_type=MESH,
        ).start()
    tg[second] = tok[own_rows, :]
    all_wg = pltpu.make_async_remote_copy(
        src_ref=wg.at[:, pl.ds(0, n - 1)],
        dst_ref=wg.at[:, pl.ds(0, n - 1)],
        send_sem=sw,
        recv_sem=vw,
        device_id=sibling,
        device_id_type=MESH,
    )
    all_tg = pltpu.make_async_remote_copy(
        src_ref=tg.at[pl.ds(0, n - 1)],
        dst_ref=tg.at[pl.ds(0, n - 1)],
        send_sem=st,
        recv_sem=vt,
        device_id=sibling,
        device_id_type=MESH,
    )
    mine = q2f[pl.ds(pl.multiple_of(second * ROWS, 8), ROWS), :]
    for d in order:
        two[d].wait_recv()
    for d in order:
        mine = mine + r2[d - 1].astype(F32)

    def heads(kind):
        a = mine[kind * 8 : kind * 8 + 4]
        b = mine[kind * 8 + 4 : kind * 8 + 8]
        return jnp.concatenate([jnp.concatenate([a, b], axis=1), zero_rows], axis=0)

    gate8 = mine[32:40]
    lane = iota((8, 128), 1)
    row = iota((8, 128), 0)
    square = jnp.sum(jnp.where(lane == 8, gate8, 0.0), axis=1, keepdims=True)
    in_sum = jnp.sum(jnp.where(lane == 2 * tp + row % 2, gate8, 0.0), axis=1, keepdims=True)
    fg_sum = jnp.sum(jnp.where(lane == 4 + 2 * tp + row % 2, gate8, 0.0), axis=1, keepdims=True)
    scale = lax.rsqrt(square / model + EPS)
    query = (scale * heads(0)).astype(BF16).astype(F32)
    key_new = (scale * heads(1)).astype(BF16).astype(F32)
    value_new = (scale * heads(2)).astype(BF16).astype(F32)
    outgate = (scale * heads(3)).astype(BF16).astype(F32)
    in_gate = scale * in_sum
    fg = scale * fg_sum
    forget_new = jnp.minimum(fg, 0.0) - jnp.log1p(jnp.exp(-jnp.abs(fg)))
    weight_log = base + forget_new
    state_log = state_base + forget_new
    peak = jnp.maximum(jnp.maximum(state_log, in_gate), base_max + forget_new)
    query = query * (size**-0.5)
    rows = iota((8, size), 0)
    alone = [jnp.where(rows == k, query, 0.0) for k in range(4)]
    dots = dot(jnp.concatenate(alone[0:2], axis=1).astype(BF16), ck[0], 1, 1)
    dots = dots + dot(jnp.concatenate(alone[2:4], axis=1).astype(BF16), ck[1], 1, 1)
    scores = jnp.exp(weight_log - peak) * dots
    self_score = jnp.exp(in_gate - peak) * jnp.sum(query * key_new, axis=1, keepdims=True)
    carried = jnp.exp(state_log - peak)
    read = dot(alone[0].astype(BF16), split[0, 0], 1, 1)
    read = read + dot(alone[0].astype(BF16), split[1, 0], 1, 1)
    for k in range(1, 4):
        read = read + dot(alone[k].astype(BF16), split[0, k], 1, 1)
        read = read + dot(alone[k].astype(BF16), split[1, k], 1, 1)
    norm_read = jnp.sum(norm8 * query, axis=1, keepdims=True)
    values = dot(jnp.where(row64 < 2, scores, 0.0).astype(BF16), cv[0])
    values = values + dot(jnp.where(row64 >= 2, scores, 0.0).astype(BF16), cv[1])
    values = jnp.where(rows % 2 == 0, values[:, :size], values[:, size:])
    numerator = carried * read + values + self_score * value_new
    denominator = carried * norm_read + jnp.sum(scores, axis=1, keepdims=True) + self_score
    hidden = numerator / jnp.maximum(jnp.abs(denominator), 1.0)
    mixed = hidden * gain8 * jax.nn.sigmoid(outgate)
    mh[kv] = jnp.concatenate([mixed[:4, :128], mixed[:4, 128:]], axis=0).astype(BF16)

    for dz, dy in plane_order(n):
        pltpu.make_async_remote_copy(
            src_ref=mh.at[kv],
            dst_ref=mh.at[kv],
            send_sem=s3,
            recv_sem=v3,
            device_id=(dp, lax.rem(z + dz, n) * n + lax.rem(y + dy, n), tp),
            device_id_type=MESH,
        ).start()
    all_mh = pltpu.make_async_remote_copy(
        src_ref=mh.at[pl.ds(0, kvs - 1)],
        dst_ref=mh.at[pl.ds(0, kvs - 1)],
        send_sem=s3,
        recv_sem=v3,
        device_id=sibling,
        device_id_type=MESH,
    )
    all_wg.wait_recv()
    all_tg.wait_recv()
    all_mh.wait_recv()

    flat = mh[...].astype(F32).reshape(8 * kvs, 128).astype(BF16)
    picked = dot(pick[...], flat).astype(BF16)

    def project(u):
        w = wg[u].reshape(n * half, cols)
        total = dot(w[:, :128], picked[:seqs], 1, 1)
        for k in range(1, 4):
            block = picked[k * seqs : (k + 1) * seqs]
            total = total + dot(w[:, k * 128 : (k + 1) * 128], block, 1, 1)
        return total.astype(BF16)

    xs[...] = project(other)
    swap = pltpu.make_async_remote_copy(
        src_ref=xs,
        dst_ref=xr,
        send_sem=s4,
        recv_sem=v4,
        device_id=sibling,
        device_id_type=MESH,
    )
    swap.start()
    mix = project(tp)
    swap.wait_recv()
    total = tg[...].reshape(n * half, seqs).astype(F32) + (mix.astype(F32) + xr[...].astype(F32))
    rbuf[...] = total.astype(BF16).reshape(n, half, seqs)

    def gather(u):
        def rows(f):
            return rt.at[f, :, 0] if u == 0 else rt.at[:, f, 1]

        made = exchange(lambda d: rbuf, lambda d: rows(first), s5, v5, first_peer)
        if u == 0:
            rt[z, :, 0] = rbuf[...]
        else:
            rt[:, y, 1] = rbuf[...]
        for d in [0] + order[::-1]:
            if d:
                made[d].wait_recv()
            source = lax.rem(first + n - d, n)
            pltpu.make_async_remote_copy(
                src_ref=rows(source),
                dst_ref=rows(source),
                send_sem=s6.at[d],
                recv_sem=v6.at[d],
                device_id=sibling,
                device_id_type=MESH,
            ).start()

    @pl.when(tp == 0)
    def _():
        gather(0)

    @pl.when(tp == 1)
    def _():
        gather(1)

    def block_copy(send, recv):
        return pltpu.make_async_remote_copy(
            src_ref=rbuf,
            dst_ref=rt.at[0, :, 0],
            send_sem=send,
            recv_sem=recv,
            device_id=sibling,
            device_id_type=MESH,
        )

    for d in range(n):
        block_copy(s6.at[d], v6.at[d]).wait_recv()

    residual = rt[...].reshape(model, seqs)
    spread = residual.astype(F32)
    power = jnp.sum(spread * spread, axis=0, keepdims=True)
    acc = dot(gu[...], residual)
    scale_mid = lax.rsqrt(power / model + EPS)
    gate = scale_mid * acc[:HIDDEN_PAD]
    up = scale_mid * acc[HIDDEN_PAD:]
    units = (gate * jax.nn.sigmoid(gate) * up).astype(BF16)

    other_first = y + (z - y) * tp
    steps = order + [0]
    whole = dot(dt[other].reshape(kvs * half, HIDDEN_PAD), units)
    xo[...] = whole.astype(BF16).reshape(n, n * half, seqs)
    swaps = []
    for k, d in enumerate(steps):
        c = pltpu.make_async_remote_copy(
            src_ref=xo.at[lax.rem(other_first + d, n)],
            dst_ref=xi.at[k],
            send_sem=s7.at[k],
            recv_sem=v7.at[k],
            device_id=sibling,
            device_id_type=MESH,
        )
        c.start()
        swaps.append(c)
    p5[...] = dot(dt[tp].reshape(kvs * half, HIDDEN_PAD), units).reshape(n, n * half, seqs)
    for k, d in enumerate(steps):
        swaps[k].wait_recv()
        at_f = lax.rem(first + d, n)
        both = p5[at_f] + xi[k].astype(F32)
        p5b[k] = both.astype(BF16).reshape(n, half, seqs)
        if d == 0:
            p5[at_f] = both
        for e in steps:
            if d or e:
                at_s = lax.rem(second + e, n)
                pltpu.make_async_remote_copy(
                    src_ref=p5b.at[k, at_s],
                    dst_ref=r3.at[d * n + e - 1],
                    send_sem=s8,
                    recv_sem=v8,
                    device_id=(dp, at_f * far + at_s * near, tp),
                    device_id_type=MESH,
                ).start()
    last = p5[first, pl.ds(pl.multiple_of(second * half, half), half), :]
    last = last + rt[z, y, tp].astype(F32)
    all_r3 = pltpu.make_async_remote_copy(
        src_ref=r3,
        dst_ref=r3,
        send_sem=s8,
        recv_sem=v8,
        device_id=sibling,
        device_id_type=MESH,
    )
    all_r3.wait_recv()
    last = last + jnp.sum(r3[...].astype(F32), axis=0)
    result[...] = last.astype(BF16)
    written = pltpu.make_async_copy(result, out_ref, s9)
    written.start()

    for c in two.values():
        c.wait_send()
    for c in one + handed:
        c.wait_send()
    for c in swaps:
        c.wait_send()
    for c in (swap, all_mh, all_wg, all_tg, all_r3):
        c.wait_send()
    for d in range(1, n):
        block_copy(s5.at[d - 1], v5.at[d - 1]).wait_send()
    for d in range(n):
        block_copy(s6.at[d], v6.at[d]).wait_send()
    written.wait()


def per_device(n, *args):
    (tokens, pre, qw, kw, vw, ow, ig, fg, ck, cv, ci, cf, lens, sm, sn, smax) = args[:16]
    hg, mixw, mg, gw, uw, dw = args[16:]
    operands = (
        tokens.T,
        pre.reshape(1, -1),
        qw,
        kw,
        vw,
        ow,
        ig.T,
        fg.T,
        ck,
        cv,
        ci.transpose(0, 2, 1),
        cf.transpose(0, 2, 1),
        lens,
        sm,
        sn,
        smax,
        hg.reshape(1, -1),
        mixw.T,
        mg.reshape(1, -1),
        gw.T,
        uw.T,
        dw,
    )
    seqs, width = tokens.shape
    cols = qw.shape[1]
    kvs = n * n
    model = width * kvs
    span, size = ck.shape[1], sn.shape[2]
    wide = KINDS * cols + 128
    half = width // 2
    dma = pltpu.SemaphoreType.DMA
    vmem = pltpu.VMEM
    scratch = [
        vmem((width, seqs), BF16),
        vmem((1, width), F32),
        vmem((KINDS, width, cols), BF16),
        vmem((2, 4, model), BF16),
        vmem((2, span, cols), BF16),
        vmem((2, span, cols), BF16),
        vmem((2, 2, span), F32),
        vmem((2, 2, span), F32),
        pltpu.SMEM((2,), jnp.int32),
        vmem((2, 2, size, size), F32),
        vmem((2, 2, size), F32),
        pltpu.SMEM((2, 2), F32),
        vmem((1, cols), F32),
        vmem((width, cols), BF16),
        vmem((1, model), F32),
        vmem((gw.shape[1], model), BF16),
        vmem((gw.shape[1], model), BF16),
        vmem((gw.shape[1], model), BF16),
        dma((22,)),
        vmem((n, 2 * n, wide), BF16),
        vmem((n - 1, 2 * n, wide), BF16),
        vmem((2 * n, wide), BF16),
        vmem((2 * n, wide), BF16),
        vmem((n * ROWS, 128), F32),
        vmem((n, ROWS, 128), BF16),
        vmem((n - 1, ROWS, 128), BF16),
        vmem((2, 4, size, size), BF16),
        vmem((4 * seqs, 8 * kvs), BF16),
        vmem((kvs, 8, 128), BF16),
        vmem((n * half, seqs), BF16),
        vmem((n * half, seqs), BF16),
        vmem((2, n, half, cols), BF16),
        vmem((n, half, seqs), BF16),
        vmem((n, half, seqs), BF16),
        vmem((n, n, 2, half, seqs), BF16),
        vmem((2 * HIDDEN_PAD, model), BF16),
        vmem((2, kvs, half, HIDDEN_PAD), BF16),
        vmem((n, n * half, seqs), BF16),
        vmem((n, n * half, seqs), BF16),
        vmem((n, n * half, seqs), F32),
        vmem((n, n, half, seqs), BF16),
        vmem((kvs - 1, half, seqs), BF16),
        vmem((half, seqs), BF16),
        dma((n - 1,)),
        dma((n - 1,)),
        dma((n - 1,)),
        dma((n - 1,)),
        dma,
        dma,
        dma,
        dma,
        dma((n - 1,)),
        dma((n - 1,)),
        dma((n,)),
        dma((n,)),
        dma((n,)),
        dma((n,)),
        dma,
        dma,
        dma,
        dma,
        dma,
        dma,
        dma,
        dma((2,)),
        dma((2,)),
        dma,
        dma,
    ]
    out = pl.pallas_call(
        functools.partial(kernel, n),
        out_shape=jax.ShapeDtypeStruct((half, seqs), BF16),
        in_specs=[pl.BlockSpec(memory_space=pl.ANY)] * len(operands),
        out_specs=pl.BlockSpec(memory_space=pl.ANY),
        scratch_shapes=scratch,
        compiler_params=pltpu.CompilerParams(
            collective_id=0, has_side_effects=True, vmem_limit_bytes=62 * 1024 * 1024
        ),
        name="layer",
    )(*operands)
    return out.T


def solution(mesh):
    n = round(mesh.shape["kv"] ** 0.5)
    seq = ("dp", "kv")
    return jax.shard_map(
        functools.partial(per_device, n),
        mesh=mesh,
        in_specs=(
            P("dp", "kv"),
            P("kv"),
            P("kv", "tp"),
            P("kv", "tp"),
            P("kv", "tp"),
            P("kv", "tp"),
            P(),
            P(),
            P(seq, None, "tp"),
            P(seq, None, "tp"),
            P(seq, None, "tp"),
            P(seq, None, "tp"),
            P(seq),
            P(seq, "tp", None, None),
            P(seq, "tp", None),
            P(seq, "tp"),
            P("tp"),
            P("tp", "kv"),
            P(),
            P(None, ("kv", "tp")),
            P(None, ("kv", "tp")),
            P(("kv", "tp"), None),
        ),
        out_specs=P("dp", ("kv", "tp")),
        check_vma=False,
    )
```

```python
import functools

import jax
import jax.numpy as jnp
from jax import lax
from jax.experimental import pallas as pl
from jax.experimental.pallas import tpu as pltpu
from jax.sharding import PartitionSpec as P

EPS = 1e-06
MESH = pl.DeviceIdType.MESH
F32 = jnp.float32
BF16 = jnp.bfloat16
KINDS = 4
ROWS = 40
HIDDEN_PAD = 48


def ring_order(n):
    return sorted(range(1, n), key=lambda d: (-min(d, n - d), d))


def dot(a, b, ca=1, cb=0, precision=None):
    return lax.dot_general(
        a, b, (((ca,), (cb,)), ((), ())), preferred_element_type=F32, precision=precision
    )


def iota(shape, dim):
    return lax.broadcasted_iota(jnp.int32, shape, dim)


def kernel(
    n,
    tok_h,
    pre_h,
    qw_h,
    kw_h,
    vw_h,
    ow_h,
    ig_h,
    fg_h,
    ck_h,
    cv_h,
    ci_h,
    cf_h,
    len_h,
    sm_h,
    sn_h,
    smax_h,
    hg_h,
    mixw_h,
    mg_h,
    gw_h,
    uw_h,
    dw_h,
    out_ref,
    tok,
    pre,
    w4,
    gates,
    cfi,
    lens,
    smax,
    state,
    sn,
    ckv,
    hg,
    mixw,
    mg,
    gud,
    load_sem,
    p1,
    r1,
    relay,
    merged,
    q2f,
    q2b,
    r2,
    split,
    pick,
    mh,
    wg,
    tg,
    rbuf,
    rt,
    gu,
    dt,
    xo,
    xi,
    p5,
    p5b,
    r3,
    result,
    s1,
    v1,
    sr,
    vr,
    s2,
    v2,
    sw,
    vw,
    st,
    vt,
    s3,
    v3,
    s5,
    v5,
    s6,
    v6,
    s7,
    v7,
    s8,
    v8,
    s9,
):
    kvs = n * n
    width = tok.shape[0]
    seqs = tok.shape[1]
    cols = w4.shape[2]
    wide = p1.shape[2]
    blocks = cols // 128
    model = width * kvs
    dp = lax.axis_index("dp")
    kv = lax.axis_index("kv")
    tp = lax.axis_index("tp")
    z, y = kv // n, kv % n
    far = n - (n - 1) * tp
    near = 1 + (n - 1) * tp
    first = z + (y - z) * tp
    second = y + (z - y) * tp
    other = 1 - tp
    order = ring_order(n)

    def first_peer(d):
        return (dp, lax.rem(first + d, n) * far + second * near, tp)

    def second_peer(d):
        return (dp, first * far + lax.rem(second + d, n) * near, tp)

    sibling = (dp, kv, other)

    loads = [
        (tok_h, tok, 0),
        (pre_h, pre, 1),
        (qw_h, w4.at[0], 2),
        (kw_h, w4.at[1], 2),
        (vw_h, w4.at[2], 2),
        (ow_h, w4.at[3], 2),
        (ig_h, gates.at[0], 3),
        (fg_h, gates.at[1], 3),
        (cf_h, cfi.at[0], 4),
        (ci_h, cfi.at[1], 4),
        (len_h, lens, 5),
        (smax_h, smax, 6),
        (sm_h, state, 7),
        (sn_h, sn, 8),
        (ck_h, ckv.at[0], 9),
        (cv_h, ckv.at[1], 9),
        (hg_h, hg, 10),
        (mixw_h, mixw, 11),
        (mg_h, mg, 12),
        (gw_h, gud.at[0], 13),
        (uw_h, gud.at[1], 13),
        (dw_h, gud.at[2], 13),
    ]
    copies = [pltpu.make_async_copy(a, b, load_sem.at[k]) for a, b, k in loads]
    landed = [tok, pre, w4, gates, cfi, lens, smax, state, sn, ckv, hg, mixw, mg, gud]
    arrived = [pltpu.make_async_copy(r, r, load_sem.at[k]) for k, r in enumerate(landed)]
    for c in copies[:8]:
        c.start()
    barrier = pltpu.get_barrier_semaphore()
    for d in range(1, n):
        pl.semaphore_signal(barrier, inc=1, device_id=first_peer(d), device_id_type=MESH)
        pl.semaphore_signal(barrier, inc=1, device_id=second_peer(d), device_id_type=MESH)
        across = (dp, z * n + lax.rem(y + d, n), other)
        pl.semaphore_signal(barrier, inc=1, device_id=across, device_id_type=MESH)
    pl.semaphore_signal(barrier, inc=1, device_id=sibling, device_id_type=MESH)
    for c in copies[8:]:
        c.start()
    for c in arrived[:4]:
        c.wait()

    r = iota((seqs, seqs), 0)
    owner = (r // (2 * n)) * far + (r % n) * near
    perm = jnp.where(iota((seqs, seqs), 1) == owner * 2 + (r // n) % 2, 1.0, 0.0).astype(BF16)
    tokens = dot(perm, tok[...], 1, 1)
    squares = jnp.sum(tokens * tokens, axis=1, keepdims=True)
    normed = (tokens * pre[...]).astype(BF16)
    for k in range(KINDS):
        prod = dot(normed, w4[k]).astype(BF16)
        p1[:, :, k * cols : (k + 1) * cols] = prod.reshape(n, 2 * n, cols)
    lane0 = pl.multiple_of((kv // (128 // width)) * 128, 128)
    both = jnp.concatenate(
        [gates[0, :, pl.ds(lane0, 128)].astype(F32), gates[1, :, pl.ds(lane0, 128)].astype(F32)],
        axis=0,
    ).astype(BF16)
    at = (kv % (128 // width)) * width
    sel = jnp.where(iota((width, 128), 1) == iota((width, 128), 0) + at, 1.0, 0.0).astype(BF16)
    own_gates = dot(both, sel, 1, 1)
    own_gates = jnp.concatenate([own_gates, jnp.zeros((120, width), F32)], axis=0).astype(BF16)
    g = dot(normed, own_gates, 1, 1)
    g = jnp.where(iota((seqs, 128), 1) == 8, squares, g)
    p1[:, :, KINDS * cols :] = g.astype(BF16).reshape(n, 2 * n, 128)

    pl.semaphore_wait(barrier, 3 * (n - 1) + 1)

    def total(ref, send, recv):
        return pltpu.make_async_remote_copy(
            src_ref=ref,
            dst_ref=ref,
            send_sem=send,
            recv_sem=recv,
            device_id=sibling,
            device_id_type=MESH,
        )

    def send(src, dst, send_sem, recv_sem, peer):
        pltpu.make_async_remote_copy(
            src_ref=src,
            dst_ref=dst,
            send_sem=send_sem,
            recv_sem=recv_sem,
            device_id=peer,
            device_id_type=MESH,
        ).start()

    far_d = n // 2
    cut = (KINDS * blocks // 2 + 1) * 128
    parts = (pl.ds(0, cut), pl.ds(cut, wide - cut))

    def rows_for(d):
        return p1.at[lax.rem(first + d, n)]

    hops = (n - 1, 1)
    last_d = (far_d + 1, far_d - 1)
    slot = {d: k for k, d in enumerate(d for d in range(1, n) if d != far_d)}
    for k in range(2):
        part = rows_for(far_d).at[:, parts[k]]
        send(part, relay.at[:, parts[k]], sr, vr.at[k], first_peer(hops[k]))
    for k in range(2):
        d, own_part = last_d[k], parts[1 - k]
        send(rows_for(d).at[:, own_part], r1.at[slot[d], :, own_part], s1, v1, first_peer(d))
    direct = [d for d in order if d != far_d and d not in last_d]
    for d in direct:
        if d not in hops:
            send(rows_for(d), r1.at[slot[d]], s1, v1, first_peer(d))

    for c in arrived[4:]:
        c.wait()
    row64 = iota((8, ckv.shape[2]), 0)
    lane64 = iota((8, ckv.shape[2]), 1)
    zero4 = jnp.zeros((4, ckv.shape[2]), F32)
    forget = jnp.concatenate([cfi[0, 0], cfi[0, 1], zero4], axis=0)
    gain_in = jnp.concatenate([cfi[1, 0], cfi[1, 1], zero4], axis=0)
    length = jnp.where(row64 < 2, lens[0], lens[1])
    live = lane64 < length
    forget = jnp.where(live, forget, 0.0)
    span = ckv.shape[2]
    tri = jnp.where(iota((span, span), 0) <= iota((span, span), 1), 1.0, 0.0)
    running = dot(forget, tri, precision=lax.Precision.HIGHEST)
    run_last = jnp.sum(forget, axis=1, keepdims=True)
    base = jnp.where(live, run_last - running + gain_in, -jnp.inf)
    base = jnp.where(row64 < 4, base, 0.0)
    base_max = jnp.max(base, axis=1, keepdims=True)
    row1 = iota((8, 1), 0)
    state_top = jnp.where(
        row1 == 0,
        smax[0, 0],
        jnp.where(row1 == 1, smax[0, 1], jnp.where(row1 == 2, smax[1, 0], smax[1, 1])),
    )
    state_base = run_last + state_top
    for i in range(2):
        for h in range(2):
            whole = state[i, h]
            high = whole.astype(BF16)
            split[0, 2 * i + h] = high
            split[1, 2 * i + h] = (whole - high.astype(F32)).astype(BF16)
    size = sn.shape[2]
    zero_rows = jnp.zeros((4, size), F32)
    norm8 = jnp.concatenate([sn[0], sn[1], zero_rows], axis=0)
    halves = [hg[:, :size], hg[:, size:]]
    gain8 = jnp.concatenate(halves + halves + [zero_rows], axis=0)
    pr = iota((8 * n, 8 * n), 0)
    pc = iota((8 * n, 8 * n), 1)
    seq, hu = pr % (2 * n), pr // (2 * n)
    target = (seq // 2) * 8 + (hu % 2) * 4 + (seq % 2) * 2 + hu // 2
    pick[...] = jnp.where(pc == target, 1.0, 0.0).astype(BF16)
    hidden_cols = gud.shape[1]
    line = n * width
    c1 = iota((line, line), 1)
    source = ((c1 % (line // 2)) // (width // 2)) * width
    source = source + (c1 // (line // 2)) * (width // 2) + c1 % (width // 2)
    compress = jnp.where(iota((line, line), 0) == source, 1.0, 0.0).astype(BF16)
    pad = jnp.zeros((HIDDEN_PAD - hidden_cols, line), F32)
    for k in range(n):
        at = slice(k * line, (k + 1) * line)
        gain = mg[:, at]
        block = [(gud[u, :, at].astype(F32) * gain) for u in range(2)]
        block = jnp.concatenate([block[0], pad, block[1], pad], axis=0).astype(BF16)
        block = dot(block, compress).astype(BF16)
        for u in range(2):
            to = (u * n + k) * (line // 2)
            gu[:, to : to + line // 2] = block[:, u * (line // 2) : (u + 1) * (line // 2)]
    group = 128 // width

    def arrange(b, carry):
        block = gud[2, :, pl.ds(pl.multiple_of(b * 128, 128), 128)].astype(F32)
        block = jnp.concatenate([block, jnp.zeros((HIDDEN_PAD - hidden_cols, 128), F32)], axis=0)
        block = block.T.astype(BF16)
        for k in range(group):
            at_kv = b * group + k
            mirrored = (at_kv % n) * n + at_kv // n
            half = width // 2
            dt[0, at_kv] = block[k * width : k * width + half]
            dt[1, mirrored] = block[k * width + half : (k + 1) * width]
        return carry

    lax.fori_loop(0, kvs // group, arrange, 0)

    for k in range(2):
        d = last_d[k]
        total(relay.at[:, parts[k]], sr, vr.at[k]).wait_recv()
        mine = p1[lax.rem(first + d, n), :, parts[k]].astype(F32)
        merged[:, parts[k]] = (mine + relay[:, parts[k]].astype(F32)).astype(BF16)
        send(merged.at[:, parts[k]], r1.at[slot[d], :, parts[k]], s1, v1, first_peer(d))
    for d in direct:
        if d in hops:
            send(rows_for(d), r1.at[slot[d]], s1, v1, first_peer(d))
    half = width // 2
    own_rows = pl.ds(pl.multiple_of(tp * half, half), half)
    rest = pl.ds(pl.multiple_of(other * half, half), half)

    def share_weights():
        for d in order:
            along_y = z * n + lax.rem(y + d, n)
            send(tok.at[own_rows], tg.at[y], st, vt, (dp, along_y, tp))
            send(mixw.at[own_rows], wg.at[tp, y], sw, vw, (dp, along_y, tp))
            send(mixw.at[rest], wg.at[tp, y], sw, vw, (dp, along_y, other))
        send(mixw.at[rest], wg.at[tp, y], sw, vw, sibling)

    @pl.when(tp == 1)
    def _():
        share_weights()

    own = p1[first].astype(F32)
    total(r1, s1, v1).wait_recv()
    for k in range(n - 2):
        own = own + r1[k].astype(F32)
    q2f[...] = jnp.zeros_like(q2f)
    for i in range(2):
        part = own[i * n : (i + 1) * n]
        for c in range(KINDS * blocks):
            kind, h, u = c // blocks, (c % blocks) // 2, c % 2
            q2f[pl.ds(kind * 8 + u * 4 + i * 2 + h, n, stride=ROWS), :] = part[
                :, c * 128 : (c + 1) * 128
            ]
        for h in range(2):
            q2f[pl.ds(32 + i * 2 + h, n, stride=ROWS), :] = part[:, KINDS * cols :]
    q2b[...] = q2f[...].reshape(n, ROWS, 128).astype(BF16)
    for d in order:
        send(q2b.at[lax.rem(second + d, n)], r2.at[d - 1], s2, v2, second_peer(d))
    @pl.when(tp == 0)
    def _():
        share_weights()

    wg[tp, y] = mixw[own_rows, :]
    tg[y] = tok[own_rows, :]
    mine = q2f[pl.ds(pl.multiple_of(second * ROWS, 8), ROWS), :]
    total(r2, s2, v2).wait_recv()
    for k in range(n - 1):
        mine = mine + r2[k].astype(F32)

    def heads(kind):
        a = mine[kind * 8 : kind * 8 + 4]
        b = mine[kind * 8 + 4 : kind * 8 + 8]
        return jnp.concatenate([jnp.concatenate([a, b], axis=1), zero_rows], axis=0)

    gate8 = mine[32:40]
    lane = iota((8, 128), 1)
    row = iota((8, 128), 0)
    square = jnp.sum(jnp.where(lane == 8, gate8, 0.0), axis=1, keepdims=True)
    in_sum = jnp.sum(jnp.where(lane == 2 * tp + row % 2, gate8, 0.0), axis=1, keepdims=True)
    fg_sum = jnp.sum(jnp.where(lane == 4 + 2 * tp + row % 2, gate8, 0.0), axis=1, keepdims=True)
    scale = lax.rsqrt(square / model + EPS)
    query = (scale * heads(0)).astype(BF16).astype(F32)
    key_new = (scale * heads(1)).astype(BF16).astype(F32)
    value_new = (scale * heads(2)).astype(BF16).astype(F32)
    outgate = (scale * heads(3)).astype(BF16).astype(F32)
    in_gate = scale * in_sum
    fg = scale * fg_sum
    forget_new = jnp.minimum(fg, 0.0) - jnp.log1p(jnp.exp(-jnp.abs(fg)))
    weight_log = base + forget_new
    state_log = state_base + forget_new
    peak = jnp.maximum(jnp.maximum(state_log, in_gate), base_max + forget_new)
    query = query * (size**-0.5)
    rows = iota((8, size), 0)
    alone = [jnp.where(rows == k, query, 0.0) for k in range(4)]
    dots = dot(jnp.concatenate(alone[0:2], axis=1).astype(BF16), ckv[0, 0], 1, 1)
    dots = dots + dot(jnp.concatenate(alone[2:4], axis=1).astype(BF16), ckv[0, 1], 1, 1)
    scores = jnp.exp(weight_log - peak) * dots
    self_score = jnp.exp(in_gate - peak) * jnp.sum(query * key_new, axis=1, keepdims=True)
    carried = jnp.exp(state_log - peak)
    read = dot(alone[0].astype(BF16), split[0, 0], 1, 1)
    read = read + dot(alone[0].astype(BF16), split[1, 0], 1, 1)
    for k in range(1, 4):
        read = read + dot(alone[k].astype(BF16), split[0, k], 1, 1)
        read = read + dot(alone[k].astype(BF16), split[1, k], 1, 1)
    norm_read = jnp.sum(norm8 * query, axis=1, keepdims=True)
    values = dot(jnp.where(row64 < 2, scores, 0.0).astype(BF16), ckv[1, 0])
    values = values + dot(jnp.where(row64 >= 2, scores, 0.0).astype(BF16), ckv[1, 1])
    values = jnp.where(rows % 2 == 0, values[:, :size], values[:, size:])
    numerator = carried * read + values + self_score * value_new
    denominator = carried * norm_read + jnp.sum(scores, axis=1, keepdims=True) + self_score
    hidden = numerator / jnp.maximum(jnp.abs(denominator), 1.0)
    mixed = hidden * gain8 * jax.nn.sigmoid(outgate)
    mh[tp, z] = jnp.concatenate([mixed[:4, :128], mixed[:4, 128:]], axis=0).astype(BF16)

    for d in order:
        along_z = lax.rem(z + d, n) * n + y
        for core in (tp, other):
            send(mh.at[tp, z], mh.at[tp, z], s3, v3, (dp, along_z, core))
    send(mh.at[tp, z], mh.at[tp, z], s3, v3, sibling)
    flat_w = wg.reshape(2 * n, half, cols)
    flat_m = mh.reshape(2 * n, 8, 128)
    all_wg = total(flat_w.at[pl.ds(0, 2 * n - 1)], sw, vw)
    all_tg = total(tg.at[pl.ds(0, n - 1)], st, vt)
    all_mh = total(flat_m.at[pl.ds(0, 2 * n - 1)], s3, v3)
    for c in (all_wg, all_tg, all_mh):
        c.wait_recv()

    def project(u):
        flat = mh[u].astype(F32).reshape(8 * n, 128).astype(BF16)
        picked = dot(pick[...], flat).astype(BF16)
        w = wg[u].reshape(n * half, cols)
        out = dot(picked[: 2 * n], w[:, :128], 1, 1)
        for k in range(1, 4):
            block = picked[2 * n * k : 2 * n * (k + 1)]
            out = out + dot(block, w[:, k * 128 : (k + 1) * 128], 1, 1)
        return out.astype(BF16).astype(F32)

    q = iota((2 * n, seqs), 0)
    here = jnp.where(iota((2 * n, seqs), 1) == ((q // 2) * n + y) * 2 + q % 2, 1.0, 0.0)
    own_tokens = dot(here.astype(BF16), tg[...].reshape(n * half, seqs), 1, 1)
    rbuf[...] = (own_tokens + (project(0) + project(1))).astype(BF16)

    rt[tp, z, y] = rbuf[...]
    rows_order = order + [0]
    for dz in rows_order:
        for dy in rows_order:
            if dz or dy:
                peer = lax.rem(z + dz, n) * n + lax.rem(y + dy, n)
                send(rbuf, rt.at[tp, z, y], s5, v5.at[dz], (dp, peer, tp))
    for dz in rows_order:
        count = n if dz else n - 1
        total(rt.at[0, 0, pl.ds(0, count)], s5, v5.at[dz]).wait_recv()
        source = lax.rem(z + n - dz, n)
        send(rt.at[tp, source], rt.at[tp, source], s6, v6, sibling)
    total(rt.at[0], s6, v6).wait_recv()

    lanes = n * half
    power = jnp.zeros((seqs, lanes), F32)
    acc = jnp.zeros((2 * HIDDEN_PAD, seqs), F32)
    for u in range(2):
        for k in range(0, n, 2):
            pair = [rt[u, k + e].reshape(seqs, lanes) for e in range(2)]
            at = (u * n + k) * lanes
            wide_pair = jnp.concatenate(pair, axis=1)
            acc = acc + dot(gu[:, at : at + 2 * lanes], wide_pair, 1, 1)
            for block in pair:
                spread = block.astype(F32)
                power = power + spread * spread
    power = dot(jnp.ones((8, lanes), F32), power, 1, 1, precision=lax.Precision.HIGHEST)[:1]
    scale_mid = lax.rsqrt(power / model + EPS)
    gate = scale_mid * acc[:HIDDEN_PAD]
    up = scale_mid * acc[HIDDEN_PAD:]
    units = (gate * jax.nn.sigmoid(gate) * up).astype(BF16)

    other_first = y + (z - y) * tp
    steps = order + [0]
    whole = dot(dt[other].reshape(kvs * half, HIDDEN_PAD), units)
    xo[...] = whole.astype(BF16).reshape(n, n * half, seqs)
    for k, d in enumerate(steps):
        send(xo.at[lax.rem(other_first + d, n)], xi.at[k], s7, v7.at[k], sibling)
    p5[...] = dot(dt[tp].reshape(kvs * half, HIDDEN_PAD), units).reshape(n, n * half, seqs)
    for k, d in enumerate(steps):
        total(xi.at[k], s7, v7.at[k]).wait_recv()
        at_f = lax.rem(first + d, n)
        both = p5[at_f] + xi[k].astype(F32)
        p5b[k] = both.astype(BF16).reshape(n, half, seqs)
        if d == 0:
            p5[at_f] = both
        for e in steps:
            if d or e:
                at_s = lax.rem(second + e, n)
                peer = (dp, at_f * far + at_s * near, tp)
                send(p5b.at[k, at_s], r3.at[d * n + e - 1], s8, v8, peer)
    mine_at = jnp.where(iota((half, lanes), 1) == iota((half, lanes), 0) + y * half, 1.0, 0.0)
    last = dot(mine_at.astype(BF16), rt[tp, z].reshape(seqs, lanes), 1, 1)
    last = last + p5[first, pl.ds(pl.multiple_of(second * half, half), half), :]
    c2 = iota((seqs, seqs), 1)
    back = ((c2 // 2) % n) * 2 * n + (c2 // (2 * n)) * 2 + c2 % 2
    back = jnp.where(iota((seqs, seqs), 0) == back, 1.0, 0.0).astype(BF16)
    total(r3, s8, v8).wait_recv()
    last = last + jnp.sum(r3[...].astype(F32), axis=0)
    result[...] = dot(last.astype(BF16), back).astype(BF16)
    written = pltpu.make_async_copy(result, out_ref, s9)
    written.start()

    total(relay, sr, vr.at[0]).wait_send()
    total(r1, s1, v1).wait_send()
    total(r2, s2, v2).wait_send()
    for c in (all_wg, all_tg, all_mh):
        c.wait_send()
    flat_r = rt.reshape(2 * kvs, 2 * n, lanes)
    total(flat_r.at[pl.ds(0, kvs - 1)], s5, v5.at[0]).wait_send()
    total(rt.at[0], s6, v6).wait_send()
    total(xi, s7, v7.at[0]).wait_send()
    total(r3, s8, v8).wait_send()
    written.wait()


def per_device(n, *args):
    (tokens, pre, qw, kw, vw, ow, ig, fg, ck, cv, ci, cf, lens, sm, sn, smax) = args[:16]
    hg, mixw, mg, gw, uw, dw = args[16:]
    operands = (
        tokens.T,
        pre.reshape(1, -1),
        qw,
        kw,
        vw,
        ow,
        ig.T,
        fg.T,
        ck,
        cv,
        ci.transpose(0, 2, 1),
        cf.transpose(0, 2, 1),
        lens,
        sm,
        sn,
        smax,
        hg.reshape(1, -1),
        mixw.T,
        mg.reshape(1, -1),
        gw.T,
        uw.T,
        dw,
    )
    seqs, width = tokens.shape
    cols = qw.shape[1]
    kvs = n * n
    model = width * kvs
    span, size = ck.shape[1], sn.shape[2]
    wide = KINDS * cols + 128
    half = width // 2
    dma = pltpu.SemaphoreType.DMA
    vmem = pltpu.VMEM
    ff = gw.shape[1]
    scratch = [
        vmem((width, seqs), BF16),
        vmem((1, width), F32),
        vmem((KINDS, width, cols), BF16),
        vmem((2, 4, model), BF16),
        vmem((2, 2, 2, span), F32),
        pltpu.SMEM((2,), jnp.int32),
        pltpu.SMEM((2, 2), F32),
        vmem((2, 2, size, size), F32),
        vmem((2, 2, size), F32),
        vmem((2, 2, span, cols), BF16),
        vmem((1, cols), F32),
        vmem((width, cols), BF16),
        vmem((1, model), F32),
        vmem((3, ff, model), BF16),
        dma((14,)),
        vmem((n, 2 * n, wide), BF16),
        vmem((n - 2, 2 * n, wide), BF16),
        vmem((2 * n, wide), BF16),
        vmem((2 * n, wide), BF16),
        vmem((n * ROWS, 128), F32),
        vmem((n, ROWS, 128), BF16),
        vmem((n - 1, ROWS, 128), BF16),
        vmem((2, 4, size, size), BF16),
        vmem((8 * n, 8 * n), BF16),
        vmem((2, n, 8, 128), BF16),
        vmem((2, n, half, cols), BF16),
        vmem((n, half, seqs), BF16),
        vmem((2 * n, n * half), BF16),
        vmem((2, n, n, 2 * n, n * half), BF16),
        vmem((2 * HIDDEN_PAD, model), BF16),
        vmem((2, kvs, half, HIDDEN_PAD), BF16),
        vmem((n, n * half, seqs), BF16),
        vmem((n, n * half, seqs), BF16),
        vmem((n, n * half, seqs), F32),
        vmem((n, n, half, seqs), BF16),
        vmem((kvs - 1, half, seqs), BF16),
        vmem((half, seqs), BF16),
        dma,
        dma,
        dma,
        dma((2,)),
        dma,
        dma,
        dma,
        dma,
        dma,
        dma,
        dma,
        dma,
        dma,
        dma((n,)),
        dma,
        dma,
        dma,
        dma((n,)),
        dma,
        dma,
        dma,
    ]
    out = pl.pallas_call(
        functools.partial(kernel, n),
        out_shape=jax.ShapeDtypeStruct((half, seqs), BF16),
        in_specs=[pl.BlockSpec(memory_space=pl.ANY)] * len(operands),
        out_specs=pl.BlockSpec(memory_space=pl.ANY),
        scratch_shapes=scratch,
        compiler_params=pltpu.CompilerParams(
            collective_id=0, has_side_effects=True, vmem_limit_bytes=62 * 1024 * 1024
        ),
        name="layer",
    )(*operands)
    return out.T


def solution(mesh):
    n = round(mesh.shape["kv"] ** 0.5)
    seq = ("dp", "kv")
    return jax.shard_map(
        functools.partial(per_device, n),
        mesh=mesh,
        in_specs=(
            P("dp", "kv"),
            P("kv"),
            P("kv", "tp"),
            P("kv", "tp"),
            P("kv", "tp"),
            P("kv", "tp"),
            P(),
            P(),
            P(seq, None, "tp"),
            P(seq, None, "tp"),
            P(seq, None, "tp"),
            P(seq, None, "tp"),
            P(seq),
            P(seq, "tp", None, None),
            P(seq, "tp", None),
            P(seq, "tp"),
            P("tp"),
            P("tp", "kv"),
            P(),
            P(None, ("kv", "tp")),
            P(None, ("kv", "tp")),
            P(("kv", "tp"), None),
        ),
        out_specs=P("dp", ("kv", "tp")),
        check_vma=False,
    )
```

```python
import functools

import jax
import jax.numpy as jnp
from jax import lax
from jax.experimental import pallas as pl
from jax.experimental.pallas import tpu as pltpu
from jax.sharding import PartitionSpec as P

EPS = 1e-06
MESH = pl.DeviceIdType.MESH
F32 = jnp.float32
BF16 = jnp.bfloat16
KINDS = 4
ROWS = 40
HIDDEN_PAD = 48


def ring_order(n):
    return sorted(range(1, n), key=lambda d: (-min(d, n - d), d))


def dot(a, b, ca=1, cb=0, precision=None):
    return lax.dot_general(
        a, b, (((ca,), (cb,)), ((), ())), preferred_element_type=F32, precision=precision
    )


def iota(shape, dim):
    return lax.broadcasted_iota(jnp.int32, shape, dim)


def kernel(
    n,
    tok_h,
    pre_h,
    qw_h,
    kw_h,
    vw_h,
    ow_h,
    ig_h,
    fg_h,
    ck_h,
    cv_h,
    ci_h,
    cf_h,
    len_h,
    sm_h,
    sn_h,
    smax_h,
    hg_h,
    mixw_h,
    mg_h,
    gw_h,
    uw_h,
    dw_h,
    out_ref,
    tok,
    pre,
    w4,
    gates,
    cfi,
    lens,
    smax,
    state,
    sn,
    ckv,
    hg,
    mixw,
    mg,
    gud,
    load_sem,
    p1,
    r1,
    relay,
    merged,
    q2f,
    q2b,
    r2,
    split,
    pick,
    mh,
    wg,
    tg,
    rbuf,
    rt,
    gu,
    dt,
    xo,
    xi,
    p5,
    p5b,
    r3,
    s1,
    v1,
    sr,
    vr,
    s2,
    v2,
    sw,
    vw,
    st,
    vt,
    s3,
    v3,
    s5,
    v5,
    s6,
    v6,
    s7,
    v7,
    s8,
    v8,
):
    kvs = n * n
    width = tok.shape[0]
    seqs = tok.shape[1]
    cols = w4.shape[2]
    wide = p1.shape[2]
    blocks = cols // 128
    model = width * kvs
    dp = lax.axis_index("dp")
    kv = lax.axis_index("kv")
    tp = lax.axis_index("tp")
    z, y = kv // n, kv % n
    far = n - (n - 1) * tp
    near = 1 + (n - 1) * tp
    first = z + (y - z) * tp
    second = y + (z - y) * tp
    other = 1 - tp
    order = ring_order(n)

    def first_peer(d):
        return (dp, lax.rem(first + d, n) * far + second * near, tp)

    def second_peer(d):
        return (dp, first * far + lax.rem(second + d, n) * near, tp)

    sibling = (dp, kv, other)

    loads = [
        (tok_h, tok, 0),
        (pre_h, pre, 1),
        (qw_h, w4.at[0], 2),
        (kw_h, w4.at[1], 2),
        (vw_h, w4.at[2], 2),
        (ow_h, w4.at[3], 2),
        (ig_h, gates.at[0], 3),
        (fg_h, gates.at[1], 3),
        (cf_h, cfi.at[0], 4),
        (ci_h, cfi.at[1], 4),
        (len_h, lens, 5),
        (smax_h, smax, 6),
        (sm_h, state, 7),
        (sn_h, sn, 8),
        (ck_h, ckv.at[0], 9),
        (cv_h, ckv.at[1], 9),
        (hg_h, hg, 10),
        (mixw_h, mixw, 11),
        (mg_h, mg, 12),
        (gw_h, gud.at[0], 13),
        (uw_h, gud.at[1], 13),
        (dw_h, gud.at[2], 13),
    ]
    copies = [pltpu.make_async_copy(a, b, load_sem.at[k]) for a, b, k in loads]
    landed = [tok, pre, w4, gates, cfi, lens, smax, state, sn, ckv, hg, mixw, mg, gud]
    arrived = [pltpu.make_async_copy(r, r, load_sem.at[k]) for k, r in enumerate(landed)]
    for c in copies[:8]:
        c.start()
    barrier = pltpu.get_barrier_semaphore()
    for d in range(1, n):
        pl.semaphore_signal(barrier, inc=1, device_id=first_peer(d), device_id_type=MESH)
        pl.semaphore_signal(barrier, inc=1, device_id=second_peer(d), device_id_type=MESH)
        across = (dp, z * n + lax.rem(y + d, n), other)
        pl.semaphore_signal(barrier, inc=1, device_id=across, device_id_type=MESH)
    pl.semaphore_signal(barrier, inc=1, device_id=sibling, device_id_type=MESH)
    for c in copies[8:]:
        c.start()
    for c in arrived[:4]:
        c.wait()

    r = iota((seqs, seqs), 0)
    owner = (r // (2 * n)) * far + (r % n) * near
    perm = jnp.where(iota((seqs, seqs), 1) == owner * 2 + (r // n) % 2, 1.0, 0.0).astype(BF16)
    tokens = dot(perm, tok[...], 1, 1)
    squares = jnp.sum(tokens * tokens, axis=1, keepdims=True)
    normed = (tokens * pre[...]).astype(BF16)
    for k in range(KINDS):
        prod = dot(normed, w4[k]).astype(BF16)
        p1[:, :, k * cols : (k + 1) * cols] = prod.reshape(n, 2 * n, cols)
    lane0 = pl.multiple_of((kv // (128 // width)) * 128, 128)
    both = jnp.concatenate(
        [gates[0, :, pl.ds(lane0, 128)].astype(F32), gates[1, :, pl.ds(lane0, 128)].astype(F32)],
        axis=0,
    ).astype(BF16)
    at = (kv % (128 // width)) * width
    sel = jnp.where(iota((width, 128), 1) == iota((width, 128), 0) + at, 1.0, 0.0).astype(BF16)
    own_gates = dot(both, sel, 1, 1)
    own_gates = jnp.concatenate([own_gates, jnp.zeros((120, width), F32)], axis=0).astype(BF16)
    g = dot(normed, own_gates, 1, 1)
    g = jnp.where(iota((seqs, 128), 1) == 8, squares, g)
    p1[:, :, KINDS * cols :] = g.astype(BF16).reshape(n, 2 * n, 128)

    pl.semaphore_wait(barrier, 3 * (n - 1) + 1)

    def total(ref, send, recv):
        return pltpu.make_async_remote_copy(
            src_ref=ref,
            dst_ref=ref,
            send_sem=send,
            recv_sem=recv,
            device_id=sibling,
            device_id_type=MESH,
        )

    def send(src, dst, send_sem, recv_sem, peer):
        pltpu.make_async_remote_copy(
            src_ref=src,
            dst_ref=dst,
            send_sem=send_sem,
            recv_sem=recv_sem,
            device_id=peer,
            device_id_type=MESH,
        ).start()

    far_d = n // 2
    cut = (KINDS * blocks // 2 + 1) * 128
    parts = (pl.ds(0, cut), pl.ds(cut, wide - cut))

    def rows_for(d):
        return p1.at[lax.rem(first + d, n)]

    hops = (n - 1, 1)
    last_d = (far_d + 1, far_d - 1)
    slot = {d: k for k, d in enumerate(d for d in range(1, n) if d != far_d)}
    for k in range(2):
        part = rows_for(far_d).at[:, parts[k]]
        send(part, relay.at[:, parts[k]], sr, vr.at[k], first_peer(hops[k]))
    for k in range(2):
        d, own_part = last_d[k], parts[1 - k]
        send(rows_for(d).at[:, own_part], r1.at[slot[d], :, own_part], s1, v1, first_peer(d))
    direct = [d for d in order if d != far_d and d not in last_d]
    for d in direct:
        if d not in hops:
            send(rows_for(d), r1.at[slot[d]], s1, v1, first_peer(d))

    for c in arrived[4:]:
        c.wait()
    row64 = iota((8, ckv.shape[2]), 0)
    lane64 = iota((8, ckv.shape[2]), 1)
    zero4 = jnp.zeros((4, ckv.shape[2]), F32)
    forget = jnp.concatenate([cfi[0, 0], cfi[0, 1], zero4], axis=0)
    gain_in = jnp.concatenate([cfi[1, 0], cfi[1, 1], zero4], axis=0)
    length = jnp.where(row64 < 2, lens[0], lens[1])
    live = lane64 < length
    forget = jnp.where(live, forget, 0.0)
    span = ckv.shape[2]
    tri = jnp.where(iota((span, span), 0) <= iota((span, span), 1), 1.0, 0.0)
    running = dot(forget, tri, precision=lax.Precision.HIGHEST)
    run_last = jnp.sum(forget, axis=1, keepdims=True)
    base = jnp.where(live, run_last - running + gain_in, -jnp.inf)
    base = jnp.where(row64 < 4, base, 0.0)
    base_max = jnp.max(base, axis=1, keepdims=True)
    row1 = iota((8, 1), 0)
    state_top = jnp.where(
        row1 == 0,
        smax[0, 0],
        jnp.where(row1 == 1, smax[0, 1], jnp.where(row1 == 2, smax[1, 0], smax[1, 1])),
    )
    state_base = run_last + state_top
    for i in range(2):
        for h in range(2):
            whole = state[i, h]
            high = whole.astype(BF16)
            split[0, 2 * i + h] = high
            split[1, 2 * i + h] = (whole - high.astype(F32)).astype(BF16)
    size = sn.shape[2]
    zero_rows = jnp.zeros((4, size), F32)
    norm8 = jnp.concatenate([sn[0], sn[1], zero_rows], axis=0)
    halves = [hg[:, :size], hg[:, size:]]
    gain8 = jnp.concatenate(halves + halves + [zero_rows], axis=0)
    pr = iota((8 * n, 8 * n), 0)
    pc = iota((8 * n, 8 * n), 1)
    seq, hu = pr % (2 * n), pr // (2 * n)
    target = (seq // 2) * 8 + (hu % 2) * 4 + (seq % 2) * 2 + hu // 2
    pick[...] = jnp.where(pc == target, 1.0, 0.0).astype(BF16)
    hidden_cols = gud.shape[1]
    line = n * width
    c1 = iota((line, line), 1)
    source = ((c1 % (line // 2)) // (width // 2)) * width
    source = source + (c1 // (line // 2)) * (width // 2) + c1 % (width // 2)
    compress = jnp.where(iota((line, line), 0) == source, 1.0, 0.0).astype(BF16)
    pad = jnp.zeros((HIDDEN_PAD - hidden_cols, line), F32)
    for k in range(n):
        at = slice(k * line, (k + 1) * line)
        gain = mg[:, at]
        block = [(gud[u, :, at].astype(F32) * gain) for u in range(2)]
        block = jnp.concatenate([block[0], pad, block[1], pad], axis=0).astype(BF16)
        block = dot(block, compress).astype(BF16)
        for u in range(2):
            to = (u * n + k) * (line // 2)
            gu[:, to : to + line // 2] = block[:, u * (line // 2) : (u + 1) * (line // 2)]
    group = 128 // width

    def arrange(b, carry):
        block = gud[2, :, pl.ds(pl.multiple_of(b * 128, 128), 128)].astype(F32)
        block = jnp.concatenate([block, jnp.zeros((HIDDEN_PAD - hidden_cols, 128), F32)], axis=0)
        block = block.T.astype(BF16)
        for k in range(group):
            at_kv = b * group + k
            mirrored = (at_kv % n) * n + at_kv // n
            half = width // 2
            dt[0, at_kv] = block[k * width : k * width + half]
            dt[1, mirrored] = block[k * width + half : (k + 1) * width]
        return carry

    lax.fori_loop(0, kvs // group, arrange, 0)

    for k in range(2):
        d = last_d[k]
        total(relay.at[:, parts[k]], sr, vr.at[k]).wait_recv()
        mine = p1[lax.rem(first + d, n), :, parts[k]].astype(F32)
        merged[:, parts[k]] = (mine + relay[:, parts[k]].astype(F32)).astype(BF16)
        send(merged.at[:, parts[k]], r1.at[slot[d], :, parts[k]], s1, v1, first_peer(d))
    for d in direct:
        if d in hops:
            send(rows_for(d), r1.at[slot[d]], s1, v1, first_peer(d))
    half = width // 2
    own_rows = pl.ds(pl.multiple_of(tp * half, half), half)
    rest = pl.ds(pl.multiple_of(other * half, half), half)

    def share_weights():
        for d in order:
            along_y = z * n + lax.rem(y + d, n)
            send(tok.at[own_rows], tg.at[y], st, vt, (dp, along_y, tp))
            send(mixw.at[own_rows], wg.at[tp, y], sw, vw, (dp, along_y, tp))
            send(mixw.at[rest], wg.at[tp, y], sw, vw, (dp, along_y, other))
        send(mixw.at[rest], wg.at[tp, y], sw, vw, sibling)

    @pl.when(tp == 1)
    def _():
        share_weights()

    own = p1[first].astype(F32)
    total(r1, s1, v1).wait_recv()
    for k in range(n - 2):
        own = own + r1[k].astype(F32)
    q2f[...] = jnp.zeros_like(q2f)
    for i in range(2):
        part = own[i * n : (i + 1) * n]
        for c in range(KINDS * blocks):
            kind, h, u = c // blocks, (c % blocks) // 2, c % 2
            q2f[pl.ds(kind * 8 + u * 4 + i * 2 + h, n, stride=ROWS), :] = part[
                :, c * 128 : (c + 1) * 128
            ]
        for h in range(2):
            q2f[pl.ds(32 + i * 2 + h, n, stride=ROWS), :] = part[:, KINDS * cols :]
    q2b[...] = q2f[...].reshape(n, ROWS, 128).astype(BF16)
    for d in order:
        send(q2b.at[lax.rem(second + d, n)], r2.at[d - 1], s2, v2, second_peer(d))
    @pl.when(tp == 0)
    def _():
        share_weights()

    wg[tp, y] = mixw[own_rows, :]
    tg[y] = tok[own_rows, :]
    mine = q2f[pl.ds(pl.multiple_of(second * ROWS, 8), ROWS), :]
    total(r2, s2, v2).wait_recv()
    for k in range(n - 1):
        mine = mine + r2[k].astype(F32)

    def heads(kind):
        a = mine[kind * 8 : kind * 8 + 4]
        b = mine[kind * 8 + 4 : kind * 8 + 8]
        return jnp.concatenate([jnp.concatenate([a, b], axis=1), zero_rows], axis=0)

    gate8 = mine[32:40]
    lane = iota((8, 128), 1)
    row = iota((8, 128), 0)
    square = jnp.sum(jnp.where(lane == 8, gate8, 0.0), axis=1, keepdims=True)
    in_sum = jnp.sum(jnp.where(lane == 2 * tp + row % 2, gate8, 0.0), axis=1, keepdims=True)
    fg_sum = jnp.sum(jnp.where(lane == 4 + 2 * tp + row % 2, gate8, 0.0), axis=1, keepdims=True)
    scale = lax.rsqrt(square / model + EPS)
    query = (scale * heads(0)).astype(BF16).astype(F32)
    key_new = (scale * heads(1)).astype(BF16).astype(F32)
    value_new = (scale * heads(2)).astype(BF16).astype(F32)
    outgate = (scale * heads(3)).astype(BF16).astype(F32)
    in_gate = scale * in_sum
    fg = scale * fg_sum
    forget_new = jnp.minimum(fg, 0.0) - jnp.log1p(jnp.exp(-jnp.abs(fg)))
    weight_log = base + forget_new
    state_log = state_base + forget_new
    peak = jnp.maximum(jnp.maximum(state_log, in_gate), base_max + forget_new)
    query = query * (size**-0.5)
    rows = iota((8, size), 0)
    alone = [jnp.where(rows == k, query, 0.0) for k in range(4)]
    dots = dot(jnp.concatenate(alone[0:2], axis=1).astype(BF16), ckv[0, 0], 1, 1)
    dots = dots + dot(jnp.concatenate(alone[2:4], axis=1).astype(BF16), ckv[0, 1], 1, 1)
    scores = jnp.exp(weight_log - peak) * dots
    self_score = jnp.exp(in_gate - peak) * jnp.sum(query * key_new, axis=1, keepdims=True)
    carried = jnp.exp(state_log - peak)
    read = dot(alone[0].astype(BF16), split[0, 0], 1, 1)
    read = read + dot(alone[0].astype(BF16), split[1, 0], 1, 1)
    for k in range(1, 4):
        read = read + dot(alone[k].astype(BF16), split[0, k], 1, 1)
        read = read + dot(alone[k].astype(BF16), split[1, k], 1, 1)
    norm_read = jnp.sum(norm8 * query, axis=1, keepdims=True)
    values = dot(jnp.where(row64 < 2, scores, 0.0).astype(BF16), ckv[1, 0])
    values = values + dot(jnp.where(row64 >= 2, scores, 0.0).astype(BF16), ckv[1, 1])
    values = jnp.where(rows % 2 == 0, values[:, :size], values[:, size:])
    numerator = carried * read + values + self_score * value_new
    denominator = carried * norm_read + jnp.sum(scores, axis=1, keepdims=True) + self_score
    hidden = numerator / jnp.maximum(jnp.abs(denominator), 1.0)
    mixed = hidden * gain8 * jax.nn.sigmoid(outgate)
    mh[tp, z] = jnp.concatenate([mixed[:4, :128], mixed[:4, 128:]], axis=0).astype(BF16)

    for d in order:
        along_z = lax.rem(z + d, n) * n + y
        for core in (tp, other):
            send(mh.at[tp, z], mh.at[tp, z], s3, v3, (dp, along_z, core))
    send(mh.at[tp, z], mh.at[tp, z], s3, v3, sibling)
    flat_w = wg.reshape(2 * n, half, cols)
    flat_m = mh.reshape(2 * n, 8, 128)
    all_wg = total(flat_w.at[pl.ds(0, 2 * n - 1)], sw, vw)
    all_tg = total(tg.at[pl.ds(0, n - 1)], st, vt)
    all_mh = total(flat_m.at[pl.ds(0, 2 * n - 1)], s3, v3)
    for c in (all_wg, all_tg, all_mh):
        c.wait_recv()

    def project(u):
        flat = mh[u].astype(F32).reshape(8 * n, 128).astype(BF16)
        picked = dot(pick[...], flat).astype(BF16)
        w = wg[u].reshape(n * half, cols)
        out = dot(picked[: 2 * n], w[:, :128], 1, 1)
        for k in range(1, 4):
            block = picked[2 * n * k : 2 * n * (k + 1)]
            out = out + dot(block, w[:, k * 128 : (k + 1) * 128], 1, 1)
        return out.astype(BF16).astype(F32)

    q = iota((2 * n, seqs), 0)
    here = jnp.where(iota((2 * n, seqs), 1) == ((q // 2) * n + y) * 2 + q % 2, 1.0, 0.0)
    own_tokens = dot(here.astype(BF16), tg[...].reshape(n * half, seqs), 1, 1)
    rbuf[...] = (own_tokens + (project(0) + project(1))).astype(BF16)

    rt[tp, z, y] = rbuf[...]
    rows_order = order + [0]
    for dz in rows_order:
        for dy in rows_order:
            if dz or dy:
                peer = lax.rem(z + dz, n) * n + lax.rem(y + dy, n)
                send(rbuf, rt.at[tp, z, y], s5, v5.at[dz], (dp, peer, tp))
    for dz in rows_order:
        count = n if dz else n - 1
        total(rt.at[0, 0, pl.ds(0, count)], s5, v5.at[dz]).wait_recv()
        source = lax.rem(z + n - dz, n)
        send(rt.at[tp, source], rt.at[tp, source], s6, v6, sibling)
    total(rt.at[0], s6, v6).wait_recv()

    lanes = n * half
    power = jnp.zeros((seqs, lanes), F32)
    acc = jnp.zeros((2 * HIDDEN_PAD, seqs), F32)
    for u in range(2):
        for k in range(0, n, 2):
            pair = [rt[u, k + e].reshape(seqs, lanes) for e in range(2)]
            at = (u * n + k) * lanes
            wide_pair = jnp.concatenate(pair, axis=1)
            acc = acc + dot(gu[:, at : at + 2 * lanes], wide_pair, 1, 1)
            for block in pair:
                spread = block.astype(F32)
                power = power + spread * spread
    power = dot(jnp.ones((8, lanes), F32), power, 1, 1, precision=lax.Precision.HIGHEST)[:1]
    scale_mid = lax.rsqrt(power / model + EPS)
    gate = scale_mid * acc[:HIDDEN_PAD]
    up = scale_mid * acc[HIDDEN_PAD:]
    units = (gate * jax.nn.sigmoid(gate) * up).astype(BF16)

    other_first = y + (z - y) * tp
    steps = order + [0]
    whole = dot(dt[other].reshape(kvs * half, HIDDEN_PAD), units)
    xo[...] = whole.astype(BF16).reshape(n, n * half, seqs)
    for k, d in enumerate(steps):
        send(xo.at[lax.rem(other_first + d, n)], xi.at[k], s7, v7.at[k], sibling)
    p5[...] = dot(dt[tp].reshape(kvs * half, HIDDEN_PAD), units).reshape(n, n * half, seqs)
    for k, d in enumerate(steps):
        total(xi.at[k], s7, v7.at[k]).wait_recv()
        at_f = lax.rem(first + d, n)
        both = p5[at_f] + xi[k].astype(F32)
        p5b[k] = both.astype(BF16).reshape(n, half, seqs)
        if d == 0:
            p5[at_f] = both
        for e in steps:
            if d or e:
                at_s = lax.rem(second + e, n)
                peer = (dp, at_f * far + at_s * near, tp)
                send(p5b.at[k, at_s], r3.at[d * n + e - 1], s8, v8, peer)
    mine_at = jnp.where(iota((half, lanes), 1) == iota((half, lanes), 0) + y * half, 1.0, 0.0)
    last = dot(mine_at.astype(BF16), rt[tp, z].reshape(seqs, lanes), 1, 1)
    last = last + p5[first, pl.ds(pl.multiple_of(second * half, half), half), :]
    c2 = iota((seqs, seqs), 1)
    back = ((c2 // 2) % n) * 2 * n + (c2 // (2 * n)) * 2 + c2 % 2
    back = jnp.where(iota((seqs, seqs), 0) == back, 1.0, 0.0).astype(BF16)
    total(r3, s8, v8).wait_recv()
    last = last + jnp.sum(r3[...].astype(F32), axis=0)
    out_ref[...] = dot(last.astype(BF16), back).astype(BF16)

    total(relay, sr, vr.at[0]).wait_send()
    total(r1, s1, v1).wait_send()
    total(r2, s2, v2).wait_send()
    for c in (all_wg, all_tg, all_mh):
        c.wait_send()
    flat_r = rt.reshape(2 * kvs, 2 * n, lanes)
    total(flat_r.at[pl.ds(0, kvs - 1)], s5, v5.at[0]).wait_send()
    total(rt.at[0], s6, v6).wait_send()
    total(xi, s7, v7.at[0]).wait_send()
    total(r3, s8, v8).wait_send()


def per_device(n, *args):
    (tokens, pre, qw, kw, vw, ow, ig, fg, ck, cv, ci, cf, lens, sm, sn, smax) = args[:16]
    hg, mixw, mg, gw, uw, dw = args[16:]
    operands = (
        tokens.T,
        pre.reshape(1, -1),
        qw,
        kw,
        vw,
        ow,
        ig.T,
        fg.T,
        ck,
        cv,
        ci.transpose(0, 2, 1),
        cf.transpose(0, 2, 1),
        lens,
        sm,
        sn,
        smax,
        hg.reshape(1, -1),
        mixw.T,
        mg.reshape(1, -1),
        gw.T,
        uw.T,
        dw,
    )
    seqs, width = tokens.shape
    cols = qw.shape[1]
    kvs = n * n
    model = width * kvs
    span, size = ck.shape[1], sn.shape[2]
    wide = KINDS * cols + 128
    half = width // 2
    dma = pltpu.SemaphoreType.DMA
    vmem = pltpu.VMEM
    ff = gw.shape[1]
    scratch = [
        vmem((width, seqs), BF16),
        vmem((1, width), F32),
        vmem((KINDS, width, cols), BF16),
        vmem((2, 4, model), BF16),
        vmem((2, 2, 2, span), F32),
        pltpu.SMEM((2,), jnp.int32),
        pltpu.SMEM((2, 2), F32),
        vmem((2, 2, size, size), F32),
        vmem((2, 2, size), F32),
        vmem((2, 2, span, cols), BF16),
        vmem((1, cols), F32),
        vmem((width, cols), BF16),
        vmem((1, model), F32),
        vmem((3, ff, model), BF16),
        dma((14,)),
        vmem((n, 2 * n, wide), BF16),
        vmem((n - 2, 2 * n, wide), BF16),
        vmem((2 * n, wide), BF16),
        vmem((2 * n, wide), BF16),
        vmem((n * ROWS, 128), F32),
        vmem((n, ROWS, 128), BF16),
        vmem((n - 1, ROWS, 128), BF16),
        vmem((2, 4, size, size), BF16),
        vmem((8 * n, 8 * n), BF16),
        vmem((2, n, 8, 128), BF16),
        vmem((2, n, half, cols), BF16),
        vmem((n, half, seqs), BF16),
        vmem((2 * n, n * half), BF16),
        vmem((2, n, n, 2 * n, n * half), BF16),
        vmem((2 * HIDDEN_PAD, model), BF16),
        vmem((2, kvs, half, HIDDEN_PAD), BF16),
        vmem((n, n * half, seqs), BF16),
        vmem((n, n * half, seqs), BF16),
        vmem((n, n * half, seqs), F32),
        vmem((n, n, half, seqs), BF16),
        vmem((kvs - 1, half, seqs), BF16),
        dma,
        dma,
        dma,
        dma((2,)),
        dma,
        dma,
        dma,
        dma,
        dma,
        dma,
        dma,
        dma,
        dma,
        dma((n,)),
        dma,
        dma,
        dma,
        dma((n,)),
        dma,
        dma,
    ]
    out = pl.pallas_call(
        functools.partial(kernel, n),
        out_shape=jax.ShapeDtypeStruct((half, seqs), BF16),
        in_specs=[pl.BlockSpec(memory_space=pl.ANY)] * len(operands),
        out_specs=pl.BlockSpec(memory_space=pltpu.VMEM),
        scratch_shapes=scratch,
        compiler_params=pltpu.CompilerParams(
            collective_id=0, has_side_effects=True, vmem_limit_bytes=24 * 1024 * 1024
        ),
        name="layer",
    )(*[pltpu.with_memory_space_constraint(o, pltpu.HBM) for o in operands])
    return out.T


def solution(mesh):
    n = round(mesh.shape["kv"] ** 0.5)
    seq = ("dp", "kv")
    return jax.shard_map(
        functools.partial(per_device, n),
        mesh=mesh,
        in_specs=(
            P("dp", "kv"),
            P("kv"),
            P("kv", "tp"),
            P("kv", "tp"),
            P("kv", "tp"),
            P("kv", "tp"),
            P(),
            P(),
            P(seq, None, "tp"),
            P(seq, None, "tp"),
            P(seq, None, "tp"),
            P(seq, None, "tp"),
            P(seq),
            P(seq, "tp", None, None),
            P(seq, "tp", None),
            P(seq, "tp"),
            P("tp"),
            P("tp", "kv"),
            P(),
            P(None, ("kv", "tp")),
            P(None, ("kv", "tp")),
            P(("kv", "tp"), None),
        ),
        out_specs=P("dp", ("kv", "tp")),
        check_vma=False,
    )
```

```python
import functools

import jax
import jax.numpy as jnp
from jax import lax
from jax.experimental import pallas as pl
from jax.experimental.pallas import tpu as pltpu
from jax.sharding import PartitionSpec as P

EPS = 1e-06
MESH = pl.DeviceIdType.MESH
F32 = jnp.float32
BF16 = jnp.bfloat16
KINDS = 4
ROWS = 40
HIDDEN_PAD = 48


def ring_order(n):
    return sorted(range(1, n), key=lambda d: (-min(d, n - d), d))


def dot(a, b, ca=1, cb=0, precision=None):
    return lax.dot_general(
        a, b, (((ca,), (cb,)), ((), ())), preferred_element_type=F32, precision=precision
    )


def iota(shape, dim):
    return lax.broadcasted_iota(jnp.int32, shape, dim)


def kernel(
    n,
    tok_h,
    pre_h,
    qw_h,
    kw_h,
    vw_h,
    ow_h,
    ig_h,
    fg_h,
    ck_h,
    cv_h,
    ci_h,
    cf_h,
    len_h,
    sm_h,
    sn_h,
    smax_h,
    hg_h,
    mixw_h,
    mg_h,
    gw_h,
    uw_h,
    dw_h,
    out_ref,
    tok,
    pre,
    w4,
    gates,
    cfi,
    lens,
    smax,
    state,
    sn,
    ckv,
    hg,
    mixw,
    mg,
    gud,
    load_sem,
    p1,
    r1,
    relay,
    merged,
    q2f,
    q2b,
    r2,
    split,
    pick,
    mh,
    wg,
    tg,
    rbuf,
    rt,
    gu,
    dt,
    dts,
    dtc,
    p5,
    p5b,
    r3,
    s1,
    v1,
    sr,
    vr,
    s2,
    v2,
    sw,
    vw,
    st,
    vt,
    s3,
    v3,
    s5,
    v5,
    s6,
    v6,
    sg,
    vg,
    sd,
    vd,
    s8,
    v8,
):
    kvs = n * n
    width = tok.shape[0]
    seqs = tok.shape[1]
    cols = w4.shape[2]
    wide = p1.shape[2]
    blocks = cols // 128
    model = width * kvs
    dp = lax.axis_index("dp")
    kv = lax.axis_index("kv")
    tp = lax.axis_index("tp")
    z, y = kv // n, kv % n
    far = n - (n - 1) * tp
    near = 1 + (n - 1) * tp
    first = z + (y - z) * tp
    second = y + (z - y) * tp
    other = 1 - tp
    order = ring_order(n)

    def first_peer(d):
        return (dp, lax.rem(first + d, n) * far + second * near, tp)

    def second_peer(d):
        return (dp, first * far + lax.rem(second + d, n) * near, tp)

    sibling = (dp, kv, other)

    loads = [
        (tok_h, tok, 0),
        (pre_h, pre, 1),
        (qw_h, w4.at[0], 2),
        (kw_h, w4.at[1], 2),
        (vw_h, w4.at[2], 2),
        (ow_h, w4.at[3], 2),
        (ig_h, gates.at[0], 3),
        (fg_h, gates.at[1], 3),
        (cf_h, cfi.at[0], 4),
        (ci_h, cfi.at[1], 4),
        (len_h, lens, 5),
        (smax_h, smax, 6),
        (sm_h, state, 7),
        (sn_h, sn, 8),
        (ck_h, ckv.at[0], 9),
        (cv_h, ckv.at[1], 9),
        (hg_h, hg, 10),
        (mixw_h, mixw, 11),
        (mg_h, mg, 12),
        (gw_h, gud.at[0], 13),
        (uw_h, gud.at[1], 13),
        (dw_h, gud.at[2], 13),
    ]
    copies = [pltpu.make_async_copy(a, b, load_sem.at[k]) for a, b, k in loads]
    landed = [tok, pre, w4, gates, cfi, lens, smax, state, sn, ckv, hg, mixw, mg, gud]
    arrived = [pltpu.make_async_copy(r, r, load_sem.at[k]) for k, r in enumerate(landed)]
    for c in copies[:8]:
        c.start()
    barrier = pltpu.get_barrier_semaphore()
    for d in range(1, n):
        pl.semaphore_signal(barrier, inc=1, device_id=first_peer(d), device_id_type=MESH)
        pl.semaphore_signal(barrier, inc=1, device_id=second_peer(d), device_id_type=MESH)
        across = (dp, z * n + lax.rem(y + d, n), other)
        pl.semaphore_signal(barrier, inc=1, device_id=across, device_id_type=MESH)
    pl.semaphore_signal(barrier, inc=1, device_id=sibling, device_id_type=MESH)
    for c in copies[8:]:
        c.start()
    for c in arrived[:4]:
        c.wait()

    r = iota((seqs, seqs), 0)
    owner = (r // (2 * n)) * far + (r % n) * near
    perm = jnp.where(iota((seqs, seqs), 1) == owner * 2 + (r // n) % 2, 1.0, 0.0).astype(BF16)
    tokens = dot(perm, tok[...], 1, 1)
    squares = jnp.sum(tokens * tokens, axis=1, keepdims=True)
    normed = (tokens * pre[...]).astype(BF16)
    for k in range(KINDS):
        prod = dot(normed, w4[k]).astype(BF16)
        p1[:, :, k * cols : (k + 1) * cols] = prod.reshape(n, 2 * n, cols)
    lane0 = pl.multiple_of((kv // (128 // width)) * 128, 128)
    both = jnp.concatenate(
        [gates[0, :, pl.ds(lane0, 128)].astype(F32), gates[1, :, pl.ds(lane0, 128)].astype(F32)],
        axis=0,
    ).astype(BF16)
    at = (kv % (128 // width)) * width
    sel = jnp.where(iota((width, 128), 1) == iota((width, 128), 0) + at, 1.0, 0.0).astype(BF16)
    own_gates = dot(both, sel, 1, 1)
    own_gates = jnp.concatenate([own_gates, jnp.zeros((120, width), F32)], axis=0).astype(BF16)
    g = dot(normed, own_gates, 1, 1)
    g = jnp.where(iota((seqs, 128), 1) == 8, squares, g)
    p1[:, :, KINDS * cols :] = g.astype(BF16).reshape(n, 2 * n, 128)

    pl.semaphore_wait(barrier, 3 * (n - 1) + 1)

    def total(ref, send, recv):
        return pltpu.make_async_remote_copy(
            src_ref=ref,
            dst_ref=ref,
            send_sem=send,
            recv_sem=recv,
            device_id=sibling,
            device_id_type=MESH,
        )

    def send(src, dst, send_sem, recv_sem, peer):
        pltpu.make_async_remote_copy(
            src_ref=src,
            dst_ref=dst,
            send_sem=send_sem,
            recv_sem=recv_sem,
            device_id=peer,
            device_id_type=MESH,
        ).start()

    far_d = n // 2
    cut = (KINDS * blocks // 2 + 1) * 128
    parts = (pl.ds(0, cut), pl.ds(cut, wide - cut))

    def rows_for(d):
        return p1.at[lax.rem(first + d, n)]

    hops = (n - 1, 1)
    last_d = (far_d + 1, far_d - 1)
    slot = {d: k for k, d in enumerate(d for d in range(1, n) if d != far_d)}
    for k in range(2):
        part = rows_for(far_d).at[:, parts[k]]
        send(part, relay.at[:, parts[k]], sr, vr.at[k], first_peer(hops[k]))
    for k in range(2):
        d, own_part = last_d[k], parts[1 - k]
        send(rows_for(d).at[:, own_part], r1.at[slot[d], :, own_part], s1, v1, first_peer(d))
    direct = [d for d in order if d != far_d and d not in last_d]
    for d in direct:
        if d not in hops:
            send(rows_for(d), r1.at[slot[d]], s1, v1, first_peer(d))

    for c in arrived[4:]:
        c.wait()
    row64 = iota((8, ckv.shape[2]), 0)
    lane64 = iota((8, ckv.shape[2]), 1)
    zero4 = jnp.zeros((4, ckv.shape[2]), F32)
    forget = jnp.concatenate([cfi[0, 0], cfi[0, 1], zero4], axis=0)
    gain_in = jnp.concatenate([cfi[1, 0], cfi[1, 1], zero4], axis=0)
    length = jnp.where(row64 < 2, lens[0], lens[1])
    live = lane64 < length
    forget = jnp.where(live, forget, 0.0)
    span = ckv.shape[2]
    tri = jnp.where(iota((span, span), 0) <= iota((span, span), 1), 1.0, 0.0)
    running = dot(forget, tri, precision=lax.Precision.HIGHEST)
    run_last = jnp.sum(forget, axis=1, keepdims=True)
    base = jnp.where(live, run_last - running + gain_in, -jnp.inf)
    base = jnp.where(row64 < 4, base, 0.0)
    base_max = jnp.max(base, axis=1, keepdims=True)
    row1 = iota((8, 1), 0)
    state_top = jnp.where(
        row1 == 0,
        smax[0, 0],
        jnp.where(row1 == 1, smax[0, 1], jnp.where(row1 == 2, smax[1, 0], smax[1, 1])),
    )
    state_base = run_last + state_top
    for i in range(2):
        for h in range(2):
            whole = state[i, h]
            high = whole.astype(BF16)
            split[0, 2 * i + h] = high
            split[1, 2 * i + h] = (whole - high.astype(F32)).astype(BF16)
    size = sn.shape[2]
    zero_rows = jnp.zeros((4, size), F32)
    norm8 = jnp.concatenate([sn[0], sn[1], zero_rows], axis=0)
    halves = [hg[:, :size], hg[:, size:]]
    gain8 = jnp.concatenate(halves + halves + [zero_rows], axis=0)
    pr = iota((8 * n, 8 * n), 0)
    pc = iota((8 * n, 8 * n), 1)
    seq, hu = pr % (2 * n), pr // (2 * n)
    target = (seq // 2) * 8 + (hu % 2) * 4 + (seq % 2) * 2 + hu // 2
    pick[...] = jnp.where(pc == target, 1.0, 0.0).astype(BF16)
    hidden_cols = gud.shape[1]
    line = n * width
    c1 = iota((line, line), 1)
    source = ((c1 % (line // 2)) // (width // 2)) * width
    source = source + (c1 // (line // 2)) * (width // 2) + c1 % (width // 2)
    compress = jnp.where(iota((line, line), 0) == source, 1.0, 0.0).astype(BF16)
    pad = jnp.zeros((HIDDEN_PAD - hidden_cols, line), F32)
    for k in range(n):
        at = slice(k * line, (k + 1) * line)
        gain = mg[:, at]
        block = [(gud[u, :, at].astype(F32) * gain) for u in range(2)]
        block = jnp.concatenate([block[0], pad, block[1], pad], axis=0).astype(BF16)
        block = dot(block, compress).astype(BF16)
        for u in range(2):
            to = (u * n + k) * (line // 2)
            gu[tp, :, to : to + line // 2] = block[:, u * (line // 2) : (u + 1) * (line // 2)]
    group = 128 // width

    def arrange(b, carry):
        block = gud[2, :, pl.ds(pl.multiple_of(b * 128, 128), 128)].astype(F32)
        block = jnp.concatenate([block, jnp.zeros((HIDDEN_PAD - hidden_cols, 128), F32)], axis=0)
        block = block.T.astype(BF16)
        for k in range(group):
            at_kv = b * group + k
            mirrored = (at_kv % n) * n + at_kv // n
            half = width // 2
            dt[0, at_kv] = block[k * width : k * width + half]
            dt[1, mirrored] = block[k * width + half : (k + 1) * width]
        return carry

    lax.fori_loop(0, kvs // group, arrange, 0)
    send(gu.at[tp], gu.at[tp], sg, vg, sibling)
    send(dt.at[other], dts, sd, vd, sibling)

    for k in range(2):
        d = last_d[k]
        total(relay.at[:, parts[k]], sr, vr.at[k]).wait_recv()
        mine = p1[lax.rem(first + d, n), :, parts[k]].astype(F32)
        merged[:, parts[k]] = (mine + relay[:, parts[k]].astype(F32)).astype(BF16)
        send(merged.at[:, parts[k]], r1.at[slot[d], :, parts[k]], s1, v1, first_peer(d))
    for d in direct:
        if d in hops:
            send(rows_for(d), r1.at[slot[d]], s1, v1, first_peer(d))
    half = width // 2
    own_rows = pl.ds(pl.multiple_of(tp * half, half), half)
    rest = pl.ds(pl.multiple_of(other * half, half), half)

    def share_weights():
        for d in order:
            along_y = z * n + lax.rem(y + d, n)
            send(tok.at[own_rows], tg.at[y], st, vt, (dp, along_y, tp))
            send(mixw.at[own_rows], wg.at[tp, y], sw, vw, (dp, along_y, tp))
            send(mixw.at[rest], wg.at[tp, y], sw, vw, (dp, along_y, other))
        send(mixw.at[rest], wg.at[tp, y], sw, vw, sibling)

    @pl.when(tp == 1)
    def _():
        share_weights()

    own = p1[first].astype(F32)
    total(r1, s1, v1).wait_recv()
    for k in range(n - 2):
        own = own + r1[k].astype(F32)
    q2f[...] = jnp.zeros_like(q2f)
    for i in range(2):
        part = own[i * n : (i + 1) * n]
        for c in range(KINDS * blocks):
            kind, h, u = c // blocks, (c % blocks) // 2, c % 2
            q2f[pl.ds(kind * 8 + u * 4 + i * 2 + h, n, stride=ROWS), :] = part[
                :, c * 128 : (c + 1) * 128
            ]
        for h in range(2):
            q2f[pl.ds(32 + i * 2 + h, n, stride=ROWS), :] = part[:, KINDS * cols :]
    q2b[...] = q2f[...].reshape(n, ROWS, 128).astype(BF16)
    for d in order:
        send(q2b.at[lax.rem(second + d, n)], r2.at[d - 1], s2, v2, second_peer(d))
    @pl.when(tp == 0)
    def _():
        share_weights()

    wg[tp, y] = mixw[own_rows, :]
    tg[y] = tok[own_rows, :]
    total(dts, sd, vd).wait_recv()
    half_dt = [dt[tp].reshape(kvs * half, HIDDEN_PAD), dts[...].reshape(kvs * half, HIDDEN_PAD)]
    half_dt = [jnp.where(tp == c, half_dt[0], half_dt[1]) for c in range(2)]
    dtc[...] = jnp.concatenate(half_dt, axis=1)
    mine = q2f[pl.ds(pl.multiple_of(second * ROWS, 8), ROWS), :]
    total(r2, s2, v2).wait_recv()
    for k in range(n - 1):
        mine = mine + r2[k].astype(F32)

    def heads(kind):
        a = mine[kind * 8 : kind * 8 + 4]
        b = mine[kind * 8 + 4 : kind * 8 + 8]
        return jnp.concatenate([jnp.concatenate([a, b], axis=1), zero_rows], axis=0)

    gate8 = mine[32:40]
    lane = iota((8, 128), 1)
    row = iota((8, 128), 0)
    square = jnp.sum(jnp.where(lane == 8, gate8, 0.0), axis=1, keepdims=True)
    in_sum = jnp.sum(jnp.where(lane == 2 * tp + row % 2, gate8, 0.0), axis=1, keepdims=True)
    fg_sum = jnp.sum(jnp.where(lane == 4 + 2 * tp + row % 2, gate8, 0.0), axis=1, keepdims=True)
    scale = lax.rsqrt(square / model + EPS)
    query = (scale * heads(0)).astype(BF16).astype(F32)
    key_new = (scale * heads(1)).astype(BF16).astype(F32)
    value_new = (scale * heads(2)).astype(BF16).astype(F32)
    outgate = (scale * heads(3)).astype(BF16).astype(F32)
    in_gate = scale * in_sum
    fg = scale * fg_sum
    forget_new = jnp.minimum(fg, 0.0) - jnp.log1p(jnp.exp(-jnp.abs(fg)))
    weight_log = base + forget_new
    state_log = state_base + forget_new
    peak = jnp.maximum(jnp.maximum(state_log, in_gate), base_max + forget_new)
    query = query * (size**-0.5)
    rows = iota((8, size), 0)
    alone = [jnp.where(rows == k, query, 0.0) for k in range(4)]
    dots = dot(jnp.concatenate(alone[0:2], axis=1).astype(BF16), ckv[0, 0], 1, 1)
    dots = dots + dot(jnp.concatenate(alone[2:4], axis=1).astype(BF16), ckv[0, 1], 1, 1)
    scores = jnp.exp(weight_log - peak) * dots
    self_score = jnp.exp(in_gate - peak) * jnp.sum(query * key_new, axis=1, keepdims=True)
    carried = jnp.exp(state_log - peak)
    read = dot(alone[0].astype(BF16), split[0, 0], 1, 1)
    read = read + dot(alone[0].astype(BF16), split[1, 0], 1, 1)
    for k in range(1, 4):
        read = read + dot(alone[k].astype(BF16), split[0, k], 1, 1)
        read = read + dot(alone[k].astype(BF16), split[1, k], 1, 1)
    norm_read = jnp.sum(norm8 * query, axis=1, keepdims=True)
    values = dot(jnp.where(row64 < 2, scores, 0.0).astype(BF16), ckv[1, 0])
    values = values + dot(jnp.where(row64 >= 2, scores, 0.0).astype(BF16), ckv[1, 1])
    values = jnp.where(rows % 2 == 0, values[:, :size], values[:, size:])
    numerator = carried * read + values + self_score * value_new
    denominator = carried * norm_read + jnp.sum(scores, axis=1, keepdims=True) + self_score
    hidden = numerator / jnp.maximum(jnp.abs(denominator), 1.0)
    mixed = hidden * gain8 * jax.nn.sigmoid(outgate)
    mh[tp, z] = jnp.concatenate([mixed[:4, :128], mixed[:4, 128:]], axis=0).astype(BF16)

    for d in order:
        along_z = lax.rem(z + d, n) * n + y
        for core in (tp, other):
            send(mh.at[tp, z], mh.at[tp, z], s3, v3, (dp, along_z, core))
    send(mh.at[tp, z], mh.at[tp, z], s3, v3, sibling)
    flat_w = wg.reshape(2 * n, half, cols)
    flat_m = mh.reshape(2 * n, 8, 128)
    all_wg = total(flat_w.at[pl.ds(0, 2 * n - 1)], sw, vw)
    all_tg = total(tg.at[pl.ds(0, n - 1)], st, vt)
    all_mh = total(flat_m.at[pl.ds(0, 2 * n - 1)], s3, v3)
    for c in (all_wg, all_tg, all_mh):
        c.wait_recv()

    def project(u):
        flat = mh[u].astype(F32).reshape(8 * n, 128).astype(BF16)
        picked = dot(pick[...], flat).astype(BF16)
        w = wg[u].reshape(n * half, cols)
        out = dot(picked[: 2 * n], w[:, :128], 1, 1)
        for k in range(1, 4):
            block = picked[2 * n * k : 2 * n * (k + 1)]
            out = out + dot(block, w[:, k * 128 : (k + 1) * 128], 1, 1)
        return out.astype(BF16).astype(F32)

    q = iota((2 * n, seqs), 0)
    here = jnp.where(iota((2 * n, seqs), 1) == ((q // 2) * n + y) * 2 + q % 2, 1.0, 0.0)
    own_tokens = dot(here.astype(BF16), tg[...].reshape(n * half, seqs), 1, 1)
    rbuf[...] = (own_tokens + (project(0) + project(1))).astype(BF16)

    rt[tp, z, y] = rbuf[...]
    rows_order = order + [0]
    for dz in rows_order:
        for dy in rows_order:
            if dz or dy:
                peer = lax.rem(z + dz, n) * n + lax.rem(y + dy, n)
                send(rbuf, rt.at[tp, z, y], s5, v5.at[dz], (dp, peer, tp))
    for dz in rows_order:
        count = n if dz else n - 1
        total(rt.at[0, 0, pl.ds(0, count)], s5, v5.at[dz]).wait_recv()
        source = lax.rem(z + n - dz, n)
        send(rt.at[tp, source], rt.at[tp, source], s6, v6, sibling)
    total(rt.at[0], s6, v6).wait_recv()

    lanes = n * half
    power = jnp.zeros((seqs, lanes), F32)
    acc = jnp.zeros((4 * HIDDEN_PAD, seqs), F32)
    total(gu.at[0], sg, vg).wait_recv()
    for u in range(2):
        for k in range(0, n, 2):
            pair = [rt[u, k + e].reshape(seqs, lanes) for e in range(2)]
            at = (u * n + k) * lanes
            wide_pair = jnp.concatenate(pair, axis=1)
            both = gu[:, :, at : at + 2 * lanes].reshape(4 * HIDDEN_PAD, 2 * lanes)
            acc = acc + dot(both, wide_pair, 1, 1)
            for block in pair:
                spread = block.astype(F32)
                power = power + spread * spread
    power = dot(jnp.ones((8, lanes), F32), power, 1, 1, precision=lax.Precision.HIGHEST)[:1]
    scale_mid = lax.rsqrt(power / model + EPS)
    acc = scale_mid * acc
    units = []
    for c in range(2):
        gate = acc[2 * c * HIDDEN_PAD : (2 * c + 1) * HIDDEN_PAD]
        up = acc[(2 * c + 1) * HIDDEN_PAD : (2 * c + 2) * HIDDEN_PAD]
        units.append(gate * jax.nn.sigmoid(gate) * up)
    units = jnp.concatenate(units, axis=0).astype(BF16)

    steps = order + [0]
    sums = dot(dtc[...], units)
    p5b[...] = sums.astype(BF16).reshape(n, n, half, seqs)
    p5[...] = sums.reshape(n, n * half, seqs)
    for d in steps:
        at_f = lax.rem(first + d, n)
        for e in steps:
            if d or e:
                at_s = lax.rem(second + e, n)
                peer = (dp, at_f * far + at_s * near, tp)
                send(p5b.at[at_f, at_s], r3.at[d * n + e - 1], s8, v8, peer)
    mine_at = jnp.where(iota((half, lanes), 1) == iota((half, lanes), 0) + y * half, 1.0, 0.0)
    last = dot(mine_at.astype(BF16), rt[tp, z].reshape(seqs, lanes), 1, 1)
    last = last + p5[first, pl.ds(pl.multiple_of(second * half, half), half), :]
    c2 = iota((seqs, seqs), 1)
    back = ((c2 // 2) % n) * 2 * n + (c2 // (2 * n)) * 2 + c2 % 2
    back = jnp.where(iota((seqs, seqs), 0) == back, 1.0, 0.0).astype(BF16)
    total(r3, s8, v8).wait_recv()
    last = last + jnp.sum(r3[...].astype(F32), axis=0)
    out_ref[...] = dot(last.astype(BF16), back).astype(BF16)

    total(relay, sr, vr.at[0]).wait_send()
    total(r1, s1, v1).wait_send()
    total(r2, s2, v2).wait_send()
    for c in (all_wg, all_tg, all_mh):
        c.wait_send()
    flat_r = rt.reshape(2 * kvs, 2 * n, lanes)
    total(flat_r.at[pl.ds(0, kvs - 1)], s5, v5.at[0]).wait_send()
    total(rt.at[0], s6, v6).wait_send()
    total(gu.at[0], sg, vg).wait_send()
    total(dts, sd, vd).wait_send()
    total(r3, s8, v8).wait_send()


def per_device(n, *args):
    (tokens, pre, qw, kw, vw, ow, ig, fg, ck, cv, ci, cf, lens, sm, sn, smax) = args[:16]
    hg, mixw, mg, gw, uw, dw = args[16:]
    operands = (
        tokens.T,
        pre.reshape(1, -1),
        qw,
        kw,
        vw,
        ow,
        ig.T,
        fg.T,
        ck,
        cv,
        ci.transpose(0, 2, 1),
        cf.transpose(0, 2, 1),
        lens,
        sm,
        sn,
        smax,
        hg.reshape(1, -1),
        mixw.T,
        mg.reshape(1, -1),
        gw.T,
        uw.T,
        dw,
    )
    seqs, width = tokens.shape
    cols = qw.shape[1]
    kvs = n * n
    model = width * kvs
    span, size = ck.shape[1], sn.shape[2]
    wide = KINDS * cols + 128
    half = width // 2
    dma = pltpu.SemaphoreType.DMA
    vmem = pltpu.VMEM
    ff = gw.shape[1]
    scratch = [
        vmem((width, seqs), BF16),
        vmem((1, width), F32),
        vmem((KINDS, width, cols), BF16),
        vmem((2, 4, model), BF16),
        vmem((2, 2, 2, span), F32),
        pltpu.SMEM((2,), jnp.int32),
        pltpu.SMEM((2, 2), F32),
        vmem((2, 2, size, size), F32),
        vmem((2, 2, size), F32),
        vmem((2, 2, span, cols), BF16),
        vmem((1, cols), F32),
        vmem((width, cols), BF16),
        vmem((1, model), F32),
        vmem((3, ff, model), BF16),
        dma((14,)),
        vmem((n, 2 * n, wide), BF16),
        vmem((n - 2, 2 * n, wide), BF16),
        vmem((2 * n, wide), BF16),
        vmem((2 * n, wide), BF16),
        vmem((n * ROWS, 128), F32),
        vmem((n, ROWS, 128), BF16),
        vmem((n - 1, ROWS, 128), BF16),
        vmem((2, 4, size, size), BF16),
        vmem((8 * n, 8 * n), BF16),
        vmem((2, n, 8, 128), BF16),
        vmem((2, n, half, cols), BF16),
        vmem((n, half, seqs), BF16),
        vmem((2 * n, n * half), BF16),
        vmem((2, n, n, 2 * n, n * half), BF16),
        vmem((2, 2 * HIDDEN_PAD, model), BF16),
        vmem((2, kvs, half, HIDDEN_PAD), BF16),
        vmem((kvs, half, HIDDEN_PAD), BF16),
        vmem((kvs * half, 2 * HIDDEN_PAD), BF16),
        vmem((n, n * half, seqs), F32),
        vmem((n, n, half, seqs), BF16),
        vmem((kvs - 1, half, seqs), BF16),
        dma,
        dma,
        dma,
        dma((2,)),
        dma,
        dma,
        dma,
        dma,
        dma,
        dma,
        dma,
        dma,
        dma,
        dma((n,)),
        dma,
        dma,
        dma,
        dma,
        dma,
        dma,
        dma,
        dma,
    ]
    out = pl.pallas_call(
        functools.partial(kernel, n),
        out_shape=jax.ShapeDtypeStruct((half, seqs), BF16),
        in_specs=[pl.BlockSpec(memory_space=pl.ANY)] * len(operands),
        out_specs=pl.BlockSpec(memory_space=pltpu.VMEM),
        scratch_shapes=scratch,
        compiler_params=pltpu.CompilerParams(
            collective_id=0, has_side_effects=True, vmem_limit_bytes=24 * 1024 * 1024
        ),
        name="layer",
    )(*[pltpu.with_memory_space_constraint(o, pltpu.HBM) for o in operands])
    return out.T


def solution(mesh):
    n = round(mesh.shape["kv"] ** 0.5)
    seq = ("dp", "kv")
    return jax.shard_map(
        functools.partial(per_device, n),
        mesh=mesh,
        in_specs=(
            P("dp", "kv"),
            P("kv"),
            P("kv", "tp"),
            P("kv", "tp"),
            P("kv", "tp"),
            P("kv", "tp"),
            P(),
            P(),
            P(seq, None, "tp"),
            P(seq, None, "tp"),
            P(seq, None, "tp"),
            P(seq, None, "tp"),
            P(seq),
            P(seq, "tp", None, None),
            P(seq, "tp", None),
            P(seq, "tp"),
            P("tp"),
            P("tp", "kv"),
            P(),
            P(None, ("kv", "tp")),
            P(None, ("kv", "tp")),
            P(("kv", "tp"), None),
        ),
        out_specs=P("dp", ("kv", "tp")),
        check_vma=False,
    )
```

```python
import functools

import jax
import jax.numpy as jnp
from jax import lax
from jax.experimental import pallas as pl
from jax.experimental.pallas import tpu as pltpu
from jax.sharding import PartitionSpec as P

EPS = 1e-06
MESH = pl.DeviceIdType.MESH
F32 = jnp.float32
BF16 = jnp.bfloat16
KINDS = 4
ROWS = 40
HIDDEN_PAD = 48


def ring_order(n):
    return sorted(range(1, n), key=lambda d: (-min(d, n - d), d))


def dot(a, b, ca=1, cb=0, precision=None):
    return lax.dot_general(
        a, b, (((ca,), (cb,)), ((), ())), preferred_element_type=F32, precision=precision
    )


def iota(shape, dim):
    return lax.broadcasted_iota(jnp.int32, shape, dim)


def kernel(
    n,
    tok_h,
    pre_h,
    qw_h,
    kw_h,
    vw_h,
    ow_h,
    ig_h,
    fg_h,
    ck_h,
    cv_h,
    ci_h,
    cf_h,
    len_h,
    sm_h,
    sn_h,
    smax_h,
    hg_h,
    mixw_h,
    mg_h,
    gw_h,
    uw_h,
    dw_h,
    out_ref,
    tok,
    pre,
    w4,
    gates,
    cfi,
    lens,
    smax,
    state,
    sn,
    ckv,
    hg,
    mixw,
    mg,
    gud,
    load_sem,
    p1,
    r1,
    relay,
    merged,
    q2f,
    q2b,
    r2,
    split,
    pick,
    mh,
    wg,
    tg,
    rbuf,
    rt,
    gu,
    dt,
    dts,
    dtc,
    p5,
    p5b,
    r3,
    s1,
    v1,
    sr,
    vr,
    s2,
    v2,
    sw,
    vw,
    st,
    vt,
    s3,
    v3,
    s5,
    v5,
    s6,
    v6,
    sg,
    vg,
    sd,
    vd,
    s8,
    v8,
):
    kvs = n * n
    width = tok.shape[0]
    seqs = tok.shape[1]
    cols = w4.shape[2]
    wide = p1.shape[2]
    blocks = cols // 128
    model = width * kvs
    dp = lax.axis_index("dp")
    kv = lax.axis_index("kv")
    tp = lax.axis_index("tp")
    z, y = kv // n, kv % n
    far = n - (n - 1) * tp
    near = 1 + (n - 1) * tp
    first = z + (y - z) * tp
    second = y + (z - y) * tp
    other = 1 - tp
    order = ring_order(n)

    def first_peer(d):
        return (dp, lax.rem(first + d, n) * far + second * near, tp)

    def second_peer(d):
        return (dp, first * far + lax.rem(second + d, n) * near, tp)

    sibling = (dp, kv, other)

    loads = [
        (tok_h, tok, 0),
        (pre_h, pre, 1),
        (qw_h, w4.at[0], 2),
        (kw_h, w4.at[1], 2),
        (vw_h, w4.at[2], 2),
        (ow_h, w4.at[3], 2),
        (ig_h, gates.at[0], 3),
        (fg_h, gates.at[1], 3),
        (cf_h, cfi.at[0], 4),
        (ci_h, cfi.at[1], 4),
        (len_h, lens, 5),
        (smax_h, smax, 6),
        (sm_h, state, 7),
        (sn_h, sn, 8),
        (ck_h, ckv.at[0], 9),
        (cv_h, ckv.at[1], 9),
        (hg_h, hg, 10),
        (mixw_h, mixw, 11),
        (mg_h, mg, 12),
        (gw_h, gud.at[0], 13),
        (uw_h, gud.at[1], 13),
        (dw_h, gud.at[2], 13),
    ]
    copies = [pltpu.make_async_copy(a, b, load_sem.at[k]) for a, b, k in loads]
    landed = [tok, pre, w4, gates, cfi, lens, smax, state, sn, ckv, hg, mixw, mg, gud]
    arrived = [pltpu.make_async_copy(r, r, load_sem.at[k]) for k, r in enumerate(landed)]
    for c in copies[:8]:
        c.start()
    barrier = pltpu.get_barrier_semaphore()
    for d in range(1, n):
        pl.semaphore_signal(barrier, inc=1, device_id=first_peer(d), device_id_type=MESH)
        pl.semaphore_signal(barrier, inc=1, device_id=second_peer(d), device_id_type=MESH)
        across = (dp, z * n + lax.rem(y + d, n), other)
        pl.semaphore_signal(barrier, inc=1, device_id=across, device_id_type=MESH)
    pl.semaphore_signal(barrier, inc=1, device_id=sibling, device_id_type=MESH)
    for c in copies[8:]:
        c.start()
    for c in arrived[:4]:
        c.wait()

    r = iota((seqs, seqs), 0)
    owner = (r // (2 * n)) * far + (r % n) * near
    perm = jnp.where(iota((seqs, seqs), 1) == owner * 2 + (r // n) % 2, 1.0, 0.0).astype(BF16)
    tokens = dot(perm, tok[...], 1, 1)
    squares = jnp.sum(tokens * tokens, axis=1, keepdims=True)
    normed = (tokens * pre[...]).astype(BF16)
    for k in range(KINDS):
        prod = dot(normed, w4[k]).astype(BF16)
        p1[:, :, k * cols : (k + 1) * cols] = prod.reshape(n, 2 * n, cols)
    lane0 = pl.multiple_of((kv // (128 // width)) * 128, 128)
    both = jnp.concatenate(
        [gates[0, :, pl.ds(lane0, 128)].astype(F32), gates[1, :, pl.ds(lane0, 128)].astype(F32)],
        axis=0,
    ).astype(BF16)
    at = (kv % (128 // width)) * width
    sel = jnp.where(iota((width, 128), 1) == iota((width, 128), 0) + at, 1.0, 0.0).astype(BF16)
    own_gates = dot(both, sel, 1, 1)
    own_gates = jnp.concatenate([own_gates, jnp.zeros((120, width), F32)], axis=0).astype(BF16)
    g = dot(normed, own_gates, 1, 1)
    g = jnp.where(iota((seqs, 128), 1) == 8, squares, g)
    p1[:, :, KINDS * cols :] = g.astype(BF16).reshape(n, 2 * n, 128)

    pl.semaphore_wait(barrier, 3 * (n - 1) + 1)

    def total(ref, send, recv):
        return pltpu.make_async_remote_copy(
            src_ref=ref,
            dst_ref=ref,
            send_sem=send,
            recv_sem=recv,
            device_id=sibling,
            device_id_type=MESH,
        )

    def send(src, dst, send_sem, recv_sem, peer):
        pltpu.make_async_remote_copy(
            src_ref=src,
            dst_ref=dst,
            send_sem=send_sem,
            recv_sem=recv_sem,
            device_id=peer,
            device_id_type=MESH,
        ).start()

    far_d = n // 2
    cut = (KINDS * blocks // 2 + 1) * 128
    parts = (pl.ds(0, cut), pl.ds(cut, wide - cut))

    def rows_for(d):
        return p1.at[lax.rem(first + d, n)]

    hops = (n - 1, 1)
    last_d = (far_d + 1, far_d - 1)
    slot = {d: k for k, d in enumerate(d for d in range(1, n) if d != far_d)}
    for k in range(2):
        part = rows_for(far_d).at[:, parts[k]]
        send(part, relay.at[:, parts[k]], sr, vr.at[k], first_peer(hops[k]))
    for k in range(2):
        d, own_part = last_d[k], parts[1 - k]
        send(rows_for(d).at[:, own_part], r1.at[slot[d], :, own_part], s1, v1, first_peer(d))
    direct = [d for d in order if d != far_d and d not in last_d]
    for d in direct:
        if d not in hops:
            send(rows_for(d), r1.at[slot[d]], s1, v1, first_peer(d))

    for c in arrived[4:]:
        c.wait()
    row64 = iota((8, ckv.shape[2]), 0)
    lane64 = iota((8, ckv.shape[2]), 1)
    zero4 = jnp.zeros((4, ckv.shape[2]), F32)
    forget = jnp.concatenate([cfi[0, 0], cfi[0, 1], zero4], axis=0)
    gain_in = jnp.concatenate([cfi[1, 0], cfi[1, 1], zero4], axis=0)
    length = jnp.where(row64 < 2, lens[0], lens[1])
    live = lane64 < length
    forget = jnp.where(live, forget, 0.0)
    span = ckv.shape[2]
    tri = jnp.where(iota((span, span), 0) <= iota((span, span), 1), 1.0, 0.0)
    running = dot(forget, tri, precision=lax.Precision.HIGHEST)
    run_last = jnp.sum(forget, axis=1, keepdims=True)
    base = jnp.where(live, run_last - running + gain_in, -jnp.inf)
    base = jnp.where(row64 < 4, base, 0.0)
    base_max = jnp.max(base, axis=1, keepdims=True)
    row1 = iota((8, 1), 0)
    state_top = jnp.where(
        row1 == 0,
        smax[0, 0],
        jnp.where(row1 == 1, smax[0, 1], jnp.where(row1 == 2, smax[1, 0], smax[1, 1])),
    )
    state_base = run_last + state_top
    for i in range(2):
        for h in range(2):
            whole = state[i, h]
            high = whole.astype(BF16)
            split[0, 2 * i + h] = high
            split[1, 2 * i + h] = (whole - high.astype(F32)).astype(BF16)
    size = sn.shape[2]
    zero_rows = jnp.zeros((4, size), F32)
    norm8 = jnp.concatenate([sn[0], sn[1], zero_rows], axis=0)
    halves = [hg[:, :size], hg[:, size:]]
    gain8 = jnp.concatenate(halves + halves + [zero_rows], axis=0)
    pr = iota((8 * n, 8 * n), 0)
    pc = iota((8 * n, 8 * n), 1)
    seq, hu = pr % (2 * n), pr // (2 * n)
    target = (seq // 2) * 8 + (hu % 2) * 4 + (seq % 2) * 2 + hu // 2
    pick[...] = jnp.where(pc == target, 1.0, 0.0).astype(BF16)
    hidden_cols = gud.shape[1]
    line = n * width
    c1 = iota((line, line), 1)
    source = ((c1 % (line // 2)) // (width // 2)) * width
    source = source + (c1 // (line // 2)) * (width // 2) + c1 % (width // 2)
    compress = jnp.where(iota((line, line), 0) == source, 1.0, 0.0).astype(BF16)
    pad = jnp.zeros((HIDDEN_PAD - hidden_cols, line), F32)
    for k in range(n):
        at = slice(k * line, (k + 1) * line)
        gain = mg[:, at]
        block = [(gud[u, :, at].astype(F32) * gain) for u in range(2)]
        block = jnp.concatenate([block[0], pad, block[1], pad], axis=0).astype(BF16)
        block = dot(block, compress).astype(BF16)
        for u in range(2):
            to = (u * n + k) * (line // 2)
            gu[tp, :, to : to + line // 2] = block[:, u * (line // 2) : (u + 1) * (line // 2)]
    group = 128 // width

    def arrange(b, carry):
        block = gud[2, :, pl.ds(pl.multiple_of(b * 128, 128), 128)].astype(F32)
        block = jnp.concatenate([block, jnp.zeros((HIDDEN_PAD - hidden_cols, 128), F32)], axis=0)
        block = block.T.astype(BF16)
        for k in range(group):
            at_kv = b * group + k
            mirrored = (at_kv % n) * n + at_kv // n
            half = width // 2
            dt[0, at_kv] = block[k * width : k * width + half]
            dt[1, mirrored] = block[k * width + half : (k + 1) * width]
        return carry

    lax.fori_loop(0, kvs // group, arrange, 0)
    send(gu.at[tp], gu.at[tp], sg, vg, sibling)
    send(dt.at[other], dts, sd, vd, sibling)

    for k in range(2):
        d = last_d[k]
        total(relay.at[:, parts[k]], sr, vr.at[k]).wait_recv()
        mine = p1[lax.rem(first + d, n), :, parts[k]].astype(F32)
        merged[:, parts[k]] = (mine + relay[:, parts[k]].astype(F32)).astype(BF16)
        send(merged.at[:, parts[k]], r1.at[slot[d], :, parts[k]], s1, v1, first_peer(d))
    for d in direct:
        if d in hops:
            send(rows_for(d), r1.at[slot[d]], s1, v1, first_peer(d))
    half = width // 2
    own_rows = pl.ds(pl.multiple_of(tp * half, half), half)
    rest = pl.ds(pl.multiple_of(other * half, half), half)

    def share_weights():
        for d in order:
            along_y = z * n + lax.rem(y + d, n)
            send(tok.at[own_rows], tg.at[y], st, vt, (dp, along_y, tp))
            send(mixw.at[own_rows], wg.at[tp, y], sw, vw, (dp, along_y, tp))
            send(mixw.at[rest], wg.at[tp, y], sw, vw, (dp, along_y, other))
        send(mixw.at[rest], wg.at[tp, y], sw, vw, sibling)

    @pl.when(tp == 1)
    def _():
        share_weights()

    own = p1[first].astype(F32)
    total(r1, s1, v1).wait_recv()
    for k in range(n - 2):
        own = own + r1[k].astype(F32)
    q2f[...] = jnp.zeros_like(q2f)
    for i in range(2):
        part = own[i * n : (i + 1) * n]
        for c in range(KINDS * blocks):
            kind, h, u = c // blocks, (c % blocks) // 2, c % 2
            q2f[pl.ds(kind * 8 + u * 4 + i * 2 + h, n, stride=ROWS), :] = part[
                :, c * 128 : (c + 1) * 128
            ]
        for h in range(2):
            q2f[pl.ds(32 + i * 2 + h, n, stride=ROWS), :] = part[:, KINDS * cols :]
    q2b[...] = q2f[...].reshape(n, ROWS, 128).astype(BF16)
    for d in order:
        send(q2b.at[lax.rem(second + d, n)], r2.at[d - 1], s2, v2, second_peer(d))
    @pl.when(tp == 0)
    def _():
        share_weights()

    wg[tp, y] = mixw[own_rows, :]
    tg[y] = tok[own_rows, :]
    total(dts, sd, vd).wait_recv()
    half_dt = [dt[tp].reshape(kvs * half, HIDDEN_PAD), dts[...].reshape(kvs * half, HIDDEN_PAD)]
    half_dt = [jnp.where(tp == c, half_dt[0], half_dt[1]) for c in range(2)]
    dtc[...] = jnp.concatenate(half_dt, axis=1)
    mine = q2f[pl.ds(pl.multiple_of(second * ROWS, 8), ROWS), :]
    total(r2, s2, v2).wait_recv()
    for k in range(n - 1):
        mine = mine + r2[k].astype(F32)

    def heads(kind):
        a = mine[kind * 8 : kind * 8 + 4]
        b = mine[kind * 8 + 4 : kind * 8 + 8]
        return jnp.concatenate([jnp.concatenate([a, b], axis=1), zero_rows], axis=0)

    gate8 = mine[32:40]
    lane = iota((8, 128), 1)
    row = iota((8, 128), 0)
    square = jnp.sum(jnp.where(lane == 8, gate8, 0.0), axis=1, keepdims=True)
    in_sum = jnp.sum(jnp.where(lane == 2 * tp + row % 2, gate8, 0.0), axis=1, keepdims=True)
    fg_sum = jnp.sum(jnp.where(lane == 4 + 2 * tp + row % 2, gate8, 0.0), axis=1, keepdims=True)
    scale = lax.rsqrt(square / model + EPS)
    query = (scale * heads(0)).astype(BF16).astype(F32)
    key_new = (scale * heads(1)).astype(BF16).astype(F32)
    value_new = (scale * heads(2)).astype(BF16).astype(F32)
    outgate = (scale * heads(3)).astype(BF16).astype(F32)
    in_gate = scale * in_sum
    fg = scale * fg_sum
    forget_new = jnp.minimum(fg, 0.0) - jnp.log1p(jnp.exp(-jnp.abs(fg)))
    weight_log = base + forget_new
    state_log = state_base + forget_new
    peak = jnp.maximum(jnp.maximum(state_log, in_gate), base_max + forget_new)
    query = query * (size**-0.5)
    rows = iota((8, size), 0)
    alone = [jnp.where(rows == k, query, 0.0) for k in range(4)]
    dots = dot(jnp.concatenate(alone[0:2], axis=1).astype(BF16), ckv[0, 0], 1, 1)
    dots = dots + dot(jnp.concatenate(alone[2:4], axis=1).astype(BF16), ckv[0, 1], 1, 1)
    scores = jnp.exp(weight_log - peak) * dots
    self_score = jnp.exp(in_gate - peak) * jnp.sum(query * key_new, axis=1, keepdims=True)
    carried = jnp.exp(state_log - peak)
    read = dot(alone[0].astype(BF16), split[0, 0], 1, 1)
    read = read + dot(alone[0].astype(BF16), split[1, 0], 1, 1)
    for k in range(1, 4):
        read = read + dot(alone[k].astype(BF16), split[0, k], 1, 1)
        read = read + dot(alone[k].astype(BF16), split[1, k], 1, 1)
    norm_read = jnp.sum(norm8 * query, axis=1, keepdims=True)
    values = dot(jnp.where(row64 < 2, scores, 0.0).astype(BF16), ckv[1, 0])
    values = values + dot(jnp.where(row64 >= 2, scores, 0.0).astype(BF16), ckv[1, 1])
    values = jnp.where(rows % 2 == 0, values[:, :size], values[:, size:])
    numerator = carried * read + values + self_score * value_new
    denominator = carried * norm_read + jnp.sum(scores, axis=1, keepdims=True) + self_score
    hidden = numerator / jnp.maximum(jnp.abs(denominator), 1.0)
    mixed = hidden * gain8 * jax.nn.sigmoid(outgate)
    mh[tp, z] = jnp.concatenate([mixed[:4, :128], mixed[:4, 128:]], axis=0).astype(BF16)

    for d in order:
        along_z = lax.rem(z + d, n) * n + y
        for core in (tp, other):
            send(mh.at[tp, z], mh.at[tp, z], s3, v3, (dp, along_z, core))
    send(mh.at[tp, z], mh.at[tp, z], s3, v3, sibling)
    flat_w = wg.reshape(2 * n, half, cols)
    flat_m = mh.reshape(2 * n, 8, 128)
    all_wg = total(flat_w.at[pl.ds(0, 2 * n - 1)], sw, vw)
    all_tg = total(tg.at[pl.ds(0, n - 1)], st, vt)
    all_mh = total(flat_m.at[pl.ds(0, 2 * n - 1)], s3, v3)
    for c in (all_wg, all_tg, all_mh):
        c.wait_recv()

    def project(u):
        flat = mh[u].astype(F32).reshape(8 * n, 128).astype(BF16)
        picked = dot(pick[...], flat).astype(BF16)
        w = wg[u].reshape(n * half, cols)
        out = dot(picked[: 2 * n], w[:, :128], 1, 1)
        for k in range(1, 4):
            block = picked[2 * n * k : 2 * n * (k + 1)]
            out = out + dot(block, w[:, k * 128 : (k + 1) * 128], 1, 1)
        return out.astype(BF16).astype(F32)

    q = iota((2 * n, seqs), 0)
    here = jnp.where(iota((2 * n, seqs), 1) == ((q // 2) * n + y) * 2 + q % 2, 1.0, 0.0)
    own_tokens = dot(here.astype(BF16), tg[...].reshape(n * half, seqs), 1, 1)
    rbuf[...] = (own_tokens + (project(0) + project(1))).astype(BF16)

    rt[tp, z, y] = rbuf[...]
    rows_order = order + [0]
    for dz in rows_order:
        for dy in rows_order:
            if dz or dy:
                peer = lax.rem(z + dz, n) * n + lax.rem(y + dy, n)
                send(rbuf, rt.at[tp, z, y], s5, v5.at[dz], (dp, peer, tp))
    for dz in rows_order:
        count = n if dz else n - 1
        total(rt.at[0, 0, pl.ds(0, count)], s5, v5.at[dz]).wait_recv()
        source = lax.rem(z + n - dz, n)
        send(rt.at[tp, source], rt.at[tp, source], s6, v6, sibling)
    total(rt.at[0], s6, v6).wait_recv()

    lanes = n * half
    power = jnp.zeros((seqs, lanes), F32)
    acc = jnp.zeros((4 * HIDDEN_PAD, seqs), F32)
    total(gu.at[0], sg, vg).wait_recv()
    for u in range(2):
        for k in range(0, n, 2):
            pair = [rt[u, k + e].reshape(seqs, lanes) for e in range(2)]
            at = (u * n + k) * lanes
            wide_pair = jnp.concatenate(pair, axis=1)
            both = gu[:, :, at : at + 2 * lanes].reshape(4 * HIDDEN_PAD, 2 * lanes)
            acc = acc + dot(both, wide_pair, 1, 1)
            for block in pair:
                spread = block.astype(F32)
                power = power + spread * spread
    power = dot(jnp.ones((8, lanes), F32), power, 1, 1, precision=lax.Precision.HIGHEST)[:1]
    scale_mid = lax.rsqrt(power / model + EPS)
    acc = scale_mid * acc
    units = []
    for c in range(2):
        gate = acc[2 * c * HIDDEN_PAD : (2 * c + 1) * HIDDEN_PAD]
        up = acc[(2 * c + 1) * HIDDEN_PAD : (2 * c + 2) * HIDDEN_PAD]
        units.append(gate * jax.nn.sigmoid(gate) * up)
    units = jnp.concatenate(units, axis=0).astype(BF16)

    steps = order + [0]
    sums = dot(dtc[...], units)
    p5b[...] = sums.astype(BF16).reshape(n, n, half, seqs)
    p5[...] = sums.reshape(n, n * half, seqs)
    for dz, dy in sorted([(a, b) for a in steps for b in steps], key=lambda p: -min(p[0], n - p[0]) - min(p[1], n - p[1])):
        if dz or dy:
            to_z, to_y = lax.rem(z + dz, n), lax.rem(y + dy, n)
            at_f, at_s = to_z + (to_y - to_z) * tp, to_y + (to_z - to_y) * tp
            peer = (dp, to_z * n + to_y, tp)
            send(p5b.at[at_f, at_s], r3.at[dz * n + dy - 1], s8, v8, peer)
    mine_at = jnp.where(iota((half, lanes), 1) == iota((half, lanes), 0) + y * half, 1.0, 0.0)
    last = dot(mine_at.astype(BF16), rt[tp, z].reshape(seqs, lanes), 1, 1)
    last = last + p5[first, pl.ds(pl.multiple_of(second * half, half), half), :]
    c2 = iota((seqs, seqs), 1)
    back = ((c2 // 2) % n) * 2 * n + (c2 // (2 * n)) * 2 + c2 % 2
    back = jnp.where(iota((seqs, seqs), 0) == back, 1.0, 0.0).astype(BF16)
    total(r3, s8, v8).wait_recv()
    last = last + jnp.sum(r3[...].astype(F32), axis=0)
    out_ref[...] = dot(last.astype(BF16), back).astype(BF16)

    total(relay, sr, vr.at[0]).wait_send()
    total(r1, s1, v1).wait_send()
    total(r2, s2, v2).wait_send()
    for c in (all_wg, all_tg, all_mh):
        c.wait_send()
    flat_r = rt.reshape(2 * kvs, 2 * n, lanes)
    total(flat_r.at[pl.ds(0, kvs - 1)], s5, v5.at[0]).wait_send()
    total(rt.at[0], s6, v6).wait_send()
    total(gu.at[0], sg, vg).wait_send()
    total(dts, sd, vd).wait_send()
    total(r3, s8, v8).wait_send()


def per_device(n, *args):
    (tokens, pre, qw, kw, vw, ow, ig, fg, ck, cv, ci, cf, lens, sm, sn, smax) = args[:16]
    hg, mixw, mg, gw, uw, dw = args[16:]
    operands = (
        tokens.T,
        pre.reshape(1, -1),
        qw,
        kw,
        vw,
        ow,
        ig.T,
        fg.T,
        ck,
        cv,
        ci.transpose(0, 2, 1),
        cf.transpose(0, 2, 1),
        lens,
        sm,
        sn,
        smax,
        hg.reshape(1, -1),
        mixw.T,
        mg.reshape(1, -1),
        gw.T,
        uw.T,
        dw,
    )
    seqs, width = tokens.shape
    cols = qw.shape[1]
    kvs = n * n
    model = width * kvs
    span, size = ck.shape[1], sn.shape[2]
    wide = KINDS * cols + 128
    half = width // 2
    dma = pltpu.SemaphoreType.DMA
    vmem = pltpu.VMEM
    ff = gw.shape[1]
    scratch = [
        vmem((width, seqs), BF16),
        vmem((1, width), F32),
        vmem((KINDS, width, cols), BF16),
        vmem((2, 4, model), BF16),
        vmem((2, 2, 2, span), F32),
        pltpu.SMEM((2,), jnp.int32),
        pltpu.SMEM((2, 2), F32),
        vmem((2, 2, size, size), F32),
        vmem((2, 2, size), F32),
        vmem((2, 2, span, cols), BF16),
        vmem((1, cols), F32),
        vmem((width, cols), BF16),
        vmem((1, model), F32),
        vmem((3, ff, model), BF16),
        dma((14,)),
        vmem((n, 2 * n, wide), BF16),
        vmem((n - 2, 2 * n, wide), BF16),
        vmem((2 * n, wide), BF16),
        vmem((2 * n, wide), BF16),
        vmem((n * ROWS, 128), F32),
        vmem((n, ROWS, 128), BF16),
        vmem((n - 1, ROWS, 128), BF16),
        vmem((2, 4, size, size), BF16),
        vmem((8 * n, 8 * n), BF16),
        vmem((2, n, 8, 128), BF16),
        vmem((2, n, half, cols), BF16),
        vmem((n, half, seqs), BF16),
        vmem((2 * n, n * half), BF16),
        vmem((2, n, n, 2 * n, n * half), BF16),
        vmem((2, 2 * HIDDEN_PAD, model), BF16),
        vmem((2, kvs, half, HIDDEN_PAD), BF16),
        vmem((kvs, half, HIDDEN_PAD), BF16),
        vmem((kvs * half, 2 * HIDDEN_PAD), BF16),
        vmem((n, n * half, seqs), F32),
        vmem((n, n, half, seqs), BF16),
        vmem((kvs - 1, half, seqs), BF16),
        dma,
        dma,
        dma,
        dma((2,)),
        dma,
        dma,
        dma,
        dma,
        dma,
        dma,
        dma,
        dma,
        dma,
        dma((n,)),
        dma,
        dma,
        dma,
        dma,
        dma,
        dma,
        dma,
        dma,
    ]
    out = pl.pallas_call(
        functools.partial(kernel, n),
        out_shape=jax.ShapeDtypeStruct((half, seqs), BF16),
        in_specs=[pl.BlockSpec(memory_space=pl.ANY)] * len(operands),
        out_specs=pl.BlockSpec(memory_space=pltpu.VMEM),
        scratch_shapes=scratch,
        compiler_params=pltpu.CompilerParams(
            collective_id=0, has_side_effects=True, vmem_limit_bytes=24 * 1024 * 1024
        ),
        name="layer",
    )(*[pltpu.with_memory_space_constraint(o, pltpu.HBM) for o in operands])
    return out.T


def solution(mesh):
    n = round(mesh.shape["kv"] ** 0.5)
    seq = ("dp", "kv")
    return jax.shard_map(
        functools.partial(per_device, n),
        mesh=mesh,
        in_specs=(
            P("dp", "kv"),
            P("kv"),
            P("kv", "tp"),
            P("kv", "tp"),
            P("kv", "tp"),
            P("kv", "tp"),
            P(),
            P(),
            P(seq, None, "tp"),
            P(seq, None, "tp"),
            P(seq, None, "tp"),
            P(seq, None, "tp"),
            P(seq),
            P(seq, "tp", None, None),
            P(seq, "tp", None),
            P(seq, "tp"),
            P("tp"),
            P("tp", "kv"),
            P(),
            P(None, ("kv", "tp")),
            P(None, ("kv", "tp")),
            P(("kv", "tp"), None),
        ),
        out_specs=P("dp", ("kv", "tp")),
        check_vma=False,
    )
```

```python
import functools

import jax
import jax.numpy as jnp
from jax import lax
from jax.experimental import pallas as pl
from jax.experimental.pallas import tpu as pltpu
from jax.sharding import PartitionSpec as P

EPS = 1e-06
MESH = pl.DeviceIdType.MESH
F32 = jnp.float32
BF16 = jnp.bfloat16
KINDS = 4
ROWS = 40
HIDDEN_PAD = 48


def ring_order(n):
    return sorted(range(1, n), key=lambda d: (-min(d, n - d), d))


def dot(a, b, ca=1, cb=0, precision=None):
    return lax.dot_general(
        a, b, (((ca,), (cb,)), ((), ())), preferred_element_type=F32, precision=precision
    )


def iota(shape, dim):
    return lax.broadcasted_iota(jnp.int32, shape, dim)


def kernel(
    n,
    tok_h,
    pre_h,
    qw_h,
    kw_h,
    vw_h,
    ow_h,
    ig_h,
    fg_h,
    ck_h,
    cv_h,
    ci_h,
    cf_h,
    len_h,
    sm_h,
    sn_h,
    smax_h,
    hg_h,
    mixw_h,
    mg_h,
    gw_h,
    uw_h,
    dw_h,
    out_ref,
    tok,
    pre,
    w4,
    gates,
    cfi,
    lens,
    smax,
    state,
    sn,
    ckv,
    hg,
    mixw,
    mg,
    gud,
    load_sem,
    p1,
    r1,
    relay,
    merged,
    q2f,
    q2b,
    r2,
    split,
    pick,
    mh,
    wg,
    tg,
    rbuf,
    rt,
    gu,
    dt,
    dts,
    dtc,
    p5,
    p5b,
    r3,
    s1,
    v1,
    sr,
    vr,
    s2,
    v2,
    sw,
    vw,
    st,
    vt,
    s3,
    v3,
    s5,
    v5,
    s6,
    v6,
    sg,
    vg,
    sd,
    vd,
    s8,
    v8,
):
    kvs = n * n
    width = tok.shape[0]
    seqs = tok.shape[1]
    cols = w4.shape[2]
    wide = p1.shape[2]
    blocks = cols // 128
    model = width * kvs
    dp = lax.axis_index("dp")
    kv = lax.axis_index("kv")
    tp = lax.axis_index("tp")
    z, y = kv // n, kv % n
    far = n - (n - 1) * tp
    near = 1 + (n - 1) * tp
    first = z + (y - z) * tp
    second = y + (z - y) * tp
    other = 1 - tp
    order = ring_order(n)

    def first_peer(d):
        return (dp, lax.rem(first + d, n) * far + second * near, tp)

    def second_peer(d):
        return (dp, first * far + lax.rem(second + d, n) * near, tp)

    sibling = (dp, kv, other)

    loads = [
        (tok_h, tok, 0),
        (pre_h, pre, 1),
        (qw_h, w4.at[0], 2),
        (kw_h, w4.at[1], 2),
        (vw_h, w4.at[2], 2),
        (ow_h, w4.at[3], 2),
        (ig_h, gates.at[0], 3),
        (fg_h, gates.at[1], 3),
        (cf_h, cfi.at[0], 4),
        (ci_h, cfi.at[1], 4),
        (len_h, lens, 5),
        (smax_h, smax, 6),
        (sm_h, state, 7),
        (sn_h, sn, 8),
        (ck_h, ckv.at[0], 9),
        (cv_h, ckv.at[1], 9),
        (hg_h, hg, 10),
        (mixw_h, mixw, 11),
        (mg_h, mg, 12),
        (gw_h, gud.at[0], 13),
        (uw_h, gud.at[1], 13),
        (dw_h, gud.at[2], 13),
    ]
    copies = [pltpu.make_async_copy(a, b, load_sem.at[k]) for a, b, k in loads]
    landed = [tok, pre, w4, gates, cfi, lens, smax, state, sn, ckv, hg, mixw, mg, gud]
    arrived = [pltpu.make_async_copy(r, r, load_sem.at[k]) for k, r in enumerate(landed)]
    for c in copies[:8]:
        c.start()
    barrier = pltpu.get_barrier_semaphore()
    for d in range(1, n):
        pl.semaphore_signal(barrier, inc=1, device_id=first_peer(d), device_id_type=MESH)
        pl.semaphore_signal(barrier, inc=1, device_id=second_peer(d), device_id_type=MESH)
        across = (dp, z * n + lax.rem(y + d, n), other)
        pl.semaphore_signal(barrier, inc=1, device_id=across, device_id_type=MESH)
    pl.semaphore_signal(barrier, inc=1, device_id=sibling, device_id_type=MESH)
    for c in copies[8:]:
        c.start()
    for c in arrived[:4]:
        c.wait()

    r = iota((seqs, seqs), 0)
    owner = (r // (2 * n)) * far + (r % n) * near
    perm = jnp.where(iota((seqs, seqs), 1) == owner * 2 + (r // n) % 2, 1.0, 0.0).astype(BF16)
    tokens = dot(perm, tok[...], 1, 1)
    squares = jnp.sum(tokens * tokens, axis=1, keepdims=True)
    normed = (tokens * pre[...]).astype(BF16)
    for k in range(KINDS):
        prod = dot(normed, w4[k]).astype(BF16)
        p1[:, :, k * cols : (k + 1) * cols] = prod.reshape(n, 2 * n, cols)
    lane0 = pl.multiple_of((kv // (128 // width)) * 128, 128)
    both = jnp.concatenate(
        [gates[0, :, pl.ds(lane0, 128)].astype(F32), gates[1, :, pl.ds(lane0, 128)].astype(F32)],
        axis=0,
    ).astype(BF16)
    at = (kv % (128 // width)) * width
    sel = jnp.where(iota((width, 128), 1) == iota((width, 128), 0) + at, 1.0, 0.0).astype(BF16)
    own_gates = dot(both, sel, 1, 1)
    own_gates = jnp.concatenate([own_gates, jnp.zeros((120, width), F32)], axis=0).astype(BF16)
    g = dot(normed, own_gates, 1, 1)
    g = jnp.where(iota((seqs, 128), 1) == 8, squares, g)
    p1[:, :, KINDS * cols :] = g.astype(BF16).reshape(n, 2 * n, 128)

    pl.semaphore_wait(barrier, 3 * (n - 1) + 1)

    def total(ref, send, recv):
        return pltpu.make_async_remote_copy(
            src_ref=ref,
            dst_ref=ref,
            send_sem=send,
            recv_sem=recv,
            device_id=sibling,
            device_id_type=MESH,
        )

    def send(src, dst, send_sem, recv_sem, peer):
        pltpu.make_async_remote_copy(
            src_ref=src,
            dst_ref=dst,
            send_sem=send_sem,
            recv_sem=recv_sem,
            device_id=peer,
            device_id_type=MESH,
        ).start()

    far_d = n // 2
    cut = (KINDS * blocks // 2 + 1) * 128
    parts = (pl.ds(0, cut), pl.ds(cut, wide - cut))

    def rows_for(d):
        return p1.at[lax.rem(first + d, n)]

    hops = (n - 1, 1)
    last_d = (far_d + 1, far_d - 1)
    slot = {d: k for k, d in enumerate(d for d in range(1, n) if d != far_d)}
    for k in range(2):
        part = rows_for(far_d).at[:, parts[k]]
        send(part, relay.at[:, parts[k]], sr, vr.at[k], first_peer(hops[k]))
    for k in range(2):
        d, own_part = last_d[k], parts[1 - k]
        send(rows_for(d).at[:, own_part], r1.at[slot[d], :, own_part], s1, v1, first_peer(d))
    direct = [d for d in order if d != far_d and d not in last_d]
    for d in direct:
        if d not in hops:
            send(rows_for(d), r1.at[slot[d]], s1, v1, first_peer(d))

    for c in arrived[4:]:
        c.wait()
    row64 = iota((8, ckv.shape[2]), 0)
    lane64 = iota((8, ckv.shape[2]), 1)
    zero4 = jnp.zeros((4, ckv.shape[2]), F32)
    forget = jnp.concatenate([cfi[0, 0], cfi[0, 1], zero4], axis=0)
    gain_in = jnp.concatenate([cfi[1, 0], cfi[1, 1], zero4], axis=0)
    length = jnp.where(row64 < 2, lens[0], lens[1])
    live = lane64 < length
    forget = jnp.where(live, forget, 0.0)
    span = ckv.shape[2]
    tri = jnp.where(iota((span, span), 0) <= iota((span, span), 1), 1.0, 0.0)
    running = dot(forget, tri, precision=lax.Precision.HIGHEST)
    run_last = jnp.sum(forget, axis=1, keepdims=True)
    base = jnp.where(live, run_last - running + gain_in, -jnp.inf)
    base = jnp.where(row64 < 4, base, 0.0)
    base_max = jnp.max(base, axis=1, keepdims=True)
    row1 = iota((8, 1), 0)
    state_top = jnp.where(
        row1 == 0,
        smax[0, 0],
        jnp.where(row1 == 1, smax[0, 1], jnp.where(row1 == 2, smax[1, 0], smax[1, 1])),
    )
    state_base = run_last + state_top
    for i in range(2):
        for h in range(2):
            whole = state[i, h]
            high = whole.astype(BF16)
            split[0, 2 * i + h] = high
            split[1, 2 * i + h] = (whole - high.astype(F32)).astype(BF16)
    size = sn.shape[2]
    zero_rows = jnp.zeros((4, size), F32)
    norm8 = jnp.concatenate([sn[0], sn[1], zero_rows], axis=0)
    halves = [hg[:, :size], hg[:, size:]]
    gain8 = jnp.concatenate(halves + halves + [zero_rows], axis=0)
    pr = iota((8 * n, 8 * n), 0)
    pc = iota((8 * n, 8 * n), 1)
    seq, hu = pr % (2 * n), pr // (2 * n)
    target = (seq // 2) * 8 + (hu % 2) * 4 + (seq % 2) * 2 + hu // 2
    pick[...] = jnp.where(pc == target, 1.0, 0.0).astype(BF16)
    hidden_cols = gud.shape[1]
    line = n * width
    c1 = iota((line, line), 1)
    source = ((c1 % (line // 2)) // (width // 2)) * width
    source = source + (c1 // (line // 2)) * (width // 2) + c1 % (width // 2)
    compress = jnp.where(iota((line, line), 0) == source, 1.0, 0.0).astype(BF16)
    pad = jnp.zeros((HIDDEN_PAD - hidden_cols, line), F32)
    for k in range(n):
        at = slice(k * line, (k + 1) * line)
        gain = mg[:, at]
        block = [(gud[u, :, at].astype(F32) * gain) for u in range(2)]
        block = jnp.concatenate([block[0], pad, block[1], pad], axis=0).astype(BF16)
        block = dot(block, compress).astype(BF16)
        for u in range(2):
            to = (u * n + k) * (line // 2)
            gu[tp, :, to : to + line // 2] = block[:, u * (line // 2) : (u + 1) * (line // 2)]
    group = 128 // width

    def arrange(b, carry):
        block = gud[2, :, pl.ds(pl.multiple_of(b * 128, 128), 128)].astype(F32)
        block = jnp.concatenate([block, jnp.zeros((HIDDEN_PAD - hidden_cols, 128), F32)], axis=0)
        block = block.T.astype(BF16)
        for k in range(group):
            at_kv = b * group + k
            mirrored = (at_kv % n) * n + at_kv // n
            half = width // 2
            dt[0, at_kv] = block[k * width : k * width + half]
            dt[1, mirrored] = block[k * width + half : (k + 1) * width]
        return carry

    lax.fori_loop(0, kvs // group, arrange, 0)
    send(gu.at[tp], gu.at[tp], sg, vg, sibling)
    send(dt.at[other], dts, sd, vd, sibling)

    for k in range(2):
        d = last_d[k]
        total(relay.at[:, parts[k]], sr, vr.at[k]).wait_recv()
        mine = p1[lax.rem(first + d, n), :, parts[k]].astype(F32)
        merged[:, parts[k]] = (mine + relay[:, parts[k]].astype(F32)).astype(BF16)
        send(merged.at[:, parts[k]], r1.at[slot[d], :, parts[k]], s1, v1, first_peer(d))
    for d in direct:
        if d in hops:
            send(rows_for(d), r1.at[slot[d]], s1, v1, first_peer(d))
    half = width // 2
    own_rows = pl.ds(pl.multiple_of(tp * half, half), half)
    rest = pl.ds(pl.multiple_of(other * half, half), half)

    def share_weights():
        for d in order:
            along_y = z * n + lax.rem(y + d, n)
            send(tok.at[own_rows], tg.at[y], st, vt, (dp, along_y, tp))
            send(mixw.at[own_rows], wg.at[tp, y], sw, vw, (dp, along_y, tp))
            send(mixw.at[rest], wg.at[tp, y], sw, vw, (dp, along_y, other))
        send(mixw.at[rest], wg.at[tp, y], sw, vw, sibling)

    @pl.when(tp == 1)
    def _():
        share_weights()

    own = p1[first].astype(F32)
    total(r1, s1, v1).wait_recv()
    for k in range(n - 2):
        own = own + r1[k].astype(F32)
    q2f[...] = jnp.zeros_like(q2f)
    for i in range(2):
        part = own[i * n : (i + 1) * n]
        for c in range(KINDS * blocks):
            kind, h, u = c // blocks, (c % blocks) // 2, c % 2
            q2f[pl.ds(kind * 8 + u * 4 + i * 2 + h, n, stride=ROWS), :] = part[
                :, c * 128 : (c + 1) * 128
            ]
        for h in range(2):
            q2f[pl.ds(32 + i * 2 + h, n, stride=ROWS), :] = part[:, KINDS * cols :]
    q2b[...] = q2f[...].reshape(n, ROWS, 128).astype(BF16)
    for d in order:
        send(q2b.at[lax.rem(second + d, n)], r2.at[d - 1], s2, v2, second_peer(d))
    @pl.when(tp == 0)
    def _():
        share_weights()

    wg[tp, y] = mixw[own_rows, :]
    tg[y] = tok[own_rows, :]
    total(dts, sd, vd).wait_recv()
    half_dt = [dt[tp].reshape(kvs * half, HIDDEN_PAD), dts[...].reshape(kvs * half, HIDDEN_PAD)]
    half_dt = [jnp.where(tp == c, half_dt[0], half_dt[1]) for c in range(2)]
    dtc[...] = jnp.concatenate(half_dt, axis=1)
    mine = q2f[pl.ds(pl.multiple_of(second * ROWS, 8), ROWS), :]
    total(r2, s2, v2).wait_recv()
    for k in range(n - 1):
        mine = mine + r2[k].astype(F32)

    def heads(kind):
        a = mine[kind * 8 : kind * 8 + 4]
        b = mine[kind * 8 + 4 : kind * 8 + 8]
        return jnp.concatenate([jnp.concatenate([a, b], axis=1), zero_rows], axis=0)

    gate8 = mine[32:40]
    lane = iota((8, 128), 1)
    row = iota((8, 128), 0)
    square = jnp.sum(jnp.where(lane == 8, gate8, 0.0), axis=1, keepdims=True)
    in_sum = jnp.sum(jnp.where(lane == 2 * tp + row % 2, gate8, 0.0), axis=1, keepdims=True)
    fg_sum = jnp.sum(jnp.where(lane == 4 + 2 * tp + row % 2, gate8, 0.0), axis=1, keepdims=True)
    scale = lax.rsqrt(square / model + EPS)
    query = (scale * heads(0)).astype(BF16).astype(F32)
    key_new = (scale * heads(1)).astype(BF16).astype(F32)
    value_new = (scale * heads(2)).astype(BF16).astype(F32)
    outgate = (scale * heads(3)).astype(BF16).astype(F32)
    in_gate = scale * in_sum
    fg = scale * fg_sum
    forget_new = jnp.minimum(fg, 0.0) - jnp.log1p(jnp.exp(-jnp.abs(fg)))
    weight_log = base + forget_new
    state_log = state_base + forget_new
    peak = jnp.maximum(jnp.maximum(state_log, in_gate), base_max + forget_new)
    query = query * (size**-0.5)
    rows = iota((8, size), 0)
    alone = [jnp.where(rows == k, query, 0.0) for k in range(4)]
    dots = dot(jnp.concatenate(alone[0:2], axis=1).astype(BF16), ckv[0, 0], 1, 1)
    dots = dots + dot(jnp.concatenate(alone[2:4], axis=1).astype(BF16), ckv[0, 1], 1, 1)
    scores = jnp.exp(weight_log - peak) * dots
    self_score = jnp.exp(in_gate - peak) * jnp.sum(query * key_new, axis=1, keepdims=True)
    carried = jnp.exp(state_log - peak)
    read = dot(alone[0].astype(BF16), split[0, 0], 1, 1)
    read = read + dot(alone[0].astype(BF16), split[1, 0], 1, 1)
    for k in range(1, 4):
        read = read + dot(alone[k].astype(BF16), split[0, k], 1, 1)
        read = read + dot(alone[k].astype(BF16), split[1, k], 1, 1)
    norm_read = jnp.sum(norm8 * query, axis=1, keepdims=True)
    values = dot(jnp.where(row64 < 2, scores, 0.0).astype(BF16), ckv[1, 0])
    values = values + dot(jnp.where(row64 >= 2, scores, 0.0).astype(BF16), ckv[1, 1])
    values = jnp.where(rows % 2 == 0, values[:, :size], values[:, size:])
    numerator = carried * read + values + self_score * value_new
    denominator = carried * norm_read + jnp.sum(scores, axis=1, keepdims=True) + self_score
    hidden = numerator / jnp.maximum(jnp.abs(denominator), 1.0)
    mixed = hidden * gain8 * jax.nn.sigmoid(outgate)
    mh[tp, z] = jnp.concatenate([mixed[:4, :128], mixed[:4, 128:]], axis=0).astype(BF16)

    for d in order:
        along_z = lax.rem(z + d, n) * n + y
        for core in (tp, other):
            send(mh.at[tp, z], mh.at[tp, z], s3, v3, (dp, along_z, core))
    send(mh.at[tp, z], mh.at[tp, z], s3, v3, sibling)
    flat_w = wg.reshape(2 * n, half, cols)
    flat_m = mh.reshape(2 * n, 8, 128)
    all_wg = total(flat_w.at[pl.ds(0, 2 * n - 1)], sw, vw)
    all_tg = total(tg.at[pl.ds(0, n - 1)], st, vt)
    all_mh = total(flat_m.at[pl.ds(0, 2 * n - 1)], s3, v3)
    for c in (all_wg, all_tg, all_mh):
        c.wait_recv()

    def project(u):
        flat = mh[u].astype(F32).reshape(8 * n, 128).astype(BF16)
        picked = dot(pick[...], flat).astype(BF16)
        w = wg[u].reshape(n * half, cols)
        out = dot(picked[: 2 * n], w[:, :128], 1, 1)
        for k in range(1, 4):
            block = picked[2 * n * k : 2 * n * (k + 1)]
            out = out + dot(block, w[:, k * 128 : (k + 1) * 128], 1, 1)
        return out.astype(BF16).astype(F32)

    q = iota((2 * n, seqs), 0)
    here = jnp.where(iota((2 * n, seqs), 1) == ((q // 2) * n + y) * 2 + q % 2, 1.0, 0.0)
    own_tokens = dot(here.astype(BF16), tg[...].reshape(n * half, seqs), 1, 1)
    rbuf[...] = (own_tokens + (project(0) + project(1))).astype(BF16)

    rt[tp, z, y] = rbuf[...]
    rows_order = order + [0]
    hops_of = lambda p: -min(p[0], n - p[0]) - min(p[1], n - p[1])
    for dz, dy in sorted([(a, b) for a in rows_order for b in rows_order], key=hops_of):
        if dz or dy:
            peer = lax.rem(z + dz, n) * n + lax.rem(y + dy, n)
            send(rbuf, rt.at[tp, z, y], s5, v5.at[dz], (dp, peer, tp))
    for dz in rows_order:
        count = n if dz else n - 1
        total(rt.at[0, 0, pl.ds(0, count)], s5, v5.at[dz]).wait_recv()
        source = lax.rem(z + n - dz, n)
        send(rt.at[tp, source], rt.at[tp, source], s6, v6, sibling)
    total(rt.at[0], s6, v6).wait_recv()

    lanes = n * half
    power = jnp.zeros((seqs, lanes), F32)
    acc = jnp.zeros((4 * HIDDEN_PAD, seqs), F32)
    total(gu.at[0], sg, vg).wait_recv()
    for u in range(2):
        for k in range(0, n, 2):
            pair = [rt[u, k + e].reshape(seqs, lanes) for e in range(2)]
            at = (u * n + k) * lanes
            wide_pair = jnp.concatenate(pair, axis=1)
            both = gu[:, :, at : at + 2 * lanes].reshape(4 * HIDDEN_PAD, 2 * lanes)
            acc = acc + dot(both, wide_pair, 1, 1)
            for block in pair:
                spread = block.astype(F32)
                power = power + spread * spread
    power = dot(jnp.ones((8, lanes), F32), power, 1, 1, precision=lax.Precision.HIGHEST)[:1]
    scale_mid = lax.rsqrt(power / model + EPS)
    acc = scale_mid * acc
    units = []
    for c in range(2):
        gate = acc[2 * c * HIDDEN_PAD : (2 * c + 1) * HIDDEN_PAD]
        up = acc[(2 * c + 1) * HIDDEN_PAD : (2 * c + 2) * HIDDEN_PAD]
        units.append(gate * jax.nn.sigmoid(gate) * up)
    units = jnp.concatenate(units, axis=0).astype(BF16)

    steps = order + [0]
    sums = dot(dtc[...], units)
    p5b[...] = sums.astype(BF16).reshape(n, n, half, seqs)
    p5[...] = sums.reshape(n, n * half, seqs)
    for dz, dy in sorted([(a, b) for a in steps for b in steps], key=lambda p: -min(p[0], n - p[0]) - min(p[1], n - p[1])):
        if dz or dy:
            to_z, to_y = lax.rem(z + dz, n), lax.rem(y + dy, n)
            at_f, at_s = to_z + (to_y - to_z) * tp, to_y + (to_z - to_y) * tp
            peer = (dp, to_z * n + to_y, tp)
            send(p5b.at[at_f, at_s], r3.at[dz * n + dy - 1], s8, v8, peer)
    mine_at = jnp.where(iota((half, lanes), 1) == iota((half, lanes), 0) + y * half, 1.0, 0.0)
    last = dot(mine_at.astype(BF16), rt[tp, z].reshape(seqs, lanes), 1, 1)
    last = last + p5[first, pl.ds(pl.multiple_of(second * half, half), half), :]
    c2 = iota((seqs, seqs), 1)
    back = ((c2 // 2) % n) * 2 * n + (c2 // (2 * n)) * 2 + c2 % 2
    back = jnp.where(iota((seqs, seqs), 0) == back, 1.0, 0.0).astype(BF16)
    total(r3, s8, v8).wait_recv()
    last = last + jnp.sum(r3[...].astype(F32), axis=0)
    out_ref[...] = dot(last.astype(BF16), back).astype(BF16)

    total(relay, sr, vr.at[0]).wait_send()
    total(r1, s1, v1).wait_send()
    total(r2, s2, v2).wait_send()
    for c in (all_wg, all_tg, all_mh):
        c.wait_send()
    flat_r = rt.reshape(2 * kvs, 2 * n, lanes)
    total(flat_r.at[pl.ds(0, kvs - 1)], s5, v5.at[0]).wait_send()
    total(rt.at[0], s6, v6).wait_send()
    total(gu.at[0], sg, vg).wait_send()
    total(dts, sd, vd).wait_send()
    total(r3, s8, v8).wait_send()


def per_device(n, *args):
    (tokens, pre, qw, kw, vw, ow, ig, fg, ck, cv, ci, cf, lens, sm, sn, smax) = args[:16]
    hg, mixw, mg, gw, uw, dw = args[16:]
    operands = (
        tokens.T,
        pre.reshape(1, -1),
        qw,
        kw,
        vw,
        ow,
        ig.T,
        fg.T,
        ck,
        cv,
        ci.transpose(0, 2, 1),
        cf.transpose(0, 2, 1),
        lens,
        sm,
        sn,
        smax,
        hg.reshape(1, -1),
        mixw.T,
        mg.reshape(1, -1),
        gw.T,
        uw.T,
        dw,
    )
    seqs, width = tokens.shape
    cols = qw.shape[1]
    kvs = n * n
    model = width * kvs
    span, size = ck.shape[1], sn.shape[2]
    wide = KINDS * cols + 128
    half = width // 2
    dma = pltpu.SemaphoreType.DMA
    vmem = pltpu.VMEM
    ff = gw.shape[1]
    scratch = [
        vmem((width, seqs), BF16),
        vmem((1, width), F32),
        vmem((KINDS, width, cols), BF16),
        vmem((2, 4, model), BF16),
        vmem((2, 2, 2, span), F32),
        pltpu.SMEM((2,), jnp.int32),
        pltpu.SMEM((2, 2), F32),
        vmem((2, 2, size, size), F32),
        vmem((2, 2, size), F32),
        vmem((2, 2, span, cols), BF16),
        vmem((1, cols), F32),
        vmem((width, cols), BF16),
        vmem((1, model), F32),
        vmem((3, ff, model), BF16),
        dma((14,)),
        vmem((n, 2 * n, wide), BF16),
        vmem((n - 2, 2 * n, wide), BF16),
        vmem((2 * n, wide), BF16),
        vmem((2 * n, wide), BF16),
        vmem((n * ROWS, 128), F32),
        vmem((n, ROWS, 128), BF16),
        vmem((n - 1, ROWS, 128), BF16),
        vmem((2, 4, size, size), BF16),
        vmem((8 * n, 8 * n), BF16),
        vmem((2, n, 8, 128), BF16),
        vmem((2, n, half, cols), BF16),
        vmem((n, half, seqs), BF16),
        vmem((2 * n, n * half), BF16),
        vmem((2, n, n, 2 * n, n * half), BF16),
        vmem((2, 2 * HIDDEN_PAD, model), BF16),
        vmem((2, kvs, half, HIDDEN_PAD), BF16),
        vmem((kvs, half, HIDDEN_PAD), BF16),
        vmem((kvs * half, 2 * HIDDEN_PAD), BF16),
        vmem((n, n * half, seqs), F32),
        vmem((n, n, half, seqs), BF16),
        vmem((kvs - 1, half, seqs), BF16),
        dma,
        dma,
        dma,
        dma((2,)),
        dma,
        dma,
        dma,
        dma,
        dma,
        dma,
        dma,
        dma,
        dma,
        dma((n,)),
        dma,
        dma,
        dma,
        dma,
        dma,
        dma,
        dma,
        dma,
    ]
    out = pl.pallas_call(
        functools.partial(kernel, n),
        out_shape=jax.ShapeDtypeStruct((half, seqs), BF16),
        in_specs=[pl.BlockSpec(memory_space=pl.ANY)] * len(operands),
        out_specs=pl.BlockSpec(memory_space=pltpu.VMEM),
        scratch_shapes=scratch,
        compiler_params=pltpu.CompilerParams(
            collective_id=0, has_side_effects=True, vmem_limit_bytes=24 * 1024 * 1024
        ),
        name="layer",
    )(*[pltpu.with_memory_space_constraint(o, pltpu.HBM) for o in operands])
    return out.T


def solution(mesh):
    n = round(mesh.shape["kv"] ** 0.5)
    seq = ("dp", "kv")
    return jax.shard_map(
        functools.partial(per_device, n),
        mesh=mesh,
        in_specs=(
            P("dp", "kv"),
            P("kv"),
            P("kv", "tp"),
            P("kv", "tp"),
            P("kv", "tp"),
            P("kv", "tp"),
            P(),
            P(),
            P(seq, None, "tp"),
            P(seq, None, "tp"),
            P(seq, None, "tp"),
            P(seq, None, "tp"),
            P(seq),
            P(seq, "tp", None, None),
            P(seq, "tp", None),
            P(seq, "tp"),
            P("tp"),
            P("tp", "kv"),
            P(),
            P(None, ("kv", "tp")),
            P(None, ("kv", "tp")),
            P(("kv", "tp"), None),
        ),
        out_specs=P("dp", ("kv", "tp")),
        check_vma=False,
    )
```
